256 devices in a mesh: grp: 2 (over y), ep: 32 (over z, core), tp: 4 (over x).
Axes of the slice: x: 4, y: 2, z: 16, core: 2. Of those that a mesh axis runs over, the one named last changes fastest.
The devices are a block of a 4x16x16 slice.
Arguments:
- conv_input: bfloat16 [40960, 2048], P(('grp', 'ep')), parts along dimension 0, may hold values from -6 to 6
- conv_taps: float32 [31, 2048], replicated, may hold values from -1 to 1
- conv_gain: float32 [2048], replicated, may hold values from 0.1 to 1.9
- conv_weight: bfloat16 [2048, 2048], P(None, 'tp'), may hold values from -0.125 to 0.125
- moe_input: bfloat16 [40960, 2048], P(('grp', 'ep')), parts along dimension 0, may hold values from -6 to 6
- moe_gain: float32 [2048], replicated, may hold values from 0.1 to 1.9
- expert_ids: int32 [40960, 2], P(('grp', 'ep')), parts along dimension 0, may hold values from 0 to 31, as said below
- route_weights: float32 [40960, 2], P(('grp', 'ep')), parts along dimension 0, may hold values from 0.1 to 1
- gate_weight: bfloat16 [32, 2048, 1024], P('ep', None, 'tp'), may hold values from -0.125 to 0.125
- up_weight: bfloat16 [32, 2048, 1024], P('ep', None, 'tp'), may hold values from -0.125 to 0.125
- down_weight: bfloat16 [32, 1024, 2048], P('ep', 'tp'), may hold values from -0.1875 to 0.1875
- post_gain: float32 [2048], replicated, may hold values from 0.1 to 1.9
Outputs:
- conv_out: bfloat16 [40960, 2048], P(('grp', 'ep'), 'tp'), parts along dimension 0
- moe_out: bfloat16 [40960, 2048], P(('grp', 'ep', 'tp')), parts along dimension 0
The draws below stay inside these ranges and needn't reach their ends.
There are 2 independent parts, one for each index of `grp`. The reference program is written for one: setup_inputs(seed, part) draws one part's arguments, and reference() takes and returns one part's arrays. A program takes and returns all parts, laid end to end along the dimension named above; an argument that names none is the same for every part. Nothing has to cross between parts.
Inputs may be any that keep to these rules, and one draw needn't show every extreme that they name: `expert_ids`: in each aligned block of 160 tokens, every expert is named exactly 10 times; a token's two experts differ and lie in one group of 4 consecutive experts.
All inputs are finite; a program needn't handle non-finite values.
Results may differ from the reference program's by a relative error of at most 0.012.
Values may be sent and summed in bfloat16 or wider, within the bound.
No kernel may reach another device: no remote copies, remote signals or barrier semaphores. Data moves between devices by JAX's collectives and lax.ppermute only.
A program may use at most 128 MiB of HBM per device.

```python
import jax
import jax.numpy as jnp
from jax import lax

D = 2048
FF = 1024
KW = 31
GROUP = 4
TOPK = 2
EXPERTS = 32
TOKENS = 20480
BLOCK = 160
N_TP = 4


def draw_expert_ids(key, part):
    block_count = TOKENS // BLOCK
    key_list = jax.random.split(jax.random.fold_in(key, 7), block_count)

    def one_block(block_key):
        key_perm, key_shift = jax.random.split(block_key)
        ordering = jax.random.permutation(key_perm, BLOCK)
        offset = jax.random.randint(key_shift, (), 0, GROUP - 1)
        primary = ordering % EXPERTS
        second = primary // GROUP * GROUP + (primary % GROUP + 1 + offset) % GROUP
        return jnp.stack([primary, second], axis=1)
    return jax.vmap(one_block)(key_list).reshape(TOKENS, 2).astype(jnp.int32)


def shard_levels(own_key, extent, cuts, low, high):
    level = 1.0
    for dim, parts in cuts:
        draws = jax.random.uniform(jax.random.fold_in(jax.random.fold_in(own_key, 6), dim), (parts,), jnp.float32, low / len(cuts), high / len(cuts))
        level = level * jnp.repeat(jnp.exp(draws), extent[dim] // parts).reshape((-1,) + (1,) * (len(extent) - 1 - dim))
    return level


def bell_draw(key, shape, scale, limit, cuts=(), kind=jnp.bfloat16):
    result = jax.random.normal(key, shape, jnp.float32) * scale
    if len(cuts) > 0:
        result = shard_levels(key, shape, cuts, -0.22, 0.18) * result
    return jnp.clip(result, min=-limit, max=limit).astype(kind)


def setup_inputs(seed: int = 0, part: int = 0) -> dict:
    keys = jax.random.split(jax.random.key(seed), 13)
    part_splits = jax.random.split(jax.random.fold_in(keys[12], part), 13)
    conv_input = bell_draw(part_splits[0], (TOKENS, D), 1.0, 6.0, ((0, 32),))
    conv_taps = bell_draw(keys[1], (KW, D), KW ** -0.5, 1.0, (), jnp.float32)
    conv_gain = jnp.clip(1.0 + 0.18 * jax.random.normal(keys[2], (D,), jnp.float32), 0.1, 1.9)
    conv_weight = bell_draw(keys[3], (D, D), D ** -0.5, 0.125, ((1, 4),))
    moe_input = bell_draw(part_splits[4], (TOKENS, D), 1.0, 6.0, ((0, 32),))
    moe_gain = jnp.clip(1.0 + 0.18 * jax.random.normal(keys[5], (D,), jnp.float32), 0.1, 1.9)
    expert_ids = draw_expert_ids(jax.random.fold_in(jax.random.fold_in(keys[12], part), 71), part)
    route_weights = jnp.clip(0.1 + 0.9 * jax.random.uniform(part_splits[7], (TOKENS, TOPK), jnp.float32) ** shard_levels(part_splits[7], (TOKENS, TOPK), ((0, 32),), -0.2, 0.2), 0.1, 1.0)
    gate_weight = bell_draw(keys[8], (EXPERTS, D, FF), D ** -0.5, 0.125, ((0, 32), (2, 4)))
    up_weight = bell_draw(keys[9], (EXPERTS, D, FF), D ** -0.5, 0.125, ((0, 32), (2, 4)))
    down_weight = bell_draw(keys[10], (EXPERTS, FF, D), FF ** -0.5, 0.1875, ((0, 32), (1, 4)))
    post_gain = jnp.clip(1.0 + 0.18 * jax.random.normal(keys[11], (D,), jnp.float32), 0.1, 1.9)
    return dict(conv_input=conv_input, conv_taps=conv_taps, conv_gain=conv_gain, conv_weight=conv_weight, moe_input=moe_input, moe_gain=moe_gain, expert_ids=expert_ids, route_weights=route_weights, gate_weight=gate_weight, up_weight=up_weight, down_weight=down_weight, post_gain=post_gain)


EPSILON = 1e-06

def channel_norm(values, scales):
    mean_square = lax.optimization_barrier(jnp.mean(values * values, axis=-1, keepdims=True))
    return values * lax.rsqrt(mean_square + EPSILON) * scales

def causal_conv(signal, kernel_taps):
    length = signal.shape[0]
    padded = jnp.pad(signal.astype(jnp.float32), ((KW - 1, 0), (0, 0)))
    conv_sum = jnp.zeros((length, signal.shape[1]), jnp.float32)
    for offset in range(KW):
        conv_sum = conv_sum + padded[offset:offset + length] * kernel_taps[offset]
    return conv_sum

def expert_apply(operands):
    expert_rows, gate_part, up_part, down_part = operands
    gate_value = jnp.dot(expert_rows, gate_part, preferred_element_type=jnp.float32)
    up_value = jnp.dot(expert_rows, up_part, preferred_element_type=jnp.float32)
    hidden = (jax.nn.silu(gate_value) * up_value).astype(jnp.bfloat16)
    pieces = hidden.reshape(hidden.shape[0], N_TP, FF // N_TP).astype(jnp.float32)
    down_pieces = down_part.reshape(N_TP, FF // N_TP, D).astype(jnp.float32)
    partial_value = jnp.einsum('ctf,tfd->tcd', pieces, down_pieces)
    partial_value = lax.optimization_barrier(partial_value.astype(jnp.bfloat16)).astype(jnp.float32)
    return lax.optimization_barrier(jnp.sum(partial_value, axis=0)).astype(jnp.bfloat16)

def reference(conv_input, conv_taps, conv_gain, conv_weight, moe_input, moe_gain, expert_ids, route_weights, gate_weight, up_weight, down_weight, post_gain):
    conv_sum = causal_conv(conv_input, conv_taps)
    activated = jax.nn.silu(channel_norm(conv_sum, conv_gain)).astype(jnp.bfloat16)
    conv_out = jnp.dot(activated, conv_weight, preferred_element_type=jnp.float32).astype(jnp.bfloat16)
    normed = channel_norm(moe_input.astype(jnp.float32), moe_gain).astype(jnp.bfloat16)
    flat_ids = expert_ids.reshape(-1).astype(jnp.int32)
    entry_count = flat_ids.shape[0]
    per_expert = entry_count // EXPERTS
    onehot = (flat_ids[:, None] == jnp.arange(EXPERTS, dtype=jnp.int32)[None, :]).astype(jnp.int32)
    position = lax.optimization_barrier(jnp.sum((jnp.cumsum(onehot, axis=0) - 1) * onehot, axis=1)).astype(jnp.int32)
    target = (flat_ids * per_expert + position).astype(jnp.int32)
    source_entry = jnp.zeros((entry_count,), jnp.int32).at[target].set(jnp.arange(entry_count, dtype=jnp.int32))
    expert_rows = normed[source_entry // 2].reshape(EXPERTS, per_expert, D)
    results = lax.map(expert_apply, (expert_rows, gate_weight, up_weight, down_weight))
    entry_results = results.reshape(entry_count, D)[target].reshape(-1, TOPK, D).astype(jnp.float32)
    mixed_rows = lax.optimization_barrier(jnp.sum(entry_results * route_weights[:, :, None], axis=1))
    moe_out = channel_norm(mixed_rows, post_gain).astype(jnp.bfloat16)
    return (conv_out, moe_out)
```

```python
import jax
import jax.numpy as jnp
from jax import lax
from jax.experimental import pallas as pl
from jax.experimental.pallas import tpu as pltpu
from jax.sharding import PartitionSpec as P

EPSILON = 1e-06
LANES = 128
F32 = jnp.float32
BF16 = jnp.bfloat16


def whole():
    return pl.BlockSpec(memory_space=pltpu.VMEM)


def dot(a, b):
    return jnp.dot(a, b, preferred_element_type=F32)


def split_rows(capacity):
    main = capacity // 8 * 8
    return main, capacity - main


def col(ref_or_value, c):
    return ref_or_value[:, c * LANES : (c + 1) * LANES]


def selection(index, first, count, dim):
    shape = (count, index.shape[1]) if dim == 0 else (index.shape[0], count)
    return index == first + lax.broadcasted_iota(jnp.int32, shape, dim)


def put_message(out_ref, head_of, tail_of, peers, head, tail, blocks):
    for c in range(0, blocks, 2):
        pair = [head_of(c + i).reshape(peers, head, LANES) for i in range(2)]
        out_ref[:, c * head : (c + 2) * head, :] = jnp.concatenate(pair, axis=1).astype(BF16)
    per = 8 // tail
    base = blocks * head
    for j in range(0, blocks // per, 2):
        pair = [tail_of(j + i).reshape(peers, 8, LANES) for i in range(2)]
        out_ref[:, base + j * 8 : base + (j + 2) * 8, :] = jnp.concatenate(pair, axis=1).astype(BF16)


def dispatch_kernel(own_ref, rows_ref, gain_ref, ids_ref, out_ref, target_ref, *, experts, capacity):
    del own_ref
    tokens, width = rows_ref.shape
    blocks = width // LANES
    head, tail = split_rows(capacity)
    per = 8 // tail
    rows = rows_ref[...].astype(F32)
    mean_square = jnp.mean(rows * rows, axis=-1, keepdims=True)
    normed = (rows * lax.rsqrt(mean_square + EPSILON) * gain_ref[...]).astype(BF16)
    ids = ids_ref[...]
    onehot = [
        (ids[k : k + 1, :] == lax.broadcasted_iota(jnp.int32, (experts, tokens), 0)).astype(F32)
        for k in range(2)
    ]
    before = lax.broadcasted_iota(jnp.int32, (tokens, tokens), 0) < lax.broadcasted_iota(
        jnp.int32, (tokens, tokens), 1
    )
    before = before.astype(F32).astype(BF16)
    counts = [dot(h.astype(BF16), before) for h in onehot]
    counts[1] = counts[1] + jnp.sum(onehot[0], axis=1, keepdims=True)
    place = [jnp.sum(c * h, axis=0, keepdims=True).astype(jnp.int32) for c, h in zip(counts, onehot)]
    place = jnp.concatenate(place, axis=0)
    target_ref[...] = ids * capacity + place
    in_head = jnp.where(place < head, ids * head + place, -64)
    in_tail = jnp.where(place < head, -64, ids * 8 + place - head)
    pick = jnp.zeros((experts * head, tokens), F32)
    picks = [jnp.zeros((experts * 8, tokens), F32) for _ in range(per)]
    for k in range(2):
        pick = pick + selection(in_head[k : k + 1], 0, experts * head, 0).astype(F32)
        for q in range(per):
            picks[q] = picks[q] + selection(in_tail[k : k + 1], -q * tail, experts * 8, 0).astype(F32)
    pick = pick.astype(BF16)
    picks = jnp.concatenate(picks, axis=1).astype(BF16)

    def tail_of(j):
        stack = [col(normed, per * j + q) for q in range(per)]
        return dot(picks, jnp.concatenate(stack, axis=0))

    put_message(
        out_ref, lambda c: dot(pick, col(normed, c)), tail_of, experts, head, tail, blocks
    )


def dispatch(own, rows, gain, ids, experts, capacity):
    tokens = ids.shape[1]
    width = rows.shape[1]
    grid_spec = pltpu.PrefetchScalarGridSpec(
        num_scalar_prefetch=1,
        grid=(1,),
        in_specs=[
            pl.BlockSpec((tokens, width), lambda i, own: (own[0], 0)),
            pl.BlockSpec((1, width), lambda i, own: (0, 0)),
            pl.BlockSpec((2, tokens), lambda i, own: (0, 0)),
        ],
        out_specs=[
            pl.BlockSpec((experts, capacity * width // LANES, LANES), lambda i, own: (0, 0, 0)),
            pl.BlockSpec((2, tokens), lambda i, own: (0, 0)),
        ],
    )

    def kernel(*refs):
        dispatch_kernel(*refs, experts=experts, capacity=capacity)

    return pl.pallas_call(
        kernel,
        grid_spec=grid_spec,
        out_shape=[
            jax.ShapeDtypeStruct((experts, capacity * width // LANES, LANES), BF16),
            jax.ShapeDtypeStruct((2, tokens), jnp.int32),
        ],
        compiler_params=pltpu.CompilerParams(vmem_limit_bytes=24 << 20),
        name="dispatch",
    )(own, rows, gain, ids)


def expert_kernel(*refs, sources, peers, capacity, blocks):
    count = len(refs) // 2 - 2
    message_ref, out_ref = refs[0], refs[count + 1]
    remote = refs[1 : count + 1]
    rows_ref, hidden_ref, signals = refs[count + 2], refs[count + 3], refs[-1]
    weights = refs[count + 4 : -1]
    copies = [
        pltpu.make_async_copy(far, near, signals.at[i])
        for i, (far, near) in enumerate(zip(remote, weights))
    ]
    for copy in copies:
        copy.start()
    head, tail = split_rows(capacity)
    per = 8 // tail
    heads = peers * head
    for c in range(0, blocks, 2):
        both = message_ref[:, c * head : (c + 2) * head, :].astype(F32)
        for i in range(2):
            part = both[:, i * head : (i + 1) * head, :].reshape(heads, LANES)
            rows_ref[0:heads, (c + i) * LANES : (c + i + 1) * LANES] = part.astype(BF16)
    base = blocks * head
    slot = lax.broadcasted_iota(jnp.int32, (peers * tail, peers * 8), 0)
    lane = lax.broadcasted_iota(jnp.int32, (peers * tail, peers * 8), 1)
    gathers = [
        (lane == slot // tail * 8 + q * tail + slot % tail).astype(F32).astype(BF16)
        for q in range(per)
    ]
    for j in range(0, blocks // per, 2):
        both = message_ref[:, base + j * 8 : base + (j + 2) * 8, :].astype(F32)
        for i in range(2):
            part = both[:, i * 8 : (i + 1) * 8, :].reshape(peers * 8, LANES).astype(BF16)
            for q in range(per):
                c = per * (j + i) + q
                rows_ref[heads:, c * LANES : (c + 1) * LANES] = dot(gathers[q], part).astype(BF16)
    at = 0
    downs = []
    for gates, ups, down_parts in sources:
        rows = rows_ref[...]
        values = []
        for group in (gates, ups):
            value = None
            begin = 0
            for g in group:
                copies[g].wait()
                size = weights[g].shape[0]
                part = dot(rows[:, begin : begin + size], weights[g][...])
                value = part if value is None else value + part
                begin += size
            values.append(value)
        gate_value, up_value = values
        hidden = gate_value / (1.0 + jnp.exp(-gate_value)) * up_value
        hidden_ref[:, at : at + hidden.shape[1]] = hidden.astype(BF16)
        for d in down_parts:
            downs.append((at, d))
            at += weights[d].shape[0]
    for _, d in downs:
        copies[d].wait()
    slot = lax.broadcasted_iota(jnp.int32, (peers * 8, peers * tail), 1)
    lane = lax.broadcasted_iota(jnp.int32, (peers * 8, peers * tail), 0)
    spreads = [
        (lane == slot // tail * 8 + q * tail + slot % tail).astype(F32).astype(BF16)
        for q in range(per)
    ]
    step = 2 * per
    for first in range(0, blocks, step):
        cols = slice(first * LANES, (first + step) * LANES)
        total = None
        for begin, d in downs:
            size = weights[d].shape[0]
            part = dot(hidden_ref[:, begin : begin + size], weights[d][:, cols])
            total = part if total is None else total + part
        for c in range(0, step, 2):
            pair = [col(total, c + i)[0:heads].reshape(peers, head, LANES) for i in range(2)]
            at_row = (first + c) * head
            out_ref[:, at_row : at_row + 2 * head, :] = jnp.concatenate(pair, axis=1).astype(BF16)
        last = total[heads:].astype(BF16)
        pair = []
        for i in range(2):
            spread = None
            for q in range(per):
                part = dot(spreads[q], col(last, per * i + q))
                spread = part if spread is None else spread + part
            pair.append(spread.reshape(peers, 8, LANES))
        at_row = base + first // per * 8
        out_ref[:, at_row : at_row + 16, :] = jnp.concatenate(pair, axis=1).astype(BF16)


def experts_apply(message, weights, sources, capacity):
    peers, lines, _ = message.shape
    blocks = lines // capacity
    units = sum(weights[d].shape[0] for s in sources for d in s[2])

    def kernel(*refs):
        expert_kernel(*refs, sources=sources, peers=peers, capacity=capacity, blocks=blocks)

    return pl.pallas_call(
        kernel,
        in_specs=[whole()] + [pl.BlockSpec(memory_space=pltpu.HBM)] * len(weights),
        out_specs=whole(),
        out_shape=jax.ShapeDtypeStruct(message.shape, BF16),
        scratch_shapes=[
            pltpu.VMEM((peers * capacity, blocks * LANES), BF16),
            pltpu.VMEM((peers * capacity, units), BF16),
            *(pltpu.VMEM(w.shape, BF16) for w in weights),
            pltpu.SemaphoreType.DMA((len(weights),)),
        ],
        compiler_params=pltpu.CompilerParams(vmem_limit_bytes=60 << 20),
        name="experts",
    )(message, *weights)


def combine_kernel(message_ref, target_ref, weight_ref, gain_ref, out_ref, mixed_ref, *, capacity):
    peers = message_ref.shape[0]
    tokens, width = out_ref.shape
    blocks = width // LANES
    head, tail = split_rows(capacity)
    per = 8 // tail
    heads = peers * head
    target = target_ref[...]
    peer = target // capacity
    place = target - peer * capacity
    in_head = jnp.where(place < head, peer * head + place, -64)
    in_tail = jnp.where(place < head, -64, peer * 8 + place - head)
    pick = [selection(in_head[:, k : k + 1], 0, heads, 1).astype(F32) for k in range(2)]
    pick = jnp.concatenate(pick, axis=0).astype(BF16)
    picks = []
    for q in range(per):
        both = [selection(in_tail[:, k : k + 1], -q * tail, peers * 8, 1).astype(F32) for k in range(2)]
        picks.append(jnp.concatenate(both, axis=0).astype(BF16))
    weight = [weight_ref[:, k : k + 1] for k in range(2)]
    base = blocks * head
    square = jnp.zeros((tokens, LANES), F32)
    for c in range(0, blocks, 2):
        both = message_ref[:, c * head : (c + 2) * head, :].astype(F32)
        for i in range(2):
            part = both[:, i * head : (i + 1) * head, :].reshape(heads, LANES).astype(BF16)
            j = (c + i) // per
            rest = message_ref[:, base + j // 2 * 16 : base + j // 2 * 16 + 16, :].astype(F32)
            rest = rest[:, j % 2 * 8 : j % 2 * 8 + 8, :].reshape(peers * 8, LANES).astype(BF16)
            rows = dot(pick, part) + dot(picks[(c + i) % per], rest)
            mixed = rows[:tokens] * weight[0] + rows[tokens:] * weight[1]
            mixed_ref[:, (c + i) * LANES : (c + i + 1) * LANES] = mixed
            square = square + mixed * mixed
    scale = lax.rsqrt(jnp.sum(square, axis=1, keepdims=True) * (1.0 / width) + EPSILON)
    out_ref[...] = (mixed_ref[...] * scale * gain_ref[...]).astype(BF16)


def combine(message, target, weight, gain, capacity):
    tokens = target.shape[0]
    width = gain.shape[1]

    def kernel(*refs):
        combine_kernel(*refs, capacity=capacity)

    return pl.pallas_call(
        kernel,
        in_specs=[whole()] * 4,
        out_specs=whole(),
        out_shape=jax.ShapeDtypeStruct((tokens, width), BF16),
        scratch_shapes=[pltpu.VMEM((tokens, width), F32)],
        compiler_params=pltpu.CompilerParams(vmem_limit_bytes=24 << 20),
        name="combine",
    )(message, target, weight, gain)


def conv_kernel(rows_ref, carried_ref, taps_ref, gain_ref, weight_ref, out_ref, line_ref, sum_ref):
    block, width = rows_ref.shape
    blocks = width // LANES
    reach = taps_ref.shape[0] - 1
    halo = line_ref.shape[1] - block
    step = pl.program_id(0)

    @pl.when(step == 0)
    def _():
        for c in range(blocks):
            line_ref[c, 0:halo, :] = col(carried_ref, c).astype(F32)

    @pl.when(step > 0)
    def _():
        for c in range(blocks):
            line_ref[c, 0:halo, :] = line_ref[c, block : block + halo, :]

    for c in range(blocks):
        line_ref[c, halo:, :] = col(rows_ref, c).astype(F32)

    strip = 64

    def column(c, square):
        parts = []
        for first in range(0, block, strip):
            total = jnp.zeros((strip, LANES), F32)
            for k in range(reach + 1):
                at = first + halo - reach + k
                total = total + line_ref[c, at : at + strip, :] * taps_ref[k, pl.ds(c, 1), :]
            sum_ref[c, first : first + strip, :] = total
            parts.append(total * total)
        return square + jnp.concatenate(parts, axis=0)

    square = lax.fori_loop(0, blocks, column, jnp.zeros((block, LANES), F32))
    scale = lax.rsqrt(jnp.sum(square, axis=1, keepdims=True) * (1.0 / width) + EPSILON)
    result = jnp.zeros((block, out_ref.shape[1]), F32)
    for c in range(0, blocks, 4):
        group = []
        for i in range(4):
            value = sum_ref[c + i] * scale * col(gain_ref, c + i)
            group.append((value / (1.0 + jnp.exp(-value))).astype(BF16))
        part = jnp.concatenate(group, axis=1)
        result = result + dot(part, weight_ref[c * LANES : (c + 4) * LANES, :])
    out_ref[...] = result.astype(BF16)


def conv_module(rows, carried, taps, gain, weight, block=128):
    count, width = rows.shape
    blocks = width // LANES
    halo = carried.shape[0]
    return pl.pallas_call(
        conv_kernel,
        grid=(count // block,),
        in_specs=[
            pl.BlockSpec((block, width), lambda i: (i, 0)),
            pl.BlockSpec((halo, width), lambda i: (0, 0)),
            pl.BlockSpec((taps.shape[0], blocks, LANES), lambda i: (0, 0, 0)),
            pl.BlockSpec((1, width), lambda i: (0, 0)),
            pl.BlockSpec(weight.shape, lambda i: (0, 0)),
        ],
        out_specs=pl.BlockSpec((block, weight.shape[1]), lambda i: (i, 0)),
        out_shape=jax.ShapeDtypeStruct((count, weight.shape[1]), BF16),
        scratch_shapes=[
            pltpu.VMEM((blocks, block + halo, LANES), F32),
            pltpu.VMEM((blocks, block, LANES), F32),
        ],
        compiler_params=pltpu.CompilerParams(vmem_limit_bytes=24 << 20),
        name="conv",
    )(rows, carried, taps.reshape(taps.shape[0], blocks, LANES), gain, weight)


EP = "ep"
GRP_EP = ("grp", "ep")
GRP_EP_TP = ("grp", "ep", "tp")
HALO = 32


def run(
    conv_input,
    conv_taps,
    conv_gain,
    conv_weight,
    moe_input,
    moe_gain,
    expert_ids,
    route_weights,
    gate_weight,
    up_weight,
    down_weight,
    post_gain,
):
    quarters = lax.axis_size("tp")
    ep_count = lax.axis_size(EP)
    width = moe_input.shape[1]
    tokens = moe_input.shape[0] // quarters
    capacity = 2 * tokens // ep_count
    own = lax.axis_index("tp").astype(jnp.int32)

    right = [(i, (i + 1) % quarters) for i in range(quarters)]
    left = [(i, (i - 1) % quarters) for i in range(quarters)]
    gate, up, down = gate_weight[0], up_weight[0], down_weight[0]
    half = down.shape[0] // 2
    down_a, down_b = down[:half], down[half:]

    def send(array, pairs):
        return lax.ppermute(array, "tp", pairs)

    gate_r, up_l = send(gate, right), send(up, left)
    own_ids = lax.dynamic_slice_in_dim(expert_ids, own * tokens, tokens, 0).T
    message, target = dispatch(
        own.reshape(1), moe_input, moe_gain.reshape(1, width), own_ids, ep_count, capacity
    )
    arrived = lax.all_to_all(message, EP, 0, 0, tiled=True)
    down_r, down_l = send(down_a, right), send(down_b, left)
    up_r, gate_l = send(up, right), send(gate, left)
    rest_r, rest_l = send(down_b, right), send(down_a, left)
    gate_far, up_far = send(gate_r, right), send(up_l, left)
    down_far, rest_far = send(down_r, right), send(down_l, left)

    pairs = [(i, i + 1) for i in range(ep_count - 1)]
    carried = lax.ppermute(conv_input[conv_input.shape[0] - HALO :], EP, pairs)
    conv_out = conv_module(conv_input, carried, conv_taps, conv_gain.reshape(1, width), conv_weight)

    weights = [gate, up, down]
    sources = [((0,), (1,), (2,))]
    for arrays in (
        (gate_r, up_r, down_r, rest_r),
        (gate_l, up_l, rest_l, down_l),
        (gate_far, up_far, down_far, rest_far),
    ):
        at = len(weights)
        weights.extend(arrays)
        sources.append(((at,), (at + 1,), (at + 2, at + 3)))
    results = experts_apply(arrived, weights, tuple(sources), capacity)
    returned = lax.all_to_all(results, EP, 0, 0, tiled=True)
    own_weights = lax.dynamic_slice_in_dim(route_weights, own * tokens, tokens, 0)
    moe_out = combine(returned, target.T, own_weights, post_gain.reshape(1, width), capacity)
    return (conv_out, moe_out)


def solution(mesh):
    return jax.shard_map(
        run,
        mesh=mesh,
        in_specs=(
            P(GRP_EP, None),
            P(),
            P(),
            P(None, "tp"),
            P(GRP_EP, None),
            P(),
            P(GRP_EP, None),
            P(GRP_EP, None),
            P(EP, None, "tp"),
            P(EP, None, "tp"),
            P(EP, "tp", None),
            P(),
        ),
        out_specs=(P(GRP_EP, "tp"), P(GRP_EP_TP, None)),
        check_vma=False,
    )
```

```python
import jax
import jax.numpy as jnp
from jax import lax
from jax.experimental import pallas as pl
from jax.experimental.pallas import tpu as pltpu
from jax.sharding import PartitionSpec as P

EPSILON = 1e-06
LANES = 128
F32 = jnp.float32
BF16 = jnp.bfloat16


def whole():
    return pl.BlockSpec(memory_space=pltpu.VMEM)


def dot(a, b):
    return jnp.dot(a, b, preferred_element_type=F32)


def split_rows(capacity):
    main = capacity // 8 * 8
    return main, capacity - main


def col(ref_or_value, c):
    return ref_or_value[:, c * LANES : (c + 1) * LANES]


def selection(index, first, count, dim):
    shape = (count, index.shape[1]) if dim == 0 else (index.shape[0], count)
    return index == first + lax.broadcasted_iota(jnp.int32, shape, dim)


def put_message(out_ref, head_of, tail_of, peers, head, tail, blocks):
    for c in range(0, blocks, 2):
        pair = [head_of(c + i).reshape(peers, head, LANES) for i in range(2)]
        out_ref[:, c * head : (c + 2) * head, :] = jnp.concatenate(pair, axis=1).astype(BF16)
    per = 8 // tail
    base = blocks * head
    for j in range(0, blocks // per, 2):
        pair = [tail_of(j + i).reshape(peers, 8, LANES) for i in range(2)]
        out_ref[:, base + j * 8 : base + (j + 2) * 8, :] = jnp.concatenate(pair, axis=1).astype(BF16)


def dispatch_kernel(
    own_ref, all_ref, gain_ref, ids_ref, out_ref, target_ref, rows_ref, signal, *, experts, capacity
):
    tokens, width = rows_ref.shape
    copy = pltpu.make_async_copy(
        all_ref.at[pl.ds(pl.multiple_of(own_ref[0] * tokens, 16), tokens), :], rows_ref, signal
    )
    copy.start()
    blocks = width // LANES
    head, tail = split_rows(capacity)
    per = 8 // tail
    ids = ids_ref[...]
    onehot = [
        (ids[k : k + 1, :] == lax.broadcasted_iota(jnp.int32, (experts, tokens), 0)).astype(F32)
        for k in range(2)
    ]
    before = lax.broadcasted_iota(jnp.int32, (tokens, tokens), 0) < lax.broadcasted_iota(
        jnp.int32, (tokens, tokens), 1
    )
    before = before.astype(F32).astype(BF16)
    counts = [dot(h.astype(BF16), before) for h in onehot]
    counts[1] = counts[1] + jnp.sum(onehot[0], axis=1, keepdims=True)
    place = [jnp.sum(c * h, axis=0, keepdims=True).astype(jnp.int32) for c, h in zip(counts, onehot)]
    place = jnp.concatenate(place, axis=0)
    target_ref[...] = ids * capacity + place
    in_head = jnp.where(place < head, ids * head + place, -64)
    in_tail = jnp.where(place < head, -64, ids * 8 + place - head)
    pick = jnp.zeros((experts * head, tokens), F32)
    picks = [jnp.zeros((experts * 8, tokens), F32) for _ in range(per)]
    for k in range(2):
        pick = pick + selection(in_head[k : k + 1], 0, experts * head, 0).astype(F32)
        for q in range(per):
            picks[q] = picks[q] + selection(in_tail[k : k + 1], -q * tail, experts * 8, 0).astype(F32)
    pick = pick.astype(BF16)
    picks = jnp.concatenate(picks, axis=1).astype(BF16)
    copy.wait()
    rows = rows_ref[...].astype(F32)
    mean_square = jnp.mean(rows * rows, axis=-1, keepdims=True)
    normed = (rows * lax.rsqrt(mean_square + EPSILON) * gain_ref[...]).astype(BF16)

    def tail_of(j):
        stack = [col(normed, per * j + q) for q in range(per)]
        return dot(picks, jnp.concatenate(stack, axis=0))

    put_message(
        out_ref, lambda c: dot(pick, col(normed, c)), tail_of, experts, head, tail, blocks
    )


def dispatch(own, rows, gain, ids, experts, capacity):
    tokens = ids.shape[1]
    width = rows.shape[1]

    def kernel(*refs):
        dispatch_kernel(*refs, experts=experts, capacity=capacity)

    return pl.pallas_call(
        kernel,
        in_specs=[
            pl.BlockSpec(memory_space=pltpu.SMEM),
            pl.BlockSpec(memory_space=pltpu.HBM),
            whole(),
            whole(),
        ],
        out_specs=[whole(), whole()],
        scratch_shapes=[pltpu.VMEM((tokens, width), BF16), pltpu.SemaphoreType.DMA],
        out_shape=[
            jax.ShapeDtypeStruct((experts, capacity * width // LANES, LANES), BF16),
            jax.ShapeDtypeStruct((2, tokens), jnp.int32),
        ],
        compiler_params=pltpu.CompilerParams(vmem_limit_bytes=24 << 20),
        name="dispatch",
    )(own, pltpu.with_memory_space_constraint(rows, pltpu.HBM), gain, ids)


def expert_kernel(*refs, sources, peers, capacity, blocks):
    odd_ref, message_ref = refs[0], refs[1]
    count = (len(refs) - 6) // 2
    remote = refs[2 : count + 2]
    out_ref, rows_ref, hidden_ref = refs[count + 2 : count + 5]
    weights = refs[count + 5 : -1]
    signals = refs[-1]
    odd = odd_ref[0] == 1
    copies = [
        pltpu.make_async_copy(far, near, signals.at[i])
        for i, (far, near) in enumerate(zip(remote, weights))
    ]
    for copy in copies:
        copy.start()
    head, tail = split_rows(capacity)
    per = 8 // tail
    heads = peers * head
    for c in range(0, blocks, 2):
        both = message_ref[:, c * head : (c + 2) * head, :].astype(F32)
        for i in range(2):
            part = both[:, i * head : (i + 1) * head, :].reshape(heads, LANES)
            rows_ref[0:heads, (c + i) * LANES : (c + i + 1) * LANES] = part.astype(BF16)
    base = blocks * head
    slot = lax.broadcasted_iota(jnp.int32, (peers * tail, peers * 8), 0)
    lane = lax.broadcasted_iota(jnp.int32, (peers * tail, peers * 8), 1)
    gathers = [
        (lane == slot // tail * 8 + q * tail + slot % tail).astype(F32).astype(BF16)
        for q in range(per)
    ]
    for j in range(0, blocks // per, 2):
        both = message_ref[:, base + j * 8 : base + (j + 2) * 8, :].astype(F32)
        for i in range(2):
            part = both[:, i * 8 : (i + 1) * 8, :].reshape(peers * 8, LANES).astype(BF16)
            for q in range(per):
                c = per * (j + i) + q
                rows_ref[heads:, c * LANES : (c + 1) * LANES] = dot(gathers[q], part).astype(BF16)
    at = 0
    downs = []
    for gates, ups, down_parts, swapped in sources:
        rows = rows_ref[...]
        values = []
        for group in (gates, ups):
            value = None
            begin = 0
            for g in group:
                copies[g].wait()
                size = weights[g].shape[0]
                part = dot(rows[:, begin : begin + size], weights[g][...])
                value = part if value is None else value + part
                begin += size
            values.append(value)
        gate_value, up_value = values
        if swapped:
            gate_value, up_value = (
                jnp.where(odd, up_value, gate_value),
                jnp.where(odd, gate_value, up_value),
            )
        hidden = gate_value / (1.0 + jnp.exp(-gate_value)) * up_value
        hidden_ref[:, at : at + hidden.shape[1]] = hidden.astype(BF16)
        for d in down_parts:
            downs.append((at, d))
            at += weights[d].shape[0]
    for _, d in downs:
        copies[d].wait()
    slot = lax.broadcasted_iota(jnp.int32, (peers * 8, peers * tail), 1)
    lane = lax.broadcasted_iota(jnp.int32, (peers * 8, peers * tail), 0)
    spreads = [
        (lane == slot // tail * 8 + q * tail + slot % tail).astype(F32).astype(BF16)
        for q in range(per)
    ]
    step = 2 * per
    for first in range(0, blocks, step):
        cols = slice(first * LANES, (first + step) * LANES)
        total = None
        for begin, d in downs:
            size = weights[d].shape[0]
            part = dot(hidden_ref[:, begin : begin + size], weights[d][:, cols])
            total = part if total is None else total + part
        for c in range(0, step, 2):
            pair = [col(total, c + i)[0:heads].reshape(peers, head, LANES) for i in range(2)]
            at_row = (first + c) * head
            out_ref[:, at_row : at_row + 2 * head, :] = jnp.concatenate(pair, axis=1).astype(BF16)
        last = total[heads:].astype(BF16)
        pair = []
        for i in range(2):
            spread = None
            for q in range(per):
                part = dot(spreads[q], col(last, per * i + q))
                spread = part if spread is None else spread + part
            pair.append(spread.reshape(peers, 8, LANES))
        at_row = base + first // per * 8
        out_ref[:, at_row : at_row + 16, :] = jnp.concatenate(pair, axis=1).astype(BF16)


def experts_apply(odd, message, weights, sources, capacity):
    peers, lines, _ = message.shape
    blocks = lines // capacity
    units = sum(weights[d].shape[0] for s in sources for d in s[2])

    def kernel(*refs):
        expert_kernel(*refs, sources=sources, peers=peers, capacity=capacity, blocks=blocks)

    return pl.pallas_call(
        kernel,
        in_specs=[pl.BlockSpec(memory_space=pltpu.SMEM), whole()]
        + [pl.BlockSpec(memory_space=pltpu.HBM)] * len(weights),
        out_specs=whole(),
        out_shape=jax.ShapeDtypeStruct(message.shape, BF16),
        scratch_shapes=[
            pltpu.VMEM((peers * capacity, blocks * LANES), BF16),
            pltpu.VMEM((peers * capacity, units), BF16),
            *(pltpu.VMEM(w.shape, BF16) for w in weights),
            pltpu.SemaphoreType.DMA((len(weights),)),
        ],
        compiler_params=pltpu.CompilerParams(vmem_limit_bytes=40 << 20),
        name="experts",
    )(odd, message, *(pltpu.with_memory_space_constraint(w, pltpu.HBM) for w in weights))


def combine_kernel(message_ref, target_ref, weight_ref, gain_ref, out_ref, mixed_ref, *, capacity):
    peers = message_ref.shape[0]
    tokens, width = out_ref.shape
    blocks = width // LANES
    head, tail = split_rows(capacity)
    per = 8 // tail
    heads = peers * head
    target = target_ref[...]
    peer = target // capacity
    place = target - peer * capacity
    in_head = jnp.where(place < head, peer * head + place, -64)
    in_tail = jnp.where(place < head, -64, peer * 8 + place - head)
    pick = [selection(in_head[:, k : k + 1], 0, heads, 1).astype(F32) for k in range(2)]
    pick = jnp.concatenate(pick, axis=0).astype(BF16)
    picks = []
    for q in range(per):
        both = [selection(in_tail[:, k : k + 1], -q * tail, peers * 8, 1).astype(F32) for k in range(2)]
        picks.append(jnp.concatenate(both, axis=0).astype(BF16))
    weight = [weight_ref[:, k : k + 1] for k in range(2)]
    base = blocks * head
    square = jnp.zeros((tokens, LANES), F32)
    for c in range(0, blocks, 2):
        both = message_ref[:, c * head : (c + 2) * head, :].astype(F32)
        for i in range(2):
            part = both[:, i * head : (i + 1) * head, :].reshape(heads, LANES).astype(BF16)
            j = (c + i) // per
            rest = message_ref[:, base + j // 2 * 16 : base + j // 2 * 16 + 16, :].astype(F32)
            rest = rest[:, j % 2 * 8 : j % 2 * 8 + 8, :].reshape(peers * 8, LANES).astype(BF16)
            rows = dot(pick, part) + dot(picks[(c + i) % per], rest)
            mixed = rows[:tokens] * weight[0] + rows[tokens:] * weight[1]
            mixed_ref[:, (c + i) * LANES : (c + i + 1) * LANES] = mixed
            square = square + mixed * mixed
    scale = lax.rsqrt(jnp.sum(square, axis=1, keepdims=True) * (1.0 / width) + EPSILON)
    out_ref[...] = (mixed_ref[...] * scale * gain_ref[...]).astype(BF16)


def combine(message, target, weight, gain, capacity):
    tokens = target.shape[0]
    width = gain.shape[1]

    def kernel(*refs):
        combine_kernel(*refs, capacity=capacity)

    return pl.pallas_call(
        kernel,
        in_specs=[whole()] * 4,
        out_specs=whole(),
        out_shape=jax.ShapeDtypeStruct((tokens, width), BF16),
        scratch_shapes=[pltpu.VMEM((tokens, width), F32)],
        compiler_params=pltpu.CompilerParams(vmem_limit_bytes=24 << 20),
        name="combine",
    )(message, target, weight, gain)


def conv_kernel(rows_ref, carried_ref, taps_ref, gain_ref, weight_ref, out_ref, line_ref, sum_ref):
    block, width = rows_ref.shape
    blocks = width // LANES
    reach = taps_ref.shape[0] - 1
    halo = line_ref.shape[1] - block
    step = pl.program_id(0)

    @pl.when(step == 0)
    def _():
        for c in range(blocks):
            line_ref[c, 0:halo, :] = col(carried_ref, c).astype(F32)

    @pl.when(step > 0)
    def _():
        for c in range(blocks):
            line_ref[c, 0:halo, :] = line_ref[c, block : block + halo, :]

    for c in range(blocks):
        line_ref[c, halo:, :] = col(rows_ref, c).astype(F32)

    strip = 64

    def column(c, square):
        parts = []
        for first in range(0, block, strip):
            total = jnp.zeros((strip, LANES), F32)
            for k in range(reach + 1):
                at = first + halo - reach + k
                total = total + line_ref[c, at : at + strip, :] * taps_ref[k, pl.ds(c, 1), :]
            sum_ref[c, first : first + strip, :] = total
            parts.append(total * total)
        return square + jnp.concatenate(parts, axis=0)

    square = lax.fori_loop(0, blocks, column, jnp.zeros((block, LANES), F32))
    scale = lax.rsqrt(jnp.sum(square, axis=1, keepdims=True) * (1.0 / width) + EPSILON)
    result = jnp.zeros((block, out_ref.shape[1]), F32)
    for c in range(0, blocks, 4):
        group = []
        for i in range(4):
            value = sum_ref[c + i] * scale * col(gain_ref, c + i)
            group.append((value / (1.0 + jnp.exp(-value))).astype(BF16))
        part = jnp.concatenate(group, axis=1)
        result = result + dot(part, weight_ref[c * LANES : (c + 4) * LANES, :])
    out_ref[...] = result.astype(BF16)


def conv_module(rows, carried, taps, gain, weight, block=128):
    count, width = rows.shape
    blocks = width // LANES
    halo = carried.shape[0]
    return pl.pallas_call(
        conv_kernel,
        grid=(count // block,),
        in_specs=[
            pl.BlockSpec((block, width), lambda i: (i, 0)),
            pl.BlockSpec((halo, width), lambda i: (0, 0)),
            pl.BlockSpec((taps.shape[0], blocks, LANES), lambda i: (0, 0, 0)),
            pl.BlockSpec((1, width), lambda i: (0, 0)),
            pl.BlockSpec(weight.shape, lambda i: (0, 0)),
        ],
        out_specs=pl.BlockSpec((block, weight.shape[1]), lambda i: (i, 0)),
        out_shape=jax.ShapeDtypeStruct((count, weight.shape[1]), BF16),
        scratch_shapes=[
            pltpu.VMEM((blocks, block + halo, LANES), F32),
            pltpu.VMEM((blocks, block, LANES), F32),
        ],
        compiler_params=pltpu.CompilerParams(vmem_limit_bytes=24 << 20),
        name="conv",
    )(rows, carried, taps.reshape(taps.shape[0], blocks, LANES), gain, weight)


EP = "ep"
GRP_EP = ("grp", "ep")
GRP_EP_TP = ("grp", "ep", "tp")
HALO = 32


def run(
    conv_input,
    conv_taps,
    conv_gain,
    conv_weight,
    moe_input,
    moe_gain,
    expert_ids,
    route_weights,
    gate_weight,
    up_weight,
    down_weight,
    post_gain,
):
    quarters = lax.axis_size("tp")
    ep_count = lax.axis_size(EP)
    width = moe_input.shape[1]
    tokens = moe_input.shape[0] // quarters
    capacity = 2 * tokens // ep_count
    own = lax.axis_index("tp").astype(jnp.int32)

    odd = (lax.axis_index("grp") % 2).astype(jnp.int32)

    right = [(i, (i + 1) % quarters) for i in range(quarters)]
    left = [(i, (i - 1) % quarters) for i in range(quarters)]
    across = [(i, i ^ 1) for i in range(lax.axis_size("grp"))]
    gate, up, down = gate_weight[0], up_weight[0], down_weight[0]
    rows, units = gate.shape[0] // 2, down.shape[0] // 2
    down_a, down_b = down[:units], down[units:]
    mine_a = jnp.where(odd == 1, up[:rows], gate[:rows])
    mine_b = jnp.where(odd == 1, up[rows:], gate[rows:])

    def send(array, pairs):
        return lax.ppermute(array, "tp", pairs)

    def swap(array):
        return lax.ppermute(array, "grp", across)

    mine_a_r, mine_b_l = send(mine_a, right), send(mine_b, left)
    own_ids = lax.dynamic_slice_in_dim(expert_ids, own * tokens, tokens, 0).T
    message, target = dispatch(
        own.reshape(1), moe_input, moe_gain.reshape(1, width), own_ids, ep_count, capacity
    )
    arrived = lax.all_to_all(message, EP, 0, 0, tiled=True)
    pairs = [(i, i + 1) for i in range(ep_count - 1)]
    carried = lax.ppermute(conv_input[conv_input.shape[0] - HALO :], EP, pairs)
    mine_b_r, mine_a_l = send(mine_b, right), send(mine_a, left)
    mine_a_far, mine_b_far = send(mine_a_r, right), send(mine_b_l, left)
    other_a_r, other_b_l = swap(mine_a_r), swap(mine_b_l)
    down_a_r, down_b_l = send(down_a, right), send(down_b, left)
    other_b_r, other_a_l = swap(mine_b_r), swap(mine_a_l)
    down_b_r, down_a_l = send(down_b, right), send(down_a, left)
    other_a_far, other_b_far = swap(mine_a_far), swap(mine_b_far)
    down_a_far, down_b_far = send(down_a_r, right), send(down_b_l, left)

    conv_out = conv_module(conv_input, carried, conv_taps, conv_gain.reshape(1, width), conv_weight)

    weights = [gate, up, down]
    sources = [((0,), (1,), (2,), False)]
    for arrays in (
        (mine_a_r, mine_b_r, other_a_r, other_b_r, down_a_r, down_b_r),
        (mine_a_l, mine_b_l, other_a_l, other_b_l, down_a_l, down_b_l),
        (mine_a_far, mine_b_far, other_a_far, other_b_far, down_a_far, down_b_far),
    ):
        at = len(weights)
        weights.extend(arrays)
        sources.append(((at, at + 1), (at + 2, at + 3), (at + 4, at + 5), True))
    results = experts_apply(odd.reshape(1), arrived, weights, tuple(sources), capacity)
    returned = lax.all_to_all(results, EP, 0, 0, tiled=True)
    own_weights = lax.dynamic_slice_in_dim(route_weights, own * tokens, tokens, 0)
    moe_out = combine(returned, target.T, own_weights, post_gain.reshape(1, width), capacity)
    return (conv_out, moe_out)


def solution(mesh):
    return jax.shard_map(
        run,
        mesh=mesh,
        in_specs=(
            P(GRP_EP, None),
            P(),
            P(),
            P(None, "tp"),
            P(GRP_EP, None),
            P(),
            P(GRP_EP, None),
            P(GRP_EP, None),
            P(EP, None, "tp"),
            P(EP, None, "tp"),
            P(EP, "tp", None),
            P(),
        ),
        out_specs=(P(GRP_EP, "tp"), P(GRP_EP_TP, None)),
        check_vma=False,
    )
```

```python
import jax
import jax.numpy as jnp
from jax import lax
from jax.experimental import pallas as pl
from jax.experimental.pallas import tpu as pltpu
from jax.sharding import PartitionSpec as P

EPSILON = 1e-06
LANES = 128
F32 = jnp.float32
BF16 = jnp.bfloat16


def whole():
    return pl.BlockSpec(memory_space=pltpu.VMEM)


def dot(a, b):
    return jnp.dot(a, b, preferred_element_type=F32)


def split_rows(capacity):
    main = capacity // 8 * 8
    return main, capacity - main


def col(ref_or_value, c):
    return ref_or_value[:, c * LANES : (c + 1) * LANES]


def selection(index, first, count, dim):
    shape = (count, index.shape[1]) if dim == 0 else (index.shape[0], count)
    return index == first + lax.broadcasted_iota(jnp.int32, shape, dim)


def put_message(out_ref, head_of, tail_of, peers, head, tail, blocks):
    for c in range(0, blocks, 2):
        pair = [head_of(c + i).reshape(peers, head, LANES) for i in range(2)]
        out_ref[:, c * head : (c + 2) * head, :] = jnp.concatenate(pair, axis=1).astype(BF16)
    per = 8 // tail
    base = blocks * head
    for j in range(0, blocks // per, 2):
        pair = [tail_of(j + i).reshape(peers, 8, LANES) for i in range(2)]
        out_ref[:, base + j * 8 : base + (j + 2) * 8, :] = jnp.concatenate(pair, axis=1).astype(BF16)


def dispatch_kernel(
    own_ref, all_ref, gain_ref, ids_ref, out_ref, target_ref, rows_ref, signal, *, experts, capacity
):
    tokens, width = rows_ref.shape
    copy = pltpu.make_async_copy(
        all_ref.at[pl.ds(pl.multiple_of(own_ref[0] * tokens, 16), tokens), :], rows_ref, signal
    )
    copy.start()
    blocks = width // LANES
    head, tail = split_rows(capacity)
    per = 8 // tail
    ids = ids_ref[...]
    onehot = [
        (ids[k : k + 1, :] == lax.broadcasted_iota(jnp.int32, (experts, tokens), 0)).astype(F32)
        for k in range(2)
    ]
    before = lax.broadcasted_iota(jnp.int32, (tokens, tokens), 0) < lax.broadcasted_iota(
        jnp.int32, (tokens, tokens), 1
    )
    before = before.astype(F32).astype(BF16)
    counts = [dot(h.astype(BF16), before) for h in onehot]
    counts[1] = counts[1] + jnp.sum(onehot[0], axis=1, keepdims=True)
    place = [jnp.sum(c * h, axis=0, keepdims=True).astype(jnp.int32) for c, h in zip(counts, onehot)]
    place = jnp.concatenate(place, axis=0)
    target_ref[...] = ids * capacity + place
    in_head = jnp.where(place < head, ids * head + place, -64)
    in_tail = jnp.where(place < head, -64, ids * 8 + place - head)
    pick = jnp.zeros((experts * head, tokens), F32)
    picks = [jnp.zeros((experts * 8, tokens), F32) for _ in range(per)]
    for k in range(2):
        pick = pick + selection(in_head[k : k + 1], 0, experts * head, 0).astype(F32)
        for q in range(per):
            picks[q] = picks[q] + selection(in_tail[k : k + 1], -q * tail, experts * 8, 0).astype(F32)
    pick = pick.astype(BF16)
    picks = jnp.concatenate(picks, axis=1).astype(BF16)
    copy.wait()
    rows = rows_ref[...].astype(F32)
    mean_square = jnp.mean(rows * rows, axis=-1, keepdims=True)
    normed = (rows * lax.rsqrt(mean_square + EPSILON) * gain_ref[...]).astype(BF16)

    def tail_of(j):
        stack = [col(normed, per * j + q) for q in range(per)]
        return dot(picks, jnp.concatenate(stack, axis=0))

    put_message(
        out_ref, lambda c: dot(pick, col(normed, c)), tail_of, experts, head, tail, blocks
    )


def dispatch(own, rows, gain, ids, experts, capacity):
    tokens = ids.shape[1]
    width = rows.shape[1]

    def kernel(*refs):
        dispatch_kernel(*refs, experts=experts, capacity=capacity)

    return pl.pallas_call(
        kernel,
        in_specs=[
            pl.BlockSpec(memory_space=pltpu.SMEM),
            pl.BlockSpec(memory_space=pltpu.HBM),
            whole(),
            whole(),
        ],
        out_specs=[whole(), whole()],
        scratch_shapes=[pltpu.VMEM((tokens, width), BF16), pltpu.SemaphoreType.DMA],
        out_shape=[
            jax.ShapeDtypeStruct((experts, capacity * width // LANES, LANES), BF16),
            jax.ShapeDtypeStruct((2, tokens), jnp.int32),
        ],
        compiler_params=pltpu.CompilerParams(vmem_limit_bytes=24 << 20),
        name="dispatch",
    )(own, pltpu.with_memory_space_constraint(rows, pltpu.HBM), gain, ids)


def expert_kernel(*refs, sources, peers, capacity, blocks):
    odd_ref, message_ref = refs[0], refs[1]
    count = (len(refs) - 6) // 2
    remote = refs[2 : count + 2]
    out_ref, rows_ref, hidden_ref = refs[count + 2 : count + 5]
    weights = refs[count + 5 : -1]
    signals = refs[-1]
    odd = odd_ref[0] == 1
    copies = [
        pltpu.make_async_copy(far, near, signals.at[i])
        for i, (far, near) in enumerate(zip(remote, weights))
    ]
    for copy in copies:
        copy.start()
    head, tail = split_rows(capacity)
    per = 8 // tail
    heads = peers * head
    for c in range(0, blocks, 2):
        both = message_ref[:, c * head : (c + 2) * head, :].astype(F32)
        for i in range(2):
            part = both[:, i * head : (i + 1) * head, :].reshape(heads, LANES)
            rows_ref[0:heads, (c + i) * LANES : (c + i + 1) * LANES] = part.astype(BF16)
    base = blocks * head
    slot = lax.broadcasted_iota(jnp.int32, (peers * tail, peers * 8), 0)
    lane = lax.broadcasted_iota(jnp.int32, (peers * tail, peers * 8), 1)
    gathers = [
        (lane == slot // tail * 8 + q * tail + slot % tail).astype(F32).astype(BF16)
        for q in range(per)
    ]
    for j in range(0, blocks // per, 2):
        both = message_ref[:, base + j * 8 : base + (j + 2) * 8, :].astype(F32)
        for i in range(2):
            part = both[:, i * 8 : (i + 1) * 8, :].reshape(peers * 8, LANES).astype(BF16)
            for q in range(per):
                c = per * (j + i) + q
                rows_ref[heads:, c * LANES : (c + 1) * LANES] = dot(gathers[q], part).astype(BF16)
    at = 0
    downs = []
    for gates, ups, down_parts, swapped in sources:
        rows = rows_ref[...]
        values = []
        for group in (gates, ups):
            value = None
            begin = 0
            for g in group:
                copies[g].wait()
                size = weights[g].shape[0]
                part = dot(rows[:, begin : begin + size], weights[g][...])
                value = part if value is None else value + part
                begin += size
            values.append(value)
        gate_value, up_value = values
        if swapped:
            gate_value, up_value = (
                jnp.where(odd, up_value, gate_value),
                jnp.where(odd, gate_value, up_value),
            )
        hidden = gate_value / (1.0 + jnp.exp(-gate_value)) * up_value
        hidden_ref[:, at : at + hidden.shape[1]] = hidden.astype(BF16)
        for d in down_parts:
            downs.append((at, d))
            at += weights[d].shape[0]
    for _, d in downs:
        copies[d].wait()
    slot = lax.broadcasted_iota(jnp.int32, (peers * 8, peers * tail), 1)
    lane = lax.broadcasted_iota(jnp.int32, (peers * 8, peers * tail), 0)
    spreads = [
        (lane == slot // tail * 8 + q * tail + slot % tail).astype(F32).astype(BF16)
        for q in range(per)
    ]
    step = 2 * per
    for first in range(0, blocks, step):
        cols = slice(first * LANES, (first + step) * LANES)
        total = None
        for begin, d in downs:
            size = weights[d].shape[0]
            part = dot(hidden_ref[:, begin : begin + size], weights[d][:, cols])
            total = part if total is None else total + part
        for c in range(0, step, 2):
            pair = [col(total, c + i)[0:heads].reshape(peers, head, LANES) for i in range(2)]
            at_row = (first + c) * head
            out_ref[:, at_row : at_row + 2 * head, :] = jnp.concatenate(pair, axis=1).astype(BF16)
        last = total[heads:].astype(BF16)
        pair = []
        for i in range(2):
            spread = None
            for q in range(per):
                part = dot(spreads[q], col(last, per * i + q))
                spread = part if spread is None else spread + part
            pair.append(spread.reshape(peers, 8, LANES))
        at_row = base + first // per * 8
        out_ref[:, at_row : at_row + 16, :] = jnp.concatenate(pair, axis=1).astype(BF16)


def experts_apply(odd, message, weights, sources, capacity):
    peers, lines, _ = message.shape
    blocks = lines // capacity
    units = sum(weights[d].shape[0] for s in sources for d in s[2])

    def kernel(*refs):
        expert_kernel(*refs, sources=sources, peers=peers, capacity=capacity, blocks=blocks)

    return pl.pallas_call(
        kernel,
        in_specs=[pl.BlockSpec(memory_space=pltpu.SMEM), whole()]
        + [pl.BlockSpec(memory_space=pltpu.HBM)] * len(weights),
        out_specs=whole(),
        out_shape=jax.ShapeDtypeStruct(message.shape, BF16),
        scratch_shapes=[
            pltpu.VMEM((peers * capacity, blocks * LANES), BF16),
            pltpu.VMEM((peers * capacity, units), BF16),
            *(pltpu.VMEM(w.shape, BF16) for w in weights),
            pltpu.SemaphoreType.DMA((len(weights),)),
        ],
        compiler_params=pltpu.CompilerParams(vmem_limit_bytes=40 << 20),
        name="experts",
    )(odd, message, *(pltpu.with_memory_space_constraint(w, pltpu.HBM) for w in weights))


def combine_kernel(
    message_ref, target_ref, far_ref, gain_ref, out_ref, mixed_ref, weight_ref, signal, *, capacity
):
    copy = pltpu.make_async_copy(far_ref, weight_ref, signal)
    copy.start()
    peers = message_ref.shape[0]
    tokens, width = out_ref.shape
    blocks = width // LANES
    head, tail = split_rows(capacity)
    per = 8 // tail
    heads = peers * head
    target = target_ref[...]
    peer = target // capacity
    place = target - peer * capacity
    in_head = jnp.where(place < head, peer * head + place, -64)
    in_tail = jnp.where(place < head, -64, peer * 8 + place - head)
    pick = [selection(in_head[:, k : k + 1], 0, heads, 1).astype(F32) for k in range(2)]
    pick = jnp.concatenate(pick, axis=0).astype(BF16)
    picks = []
    for q in range(per):
        both = [selection(in_tail[:, k : k + 1], -q * tail, peers * 8, 1).astype(F32) for k in range(2)]
        picks.append(jnp.concatenate(both, axis=0).astype(BF16))
    copy.wait()
    weight = [weight_ref[:, k : k + 1] for k in range(2)]
    base = blocks * head
    square = jnp.zeros((tokens, LANES), F32)
    for c in range(0, blocks, 2):
        both = message_ref[:, c * head : (c + 2) * head, :].astype(F32)
        for i in range(2):
            part = both[:, i * head : (i + 1) * head, :].reshape(heads, LANES).astype(BF16)
            j = (c + i) // per
            rest = message_ref[:, base + j // 2 * 16 : base + j // 2 * 16 + 16, :].astype(F32)
            rest = rest[:, j % 2 * 8 : j % 2 * 8 + 8, :].reshape(peers * 8, LANES).astype(BF16)
            rows = dot(pick, part) + dot(picks[(c + i) % per], rest)
            mixed = rows[:tokens] * weight[0] + rows[tokens:] * weight[1]
            mixed_ref[:, (c + i) * LANES : (c + i + 1) * LANES] = mixed
            square = square + mixed * mixed
    scale = lax.rsqrt(jnp.sum(square, axis=1, keepdims=True) * (1.0 / width) + EPSILON)
    out_ref[...] = (mixed_ref[...] * scale * gain_ref[...]).astype(BF16)


def combine(message, target, weight, gain, capacity):
    tokens = target.shape[0]
    width = gain.shape[1]

    def kernel(*refs):
        combine_kernel(*refs, capacity=capacity)

    return pl.pallas_call(
        kernel,
        in_specs=[whole(), whole(), pl.BlockSpec(memory_space=pltpu.HBM), whole()],
        out_specs=whole(),
        out_shape=jax.ShapeDtypeStruct((tokens, width), BF16),
        scratch_shapes=[
            pltpu.VMEM((tokens, width), F32),
            pltpu.VMEM(weight.shape, F32),
            pltpu.SemaphoreType.DMA,
        ],
        compiler_params=pltpu.CompilerParams(vmem_limit_bytes=24 << 20),
        name="combine",
    )(message, target, pltpu.with_memory_space_constraint(weight, pltpu.HBM), gain)


def conv_kernel(rows_ref, carried_ref, taps_ref, gain_ref, weight_ref, out_ref, line_ref, sum_ref):
    block, width = rows_ref.shape
    blocks = width // LANES
    reach = taps_ref.shape[0] - 1
    halo = line_ref.shape[1] - block
    step = pl.program_id(0)

    @pl.when(step == 0)
    def _():
        for c in range(blocks):
            line_ref[c, 0:halo, :] = col(carried_ref, c).astype(F32)

    @pl.when(step > 0)
    def _():
        for c in range(blocks):
            line_ref[c, 0:halo, :] = line_ref[c, block : block + halo, :]

    for c in range(blocks):
        line_ref[c, halo:, :] = col(rows_ref, c).astype(F32)

    strip = 64

    def column(c, square):
        parts = []
        for first in range(0, block, strip):
            total = jnp.zeros((strip, LANES), F32)
            for k in range(reach + 1):
                at = first + halo - reach + k
                total = total + line_ref[c, at : at + strip, :] * taps_ref[k, pl.ds(c, 1), :]
            sum_ref[c, first : first + strip, :] = total
            parts.append(total * total)
        return square + jnp.concatenate(parts, axis=0)

    square = lax.fori_loop(0, blocks, column, jnp.zeros((block, LANES), F32))
    scale = lax.rsqrt(jnp.sum(square, axis=1, keepdims=True) * (1.0 / width) + EPSILON)
    result = jnp.zeros((block, out_ref.shape[1]), F32)
    for c in range(0, blocks, 4):
        group = []
        for i in range(4):
            value = sum_ref[c + i] * scale * col(gain_ref, c + i)
            group.append((value / (1.0 + jnp.exp(-value))).astype(BF16))
        part = jnp.concatenate(group, axis=1)
        result = result + dot(part, weight_ref[c * LANES : (c + 4) * LANES, :])
    out_ref[...] = result.astype(BF16)


def conv_module(rows, carried, taps, gain, weight, block=128):
    count, width = rows.shape
    blocks = width // LANES
    halo = carried.shape[0]
    return pl.pallas_call(
        conv_kernel,
        grid=(count // block,),
        in_specs=[
            pl.BlockSpec((block, width), lambda i: (i, 0)),
            pl.BlockSpec((halo, width), lambda i: (0, 0)),
            pl.BlockSpec((taps.shape[0], blocks, LANES), lambda i: (0, 0, 0)),
            pl.BlockSpec((1, width), lambda i: (0, 0)),
            pl.BlockSpec(weight.shape, lambda i: (0, 0)),
        ],
        out_specs=pl.BlockSpec((block, weight.shape[1]), lambda i: (i, 0)),
        out_shape=jax.ShapeDtypeStruct((count, weight.shape[1]), BF16),
        scratch_shapes=[
            pltpu.VMEM((blocks, block + halo, LANES), F32),
            pltpu.VMEM((blocks, block, LANES), F32),
        ],
        compiler_params=pltpu.CompilerParams(vmem_limit_bytes=24 << 20),
        name="conv",
    )(rows, carried, taps.reshape(taps.shape[0], blocks, LANES), gain, weight)


EP = "ep"
GRP_EP = ("grp", "ep")
GRP_EP_TP = ("grp", "ep", "tp")
HALO = 32


def run(
    conv_input,
    conv_taps,
    conv_gain,
    conv_weight,
    moe_input,
    moe_gain,
    expert_ids,
    route_weights,
    gate_weight,
    up_weight,
    down_weight,
    post_gain,
):
    quarters = lax.axis_size("tp")
    ep_count = lax.axis_size(EP)
    width = moe_input.shape[1]
    tokens = moe_input.shape[0] // quarters
    capacity = 2 * tokens // ep_count
    own = lax.axis_index("tp").astype(jnp.int32)

    odd = (lax.axis_index("grp") % 2).astype(jnp.int32)

    right = [(i, (i + 1) % quarters) for i in range(quarters)]
    left = [(i, (i - 1) % quarters) for i in range(quarters)]
    across = [(i, i ^ 1) for i in range(lax.axis_size("grp"))]
    gate, up, down = gate_weight[0], up_weight[0], down_weight[0]
    rows, units = gate.shape[0] // 2, down.shape[0] // 2

    def send(array, pairs):
        return lax.ppermute(array, "tp", pairs)

    def swap(array):
        return lax.ppermute(array, "grp", across)

    down_r, down_l = send(down, right), send(down, left)
    own_ids = lax.dynamic_slice_in_dim(expert_ids, own * tokens, tokens, 0).T
    message, target = dispatch(
        own.reshape(1), moe_input, moe_gain.reshape(1, width), own_ids, ep_count, capacity
    )
    arrived = lax.all_to_all(message, EP, 0, 0, tiled=True)
    mine_a = jnp.where(odd == 1, up[:rows], gate[:rows])
    mine_b = jnp.where(odd == 1, up[rows:], gate[rows:])
    mine_a_r, mine_b_l = send(mine_a, right), send(mine_b, left)
    mine_b_r, mine_a_l = send(mine_b, right), send(mine_a, left)
    pairs = [(i, i + 1) for i in range(ep_count - 1)]
    carried = lax.ppermute(conv_input[conv_input.shape[0] - HALO :], EP, pairs)
    down_a_far, down_b_far = send(down_r[:units], right), send(down_l[units:], left)
    other_a_r, other_b_l = swap(mine_a_r), swap(mine_b_l)
    mine_a_far, mine_b_far = send(mine_a_r, right), send(mine_b_l, left)
    other_b_r, other_a_l = swap(mine_b_r), swap(mine_a_l)
    other_a_far, other_b_far = send(other_a_r, right), send(other_b_l, left)

    conv_out = conv_module(conv_input, carried, conv_taps, conv_gain.reshape(1, width), conv_weight)

    weights = [gate, up, down]
    sources = [((0,), (1,), (2,), False)]
    for arrays in (
        (mine_a_r, mine_b_r, other_a_r, other_b_r, down_r),
        (mine_a_l, mine_b_l, other_a_l, other_b_l, down_l),
        (mine_a_far, mine_b_far, other_a_far, other_b_far, down_a_far, down_b_far),
    ):
        at = len(weights)
        weights.extend(arrays)
        parts = tuple(range(at + 4, len(weights)))
        sources.append(((at, at + 1), (at + 2, at + 3), parts, True))
    results = experts_apply(odd.reshape(1), arrived, weights, tuple(sources), capacity)
    returned = lax.all_to_all(results, EP, 0, 0, tiled=True)
    own_weights = lax.dynamic_slice_in_dim(route_weights, own * tokens, tokens, 0)
    moe_out = combine(returned, target.T, own_weights, post_gain.reshape(1, width), capacity)
    return (conv_out, moe_out)


def solution(mesh):
    return jax.shard_map(
        run,
        mesh=mesh,
        in_specs=(
            P(GRP_EP, None),
            P(),
            P(),
            P(None, "tp"),
            P(GRP_EP, None),
            P(),
            P(GRP_EP, None),
            P(GRP_EP, None),
            P(EP, None, "tp"),
            P(EP, None, "tp"),
            P(EP, "tp", None),
            P(),
        ),
        out_specs=(P(GRP_EP, "tp"), P(GRP_EP_TP, None)),
        check_vma=False,
    )
```

```python
import jax
import jax.numpy as jnp
from jax import lax
from jax.experimental import pallas as pl
from jax.experimental.pallas import tpu as pltpu
from jax.sharding import PartitionSpec as P

EPSILON = 1e-06
LANES = 128
F32 = jnp.float32
BF16 = jnp.bfloat16


def whole():
    return pl.BlockSpec(memory_space=pltpu.VMEM)


def dot(a, b):
    return jnp.dot(a, b, preferred_element_type=F32)


def split_rows(capacity):
    main = capacity // 8 * 8
    return main, capacity - main


def col(ref_or_value, c):
    return ref_or_value[:, c * LANES : (c + 1) * LANES]


def selection(index, first, count, dim):
    shape = (count, index.shape[1]) if dim == 0 else (index.shape[0], count)
    return index == first + lax.broadcasted_iota(jnp.int32, shape, dim)


def put_message(out_ref, head_of, tail_of, peers, head, tail, blocks):
    for c in range(0, blocks, 2):
        pair = [head_of(c + i).reshape(peers, head, LANES) for i in range(2)]
        out_ref[:, c * head : (c + 2) * head, :] = jnp.concatenate(pair, axis=1).astype(BF16)
    per = 8 // tail
    base = blocks * head
    for j in range(0, blocks // per, 2):
        pair = [tail_of(j + i).reshape(peers, 8, LANES) for i in range(2)]
        out_ref[:, base + j * 8 : base + (j + 2) * 8, :] = jnp.concatenate(pair, axis=1).astype(BF16)


def dispatch_kernel(
    own_ref, all_ref, gain_ref, ids_ref, out_ref, target_ref, rows_ref, signal, *, experts, capacity
):
    tokens, width = rows_ref.shape
    copy = pltpu.make_async_copy(
        all_ref.at[pl.ds(pl.multiple_of(own_ref[0] * tokens, 16), tokens), :], rows_ref, signal
    )
    copy.start()
    blocks = width // LANES
    head, tail = split_rows(capacity)
    per = 8 // tail
    ids = ids_ref[...]
    onehot = [
        (ids[k : k + 1, :] == lax.broadcasted_iota(jnp.int32, (experts, tokens), 0)).astype(F32)
        for k in range(2)
    ]
    before = lax.broadcasted_iota(jnp.int32, (tokens, tokens), 0) < lax.broadcasted_iota(
        jnp.int32, (tokens, tokens), 1
    )
    before = before.astype(F32).astype(BF16)
    counts = [dot(h.astype(BF16), before) for h in onehot]
    counts[1] = counts[1] + jnp.sum(onehot[0], axis=1, keepdims=True)
    place = [jnp.sum(c * h, axis=0, keepdims=True).astype(jnp.int32) for c, h in zip(counts, onehot)]
    place = jnp.concatenate(place, axis=0)
    target_ref[...] = ids * capacity + place
    in_head = jnp.where(place < head, ids * head + place, -64)
    in_tail = jnp.where(place < head, -64, ids * 8 + place - head)
    pick = jnp.zeros((experts * head, tokens), F32)
    picks = [jnp.zeros((experts * 8, tokens), F32) for _ in range(per)]
    for k in range(2):
        pick = pick + selection(in_head[k : k + 1], 0, experts * head, 0).astype(F32)
        for q in range(per):
            picks[q] = picks[q] + selection(in_tail[k : k + 1], -q * tail, experts * 8, 0).astype(F32)
    pick = pick.astype(BF16)
    picks = jnp.concatenate(picks, axis=1).astype(BF16)
    copy.wait()
    rows = rows_ref[...].astype(F32)
    mean_square = jnp.mean(rows * rows, axis=-1, keepdims=True)
    normed = (rows * lax.rsqrt(mean_square + EPSILON) * gain_ref[...]).astype(BF16)

    def tail_of(j):
        stack = [col(normed, per * j + q) for q in range(per)]
        return dot(picks, jnp.concatenate(stack, axis=0))

    put_message(
        out_ref, lambda c: dot(pick, col(normed, c)), tail_of, experts, head, tail, blocks
    )


def dispatch(own, rows, gain, ids, experts, capacity):
    tokens = ids.shape[1]
    width = rows.shape[1]

    def kernel(*refs):
        dispatch_kernel(*refs, experts=experts, capacity=capacity)

    return pl.pallas_call(
        kernel,
        in_specs=[
            pl.BlockSpec(memory_space=pltpu.SMEM),
            pl.BlockSpec(memory_space=pltpu.HBM),
            whole(),
            whole(),
        ],
        out_specs=[whole(), whole()],
        scratch_shapes=[pltpu.VMEM((tokens, width), BF16), pltpu.SemaphoreType.DMA],
        out_shape=[
            jax.ShapeDtypeStruct((experts, capacity * width // LANES, LANES), BF16),
            jax.ShapeDtypeStruct((2, tokens), jnp.int32),
        ],
        compiler_params=pltpu.CompilerParams(vmem_limit_bytes=24 << 20),
        name="dispatch",
    )(own, pltpu.with_memory_space_constraint(rows, pltpu.HBM), gain, ids)


def expert_kernel(*refs, sources, far, peers, capacity, blocks):
    odd_ref, message_ref = refs[0], refs[1]
    given = refs[2 : len(far) + 2]
    out_ref, rows_ref, hidden_ref = refs[len(far) + 2 : len(far) + 5]
    near, signals = list(refs[len(far) + 5 : -1]), refs[-1]
    odd = odd_ref[0] == 1
    weights, copies = [], []
    for ref, moved in zip(given, far):
        weights.append(near.pop(0) if moved else ref)
        copies.append(pltpu.make_async_copy(ref, weights[-1], signals.at[len(copies)]) if moved else None)
    waves = [[*s[0], *s[1]] for s in sources] + [[d for s in sources for d in s[2]]]

    def issue(wave):
        for w in wave:
            if copies[w] is not None:
                copies[w].start()

    def settle(wave):
        for w in wave:
            if copies[w] is not None:
                copies[w].wait()

    issue(waves[0])
    issue(waves[1])
    head, tail = split_rows(capacity)
    per = 8 // tail
    heads = peers * head
    for c in range(0, blocks, 2):
        both = message_ref[:, c * head : (c + 2) * head, :].astype(F32)
        for i in range(2):
            part = both[:, i * head : (i + 1) * head, :].reshape(heads, LANES)
            rows_ref[0:heads, (c + i) * LANES : (c + i + 1) * LANES] = part.astype(BF16)
    base = blocks * head
    slot = lax.broadcasted_iota(jnp.int32, (peers * tail, peers * 8), 0)
    lane = lax.broadcasted_iota(jnp.int32, (peers * tail, peers * 8), 1)
    gathers = [
        (lane == slot // tail * 8 + q * tail + slot % tail).astype(F32).astype(BF16)
        for q in range(per)
    ]
    for j in range(0, blocks // per, 2):
        both = message_ref[:, base + j * 8 : base + (j + 2) * 8, :].astype(F32)
        for i in range(2):
            part = both[:, i * 8 : (i + 1) * 8, :].reshape(peers * 8, LANES).astype(BF16)
            for q in range(per):
                c = per * (j + i) + q
                rows_ref[heads:, c * LANES : (c + 1) * LANES] = dot(gathers[q], part).astype(BF16)
    at = 0
    downs = []
    for n, (gates, ups, down_parts, swapped) in enumerate(sources):
        settle(waves[n])
        if n + 2 < len(waves):
            issue(waves[n + 2])
        rows = rows_ref[...]
        values = []
        for group in (gates, ups):
            value = None
            begin = 0
            for g in group:
                size = weights[g].shape[0]
                part = dot(rows[:, begin : begin + size], weights[g][...])
                value = part if value is None else value + part
                begin += size
            values.append(value)
        gate_value, up_value = values
        if swapped:
            gate_value, up_value = (
                jnp.where(odd, up_value, gate_value),
                jnp.where(odd, gate_value, up_value),
            )
        hidden = gate_value / (1.0 + jnp.exp(-gate_value)) * up_value
        hidden_ref[:, at : at + hidden.shape[1]] = hidden.astype(BF16)
        for d in down_parts:
            downs.append((at, d))
            at += weights[d].shape[0]
    settle(waves[-1])
    slot = lax.broadcasted_iota(jnp.int32, (peers * 8, peers * tail), 1)
    lane = lax.broadcasted_iota(jnp.int32, (peers * 8, peers * tail), 0)
    spreads = [
        (lane == slot // tail * 8 + q * tail + slot % tail).astype(F32).astype(BF16)
        for q in range(per)
    ]
    step = 2 * per
    for first in range(0, blocks, step):
        cols = slice(first * LANES, (first + step) * LANES)
        total = None
        for begin, d in downs:
            size = weights[d].shape[0]
            part = dot(hidden_ref[:, begin : begin + size], weights[d][:, cols])
            total = part if total is None else total + part
        for c in range(0, step, 2):
            pair = [col(total, c + i)[0:heads].reshape(peers, head, LANES) for i in range(2)]
            at_row = (first + c) * head
            out_ref[:, at_row : at_row + 2 * head, :] = jnp.concatenate(pair, axis=1).astype(BF16)
        last = total[heads:].astype(BF16)
        pair = []
        for i in range(2):
            spread = None
            for q in range(per):
                part = dot(spreads[q], col(last, per * i + q))
                spread = part if spread is None else spread + part
            pair.append(spread.reshape(peers, 8, LANES))
        at_row = base + first // per * 8
        out_ref[:, at_row : at_row + 16, :] = jnp.concatenate(pair, axis=1).astype(BF16)


def experts_apply(odd, message, weights, far, sources, capacity):
    peers, lines, _ = message.shape
    blocks = lines // capacity
    units = sum(weights[d].shape[0] for s in sources for d in s[2])

    def kernel(*refs):
        expert_kernel(*refs, sources=sources, far=far, peers=peers, capacity=capacity, blocks=blocks)

    return pl.pallas_call(
        kernel,
        in_specs=[pl.BlockSpec(memory_space=pltpu.SMEM), whole()]
        + [pl.BlockSpec(memory_space=pltpu.HBM) if f else whole() for f in far],
        out_specs=whole(),
        out_shape=jax.ShapeDtypeStruct(message.shape, BF16),
        scratch_shapes=[
            pltpu.VMEM((peers * capacity, blocks * LANES), BF16),
            pltpu.VMEM((peers * capacity, units), BF16),
            *(pltpu.VMEM(w.shape, BF16) for w, f in zip(weights, far) if f),
            pltpu.SemaphoreType.DMA((len(weights),)),
        ],
        compiler_params=pltpu.CompilerParams(vmem_limit_bytes=40 << 20),
        name="experts",
    )(
        odd,
        message,
        *(pltpu.with_memory_space_constraint(w, pltpu.HBM) if f else w for w, f in zip(weights, far)),
    )


def combine_kernel(
    message_ref, target_ref, far_ref, gain_ref, out_ref, mixed_ref, weight_ref, signal, *, capacity
):
    copy = pltpu.make_async_copy(far_ref, weight_ref, signal)
    copy.start()
    peers = message_ref.shape[0]
    tokens, width = out_ref.shape
    blocks = width // LANES
    head, tail = split_rows(capacity)
    per = 8 // tail
    heads = peers * head
    target = target_ref[...]
    peer = target // capacity
    place = target - peer * capacity
    in_head = jnp.where(place < head, peer * head + place, -64)
    in_tail = jnp.where(place < head, -64, peer * 8 + place - head)
    pick = [selection(in_head[:, k : k + 1], 0, heads, 1).astype(F32) for k in range(2)]
    pick = jnp.concatenate(pick, axis=0).astype(BF16)
    picks = []
    for q in range(per):
        both = [selection(in_tail[:, k : k + 1], -q * tail, peers * 8, 1).astype(F32) for k in range(2)]
        picks.append(jnp.concatenate(both, axis=0).astype(BF16))
    copy.wait()
    weight = [weight_ref[:, k : k + 1] for k in range(2)]
    base = blocks * head
    square = jnp.zeros((tokens, LANES), F32)
    for c in range(0, blocks, 2):
        both = message_ref[:, c * head : (c + 2) * head, :].astype(F32)
        for i in range(2):
            part = both[:, i * head : (i + 1) * head, :].reshape(heads, LANES).astype(BF16)
            j = (c + i) // per
            rest = message_ref[:, base + j // 2 * 16 : base + j // 2 * 16 + 16, :].astype(F32)
            rest = rest[:, j % 2 * 8 : j % 2 * 8 + 8, :].reshape(peers * 8, LANES).astype(BF16)
            rows = dot(pick, part) + dot(picks[(c + i) % per], rest)
            mixed = rows[:tokens] * weight[0] + rows[tokens:] * weight[1]
            mixed_ref[:, (c + i) * LANES : (c + i + 1) * LANES] = mixed
            square = square + mixed * mixed
    scale = lax.rsqrt(jnp.sum(square, axis=1, keepdims=True) * (1.0 / width) + EPSILON)
    out_ref[...] = (mixed_ref[...] * scale * gain_ref[...]).astype(BF16)


def combine(message, target, weight, gain, capacity):
    tokens = target.shape[0]
    width = gain.shape[1]

    def kernel(*refs):
        combine_kernel(*refs, capacity=capacity)

    return pl.pallas_call(
        kernel,
        in_specs=[whole(), whole(), pl.BlockSpec(memory_space=pltpu.HBM), whole()],
        out_specs=whole(),
        out_shape=jax.ShapeDtypeStruct((tokens, width), BF16),
        scratch_shapes=[
            pltpu.VMEM((tokens, width), F32),
            pltpu.VMEM(weight.shape, F32),
            pltpu.SemaphoreType.DMA,
        ],
        compiler_params=pltpu.CompilerParams(vmem_limit_bytes=24 << 20),
        name="combine",
    )(message, target, pltpu.with_memory_space_constraint(weight, pltpu.HBM), gain)


def conv_kernel(rows_ref, carried_ref, taps_ref, gain_ref, weight_ref, out_ref, line_ref, sum_ref):
    block, width = rows_ref.shape
    blocks = width // LANES
    reach = taps_ref.shape[0] - 1
    halo = line_ref.shape[1] - block
    step = pl.program_id(0)

    @pl.when(step == 0)
    def _():
        for c in range(blocks):
            line_ref[c, 0:halo, :] = col(carried_ref, c).astype(F32)

    @pl.when(step > 0)
    def _():
        for c in range(blocks):
            line_ref[c, 0:halo, :] = line_ref[c, block : block + halo, :]

    for c in range(blocks):
        line_ref[c, halo:, :] = col(rows_ref, c).astype(F32)

    strip = 64

    def column(c, square):
        parts = []
        for first in range(0, block, strip):
            total = jnp.zeros((strip, LANES), F32)
            for k in range(reach + 1):
                at = first + halo - reach + k
                total = total + line_ref[c, at : at + strip, :] * taps_ref[k, pl.ds(c, 1), :]
            sum_ref[c, first : first + strip, :] = total
            parts.append(total * total)
        return square + jnp.concatenate(parts, axis=0)

    square = lax.fori_loop(0, blocks, column, jnp.zeros((block, LANES), F32))
    scale = lax.rsqrt(jnp.sum(square, axis=1, keepdims=True) * (1.0 / width) + EPSILON)
    result = jnp.zeros((block, out_ref.shape[1]), F32)
    for c in range(0, blocks, 4):
        group = []
        for i in range(4):
            value = sum_ref[c + i] * scale * col(gain_ref, c + i)
            group.append((value / (1.0 + jnp.exp(-value))).astype(BF16))
        part = jnp.concatenate(group, axis=1)
        result = result + dot(part, weight_ref[c * LANES : (c + 4) * LANES, :])
    out_ref[...] = result.astype(BF16)


def conv_module(rows, carried, taps, gain, weight, block=128):
    count, width = rows.shape
    blocks = width // LANES
    halo = carried.shape[0]
    return pl.pallas_call(
        conv_kernel,
        grid=(count // block,),
        in_specs=[
            pl.BlockSpec((block, width), lambda i: (i, 0)),
            pl.BlockSpec((halo, width), lambda i: (0, 0)),
            pl.BlockSpec((taps.shape[0], blocks, LANES), lambda i: (0, 0, 0)),
            pl.BlockSpec((1, width), lambda i: (0, 0)),
            pl.BlockSpec(weight.shape, lambda i: (0, 0)),
        ],
        out_specs=pl.BlockSpec((block, weight.shape[1]), lambda i: (i, 0)),
        out_shape=jax.ShapeDtypeStruct((count, weight.shape[1]), BF16),
        scratch_shapes=[
            pltpu.VMEM((blocks, block + halo, LANES), F32),
            pltpu.VMEM((blocks, block, LANES), F32),
        ],
        compiler_params=pltpu.CompilerParams(vmem_limit_bytes=24 << 20),
        name="conv",
    )(rows, carried, taps.reshape(taps.shape[0], blocks, LANES), gain, weight)


EP = "ep"
GRP_EP = ("grp", "ep")
GRP_EP_TP = ("grp", "ep", "tp")
HALO = 32


def run(
    conv_input,
    conv_taps,
    conv_gain,
    conv_weight,
    moe_input,
    moe_gain,
    expert_ids,
    route_weights,
    gate_weight,
    up_weight,
    down_weight,
    post_gain,
):
    quarters = lax.axis_size("tp")
    ep_count = lax.axis_size(EP)
    width = moe_input.shape[1]
    tokens = moe_input.shape[0] // quarters
    capacity = 2 * tokens // ep_count
    own = lax.axis_index("tp").astype(jnp.int32)

    odd = (lax.axis_index("grp") % 2).astype(jnp.int32)

    right = [(i, (i + 1) % quarters) for i in range(quarters)]
    left = [(i, (i - 1) % quarters) for i in range(quarters)]
    across = [(i, i ^ 1) for i in range(lax.axis_size("grp"))]
    gate, up, down = gate_weight[0], up_weight[0], down_weight[0]
    rows, units = gate.shape[0] // 2, down.shape[0] // 2

    def send(array, pairs):
        return lax.ppermute(array, "tp", pairs)

    def swap(array):
        return lax.ppermute(array, "grp", across)

    down_r, down_l = send(down, right), send(down, left)
    own_ids = lax.dynamic_slice_in_dim(expert_ids, own * tokens, tokens, 0).T
    message, target = dispatch(
        own.reshape(1), moe_input, moe_gain.reshape(1, width), own_ids, ep_count, capacity
    )
    arrived = lax.all_to_all(message, EP, 0, 0, tiled=True)
    mine_a = jnp.where(odd == 1, up[:rows], gate[:rows])
    mine_b = jnp.where(odd == 1, up[rows:], gate[rows:])
    mine_a_r, mine_b_l = send(mine_a, right), send(mine_b, left)
    mine_b_r, mine_a_l = send(mine_b, right), send(mine_a, left)
    pairs = [(i, i + 1) for i in range(ep_count - 1)]
    carried = lax.ppermute(conv_input[conv_input.shape[0] - HALO :], EP, pairs)
    down_a_far, down_b_far = send(down_r[:units], right), send(down_l[units:], left)
    other_a_r, other_b_l = swap(mine_a_r), swap(mine_b_l)
    mine_a_far, mine_b_far = send(mine_a_r, right), send(mine_b_l, left)
    other_b_r, other_a_l = swap(mine_b_r), swap(mine_a_l)
    other_a_far, other_b_far = send(other_a_r, right), send(other_b_l, left)

    conv_out = conv_module(conv_input, carried, conv_taps, conv_gain.reshape(1, width), conv_weight)

    weights = [gate, up, down]
    sources = [((0,), (1,), (2,), False)]
    for arrays in (
        (mine_a_r, mine_b_r, other_a_r, other_b_r, down_r),
        (mine_a_l, mine_b_l, other_a_l, other_b_l, down_l),
        (mine_a_far, mine_b_far, other_a_far, other_b_far, down_a_far, down_b_far),
    ):
        at = len(weights)
        weights.extend(arrays)
        parts = tuple(range(at + 4, len(weights)))
        sources.append(((at, at + 1), (at + 2, at + 3), parts, True))
    late = [id(w) for w in (other_b_r, other_a_l, other_a_far, other_b_far)]
    far = tuple(id(w) not in late for w in weights)
    results = experts_apply(odd.reshape(1), arrived, weights, far, tuple(sources), capacity)
    returned = lax.all_to_all(results, EP, 0, 0, tiled=True)
    own_weights = lax.dynamic_slice_in_dim(route_weights, own * tokens, tokens, 0)
    moe_out = combine(returned, target.T, own_weights, post_gain.reshape(1, width), capacity)
    return (conv_out, moe_out)


def solution(mesh):
    return jax.shard_map(
        run,
        mesh=mesh,
        in_specs=(
            P(GRP_EP, None),
            P(),
            P(),
            P(None, "tp"),
            P(GRP_EP, None),
            P(),
            P(GRP_EP, None),
            P(GRP_EP, None),
            P(EP, None, "tp"),
            P(EP, None, "tp"),
            P(EP, "tp", None),
            P(),
        ),
        out_specs=(P(GRP_EP, "tp"), P(GRP_EP_TP, None)),
        check_vma=False,
    )
```

```python
import jax
import jax.numpy as jnp
from jax import lax
from jax.experimental import pallas as pl
from jax.experimental.pallas import tpu as pltpu
from jax.sharding import PartitionSpec as P

EPSILON = 1e-06
LANES = 128
F32 = jnp.float32
BF16 = jnp.bfloat16


def whole():
    return pl.BlockSpec(memory_space=pltpu.VMEM)


def dot(a, b):
    return jnp.dot(a, b, preferred_element_type=F32)


def split_rows(capacity):
    main = capacity // 8 * 8
    return main, capacity - main


def col(ref_or_value, c):
    return ref_or_value[:, c * LANES : (c + 1) * LANES]


def selection(index, first, count, dim):
    shape = (count, index.shape[1]) if dim == 0 else (index.shape[0], count)
    return index == first + lax.broadcasted_iota(jnp.int32, shape, dim)


def put_message(out_ref, head_of, tail_of, peers, head, tail, blocks):
    for c in range(0, blocks, 2):
        pair = [head_of(c + i).reshape(peers, head, LANES) for i in range(2)]
        out_ref[:, c * head : (c + 2) * head, :] = jnp.concatenate(pair, axis=1).astype(BF16)
    per = 8 // tail
    base = blocks * head
    for j in range(0, blocks // per, 2):
        pair = [tail_of(j + i).reshape(peers, 8, LANES) for i in range(2)]
        out_ref[:, base + j * 8 : base + (j + 2) * 8, :] = jnp.concatenate(pair, axis=1).astype(BF16)


def dispatch_kernel(
    own_ref, all_ref, gain_ref, ids_ref, out_ref, target_ref, rows_ref, signal, *, experts, capacity
):
    tokens, width = rows_ref.shape
    copy = pltpu.make_async_copy(
        all_ref.at[pl.ds(pl.multiple_of(own_ref[0] * tokens, 16), tokens), :], rows_ref, signal
    )
    copy.start()
    blocks = width // LANES
    head, tail = split_rows(capacity)
    per = 8 // tail
    ids = ids_ref[...]
    onehot = [
        (ids[k : k + 1, :] == lax.broadcasted_iota(jnp.int32, (experts, tokens), 0)).astype(F32)
        for k in range(2)
    ]
    before = lax.broadcasted_iota(jnp.int32, (tokens, tokens), 0) < lax.broadcasted_iota(
        jnp.int32, (tokens, tokens), 1
    )
    before = before.astype(F32).astype(BF16)
    counts = [dot(h.astype(BF16), before) for h in onehot]
    counts[1] = counts[1] + jnp.sum(onehot[0], axis=1, keepdims=True)
    place = [jnp.sum(c * h, axis=0, keepdims=True).astype(jnp.int32) for c, h in zip(counts, onehot)]
    place = jnp.concatenate(place, axis=0)
    target_ref[...] = ids * capacity + place
    in_head = jnp.where(place < head, ids * head + place, -64)
    in_tail = jnp.where(place < head, -64, ids * 8 + place - head)
    pick = jnp.zeros((experts * head, tokens), F32)
    picks = [jnp.zeros((experts * 8, tokens), F32) for _ in range(per)]
    for k in range(2):
        pick = pick + selection(in_head[k : k + 1], 0, experts * head, 0).astype(F32)
        for q in range(per):
            picks[q] = picks[q] + selection(in_tail[k : k + 1], -q * tail, experts * 8, 0).astype(F32)
    pick = pick.astype(BF16)
    picks = jnp.concatenate(picks, axis=1).astype(BF16)
    copy.wait()
    rows = rows_ref[...].astype(F32)
    mean_square = jnp.mean(rows * rows, axis=-1, keepdims=True)
    normed = (rows * lax.rsqrt(mean_square + EPSILON) * gain_ref[...]).astype(BF16)

    def tail_of(j):
        stack = [col(normed, per * j + q) for q in range(per)]
        return dot(picks, jnp.concatenate(stack, axis=0))

    put_message(
        out_ref, lambda c: dot(pick, col(normed, c)), tail_of, experts, head, tail, blocks
    )


def dispatch(own, rows, gain, ids, experts, capacity):
    tokens = ids.shape[1]
    width = rows.shape[1]

    def kernel(*refs):
        dispatch_kernel(*refs, experts=experts, capacity=capacity)

    return pl.pallas_call(
        kernel,
        in_specs=[
            pl.BlockSpec(memory_space=pltpu.SMEM),
            pl.BlockSpec(memory_space=pltpu.HBM),
            whole(),
            whole(),
        ],
        out_specs=[whole(), whole()],
        scratch_shapes=[pltpu.VMEM((tokens, width), BF16), pltpu.SemaphoreType.DMA],
        out_shape=[
            jax.ShapeDtypeStruct((experts, capacity * width // LANES, LANES), BF16),
            jax.ShapeDtypeStruct((2, tokens), jnp.int32),
        ],
        compiler_params=pltpu.CompilerParams(vmem_limit_bytes=24 << 20),
        name="dispatch",
    )(own, pltpu.with_memory_space_constraint(rows, pltpu.HBM), gain, ids)


def expert_kernel(*refs, sources, far, peers, capacity, blocks):
    odd_ref, message_ref = refs[0], refs[1]
    count = sum(len(rows) for rows in far)
    given = list(refs[2 : count + 2])
    out_ref, rows_ref, hidden_ref = refs[count + 2 : count + 5]
    near, signals = list(refs[count + 5 : -1]), refs[-1]
    odd = odd_ref[0] == 1
    weights, copies = [], []
    used = 0
    for rows in far:
        pieces = [given.pop(0) for _ in rows]
        if rows == (0,):
            weights.append(pieces[0])
            copies.append([])
            continue
        weights.append(near.pop(0))
        moves, at = [], 0
        for piece, size in zip(pieces, rows):
            place = weights[-1].at[at : at + size, :]
            moves.append(pltpu.make_async_copy(piece, place, signals.at[used]))
            at += size
            used += 1
        copies.append(moves)
    waves = [[*s[0], *s[1]] for s in sources] + [[d for s in sources for d in s[2]]]

    def issue(wave):
        for w in wave:
            for move in copies[w]:
                move.start()

    def settle(wave):
        for w in wave:
            for move in copies[w]:
                move.wait()

    issue(waves[0])
    issue(waves[1])
    head, tail = split_rows(capacity)
    per = 8 // tail
    heads = peers * head
    for c in range(0, blocks, 2):
        both = message_ref[:, c * head : (c + 2) * head, :].astype(F32)
        for i in range(2):
            part = both[:, i * head : (i + 1) * head, :].reshape(heads, LANES)
            rows_ref[0:heads, (c + i) * LANES : (c + i + 1) * LANES] = part.astype(BF16)
    base = blocks * head
    slot = lax.broadcasted_iota(jnp.int32, (peers * tail, peers * 8), 0)
    lane = lax.broadcasted_iota(jnp.int32, (peers * tail, peers * 8), 1)
    gathers = [
        (lane == slot // tail * 8 + q * tail + slot % tail).astype(F32).astype(BF16)
        for q in range(per)
    ]
    for j in range(0, blocks // per, 2):
        both = message_ref[:, base + j * 8 : base + (j + 2) * 8, :].astype(F32)
        for i in range(2):
            part = both[:, i * 8 : (i + 1) * 8, :].reshape(peers * 8, LANES).astype(BF16)
            for q in range(per):
                c = per * (j + i) + q
                rows_ref[heads:, c * LANES : (c + 1) * LANES] = dot(gathers[q], part).astype(BF16)
    at = 0
    downs = []
    for n, (gates, ups, down_parts, swapped) in enumerate(sources):
        settle(waves[n])
        if n + 2 < len(waves):
            issue(waves[n + 2])
        rows = rows_ref[...]
        values = []
        for group in (gates, ups):
            value = None
            begin = 0
            for g in group:
                size = weights[g].shape[0]
                part = dot(rows[:, begin : begin + size], weights[g][...])
                value = part if value is None else value + part
                begin += size
            values.append(value)
        gate_value, up_value = values
        if swapped:
            gate_value, up_value = (
                jnp.where(odd, up_value, gate_value),
                jnp.where(odd, gate_value, up_value),
            )
        hidden = gate_value / (1.0 + jnp.exp(-gate_value)) * up_value
        hidden_ref[:, at : at + hidden.shape[1]] = hidden.astype(BF16)
        for d in down_parts:
            downs.append((at, d))
            at += weights[d].shape[0]
    settle(waves[-1])
    slot = lax.broadcasted_iota(jnp.int32, (peers * 8, peers * tail), 1)
    lane = lax.broadcasted_iota(jnp.int32, (peers * 8, peers * tail), 0)
    spreads = [
        (lane == slot // tail * 8 + q * tail + slot % tail).astype(F32).astype(BF16)
        for q in range(per)
    ]
    step = 2 * per
    for first in range(0, blocks, step):
        cols = slice(first * LANES, (first + step) * LANES)
        total = None
        for begin, d in downs:
            size = weights[d].shape[0]
            part = dot(hidden_ref[:, begin : begin + size], weights[d][:, cols])
            total = part if total is None else total + part
        for c in range(0, step, 2):
            pair = [col(total, c + i)[0:heads].reshape(peers, head, LANES) for i in range(2)]
            at_row = (first + c) * head
            out_ref[:, at_row : at_row + 2 * head, :] = jnp.concatenate(pair, axis=1).astype(BF16)
        last = total[heads:].astype(BF16)
        pair = []
        for i in range(2):
            spread = None
            for q in range(per):
                part = dot(spreads[q], col(last, per * i + q))
                spread = part if spread is None else spread + part
            pair.append(spread.reshape(peers, 8, LANES))
        at_row = base + first // per * 8
        out_ref[:, at_row : at_row + 16, :] = jnp.concatenate(pair, axis=1).astype(BF16)


def experts_apply(odd, message, matrices, direct, sources, capacity):
    peers, lines, _ = message.shape
    blocks = lines // capacity
    far = tuple((0,) if d else tuple(p.shape[0] for p in m) for m, d in zip(matrices, direct))
    units = sum(sum(p.shape[0] for p in matrices[d]) for s in sources for d in s[2])

    def kernel(*refs):
        expert_kernel(*refs, sources=sources, far=far, peers=peers, capacity=capacity, blocks=blocks)

    operands, specs, scratch = [], [], []
    for pieces, rows in zip(matrices, far):
        if rows == (0,):
            operands.extend(pieces)
            specs.append(whole())
            continue
        operands.extend(pltpu.with_memory_space_constraint(p, pltpu.HBM) for p in pieces)
        specs.extend(pl.BlockSpec(memory_space=pltpu.HBM) for _ in pieces)
        scratch.append(pltpu.VMEM((sum(rows), pieces[0].shape[1]), BF16))
    return pl.pallas_call(
        kernel,
        in_specs=[pl.BlockSpec(memory_space=pltpu.SMEM), whole(), *specs],
        out_specs=whole(),
        out_shape=jax.ShapeDtypeStruct(message.shape, BF16),
        scratch_shapes=[
            pltpu.VMEM((peers * capacity, blocks * LANES), BF16),
            pltpu.VMEM((peers * capacity, units), BF16),
            *scratch,
            pltpu.SemaphoreType.DMA((len(operands),)),
        ],
        compiler_params=pltpu.CompilerParams(vmem_limit_bytes=40 << 20),
        name="experts",
    )(odd, message, *operands)


def combine_kernel(
    message_ref, target_ref, far_ref, gain_ref, out_ref, mixed_ref, weight_ref, signal, *, capacity
):
    copy = pltpu.make_async_copy(far_ref, weight_ref, signal)
    copy.start()
    peers = message_ref.shape[0]
    tokens, width = out_ref.shape
    blocks = width // LANES
    head, tail = split_rows(capacity)
    per = 8 // tail
    heads = peers * head
    target = target_ref[...]
    peer = target // capacity
    place = target - peer * capacity
    in_head = jnp.where(place < head, peer * head + place, -64)
    in_tail = jnp.where(place < head, -64, peer * 8 + place - head)
    pick = [selection(in_head[:, k : k + 1], 0, heads, 1).astype(F32) for k in range(2)]
    pick = jnp.concatenate(pick, axis=0).astype(BF16)
    picks = []
    for q in range(per):
        both = [selection(in_tail[:, k : k + 1], -q * tail, peers * 8, 1).astype(F32) for k in range(2)]
        picks.append(jnp.concatenate(both, axis=0).astype(BF16))
    copy.wait()
    weight = [weight_ref[:, k : k + 1] for k in range(2)]
    base = blocks * head
    square = jnp.zeros((tokens, LANES), F32)
    for c in range(0, blocks, 2):
        both = message_ref[:, c * head : (c + 2) * head, :].astype(F32)
        for i in range(2):
            part = both[:, i * head : (i + 1) * head, :].reshape(heads, LANES).astype(BF16)
            j = (c + i) // per
            rest = message_ref[:, base + j // 2 * 16 : base + j // 2 * 16 + 16, :].astype(F32)
            rest = rest[:, j % 2 * 8 : j % 2 * 8 + 8, :].reshape(peers * 8, LANES).astype(BF16)
            rows = dot(pick, part) + dot(picks[(c + i) % per], rest)
            mixed = rows[:tokens] * weight[0] + rows[tokens:] * weight[1]
            mixed_ref[:, (c + i) * LANES : (c + i + 1) * LANES] = mixed
            square = square + mixed * mixed
    scale = lax.rsqrt(jnp.sum(square, axis=1, keepdims=True) * (1.0 / width) + EPSILON)
    out_ref[...] = (mixed_ref[...] * scale * gain_ref[...]).astype(BF16)


def combine(message, target, weight, gain, capacity):
    tokens = target.shape[0]
    width = gain.shape[1]

    def kernel(*refs):
        combine_kernel(*refs, capacity=capacity)

    return pl.pallas_call(
        kernel,
        in_specs=[whole(), whole(), pl.BlockSpec(memory_space=pltpu.HBM), whole()],
        out_specs=whole(),
        out_shape=jax.ShapeDtypeStruct((tokens, width), BF16),
        scratch_shapes=[
            pltpu.VMEM((tokens, width), F32),
            pltpu.VMEM(weight.shape, F32),
            pltpu.SemaphoreType.DMA,
        ],
        compiler_params=pltpu.CompilerParams(vmem_limit_bytes=24 << 20),
        name="combine",
    )(message, target, pltpu.with_memory_space_constraint(weight, pltpu.HBM), gain)


def conv_kernel(rows_ref, carried_ref, taps_ref, gain_ref, weight_ref, out_ref, line_ref, sum_ref):
    block, width = rows_ref.shape
    blocks = width // LANES
    reach = taps_ref.shape[0] - 1
    halo = line_ref.shape[1] - block
    step = pl.program_id(0)

    @pl.when(step == 0)
    def _():
        for c in range(blocks):
            line_ref[c, 0:halo, :] = col(carried_ref, c).astype(F32)

    @pl.when(step > 0)
    def _():
        for c in range(blocks):
            line_ref[c, 0:halo, :] = line_ref[c, block : block + halo, :]

    for c in range(blocks):
        line_ref[c, halo:, :] = col(rows_ref, c).astype(F32)

    strip = 64

    def column(c, square):
        parts = []
        for first in range(0, block, strip):
            total = jnp.zeros((strip, LANES), F32)
            for k in range(reach + 1):
                at = first + halo - reach + k
                total = total + line_ref[c, at : at + strip, :] * taps_ref[k, pl.ds(c, 1), :]
            sum_ref[c, first : first + strip, :] = total
            parts.append(total * total)
        return square + jnp.concatenate(parts, axis=0)

    square = lax.fori_loop(0, blocks, column, jnp.zeros((block, LANES), F32))
    scale = lax.rsqrt(jnp.sum(square, axis=1, keepdims=True) * (1.0 / width) + EPSILON)
    result = jnp.zeros((block, out_ref.shape[1]), F32)
    for c in range(0, blocks, 4):
        group = []
        for i in range(4):
            value = sum_ref[c + i] * scale * col(gain_ref, c + i)
            group.append((value / (1.0 + jnp.exp(-value))).astype(BF16))
        part = jnp.concatenate(group, axis=1)
        result = result + dot(part, weight_ref[c * LANES : (c + 4) * LANES, :])
    out_ref[...] = result.astype(BF16)


def conv_module(rows, carried, taps, gain, weight, block=128):
    count, width = rows.shape
    blocks = width // LANES
    halo = carried.shape[0]
    return pl.pallas_call(
        conv_kernel,
        grid=(count // block,),
        in_specs=[
            pl.BlockSpec((block, width), lambda i: (i, 0)),
            pl.BlockSpec((halo, width), lambda i: (0, 0)),
            pl.BlockSpec((taps.shape[0], blocks, LANES), lambda i: (0, 0, 0)),
            pl.BlockSpec((1, width), lambda i: (0, 0)),
            pl.BlockSpec(weight.shape, lambda i: (0, 0)),
        ],
        out_specs=pl.BlockSpec((block, weight.shape[1]), lambda i: (i, 0)),
        out_shape=jax.ShapeDtypeStruct((count, weight.shape[1]), BF16),
        scratch_shapes=[
            pltpu.VMEM((blocks, block + halo, LANES), F32),
            pltpu.VMEM((blocks, block, LANES), F32),
        ],
        compiler_params=pltpu.CompilerParams(vmem_limit_bytes=24 << 20),
        name="conv",
    )(rows, carried, taps.reshape(taps.shape[0], blocks, LANES), gain, weight)


EP = "ep"
GRP_EP = ("grp", "ep")
GRP_EP_TP = ("grp", "ep", "tp")
HALO = 32


def run(
    conv_input,
    conv_taps,
    conv_gain,
    conv_weight,
    moe_input,
    moe_gain,
    expert_ids,
    route_weights,
    gate_weight,
    up_weight,
    down_weight,
    post_gain,
):
    quarters = lax.axis_size("tp")
    ep_count = lax.axis_size(EP)
    width = moe_input.shape[1]
    tokens = moe_input.shape[0] // quarters
    capacity = 2 * tokens // ep_count
    own = lax.axis_index("tp").astype(jnp.int32)

    odd = (lax.axis_index("grp") % 2).astype(jnp.int32)

    right = [(i, (i + 1) % quarters) for i in range(quarters)]
    left = [(i, (i - 1) % quarters) for i in range(quarters)]
    across = [(i, i ^ 1) for i in range(lax.axis_size("grp"))]
    gate, up, down = gate_weight[0], up_weight[0], down_weight[0]
    half, part = gate.shape[0] // 2, down.shape[0] * 3 // 4

    def send(array, pairs):
        return lax.ppermute(array, "tp", pairs)

    def swap(array):
        return lax.ppermute(array, "grp", across)

    down_r = send(down, right)
    mine_a = jnp.where(odd == 1, up[:half], gate[:half])
    mine_b = jnp.where(odd == 1, up[half:], gate[half:])
    mine_a_l, mine_b_l = send(mine_a, left), send(mine_b, left)
    own_ids = lax.dynamic_slice_in_dim(expert_ids, own * tokens, tokens, 0).T
    message, target = dispatch(
        own.reshape(1), moe_input, moe_gain.reshape(1, width), own_ids, ep_count, capacity
    )
    arrived = lax.all_to_all(message, EP, 0, 0, tiled=True)
    mine_a_r, mine_b_r = send(mine_a, right), send(mine_b, right)
    other_a_l, mine_a_far = swap(mine_a_l), send(mine_a_l, left)
    down_l = send(down, left)
    pairs = [(i, i + 1) for i in range(ep_count - 1)]
    carried = lax.ppermute(conv_input[conv_input.shape[0] - HALO :], EP, pairs)
    other_b_l, mine_b_far = swap(mine_b_l), send(mine_b_l, left)
    down_a_far = send(down_r[:part], right)
    other_a_r = swap(mine_a_r)
    other_b_r = swap(mine_b_r)
    other_a_far = swap(mine_a_far)
    other_b_far, down_b_far = send(other_b_r, right), send(down_l[part:], left)

    conv_out = conv_module(conv_input, carried, conv_taps, conv_gain.reshape(1, width), conv_weight)

    matrices = [
        *((gate,), (up,), (down,)),
        *((mine_a_r, mine_b_r), (other_a_r, other_b_r), (down_r,)),
        *((mine_a_l, mine_b_l), (other_a_l, other_b_l), (down_l,)),
        *((mine_a_far,), (mine_b_far,), (other_a_far,), (other_b_far,), (down_a_far, down_b_far)),
    ]
    sources = (
        ((0,), (1,), (2,), False),
        ((6,), (7,), (8,), True),
        ((3,), (4,), (5,), True),
        ((9, 10), (11, 12), (13,), True),
    )
    direct = tuple(n in (10, 11, 12) for n in range(len(matrices)))
    results = experts_apply(odd.reshape(1), arrived, matrices, direct, sources, capacity)
    returned = lax.all_to_all(results, EP, 0, 0, tiled=True)
    own_weights = lax.dynamic_slice_in_dim(route_weights, own * tokens, tokens, 0)
    moe_out = combine(returned, target.T, own_weights, post_gain.reshape(1, width), capacity)
    return (conv_out, moe_out)


def solution(mesh):
    return jax.shard_map(
        run,
        mesh=mesh,
        in_specs=(
            P(GRP_EP, None),
            P(),
            P(),
            P(None, "tp"),
            P(GRP_EP, None),
            P(),
            P(GRP_EP, None),
            P(GRP_EP, None),
            P(EP, None, "tp"),
            P(EP, None, "tp"),
            P(EP, "tp", None),
            P(),
        ),
        out_specs=(P(GRP_EP, "tp"), P(GRP_EP_TP, None)),
        check_vma=False,
    )
```

```python
import jax
import jax.numpy as jnp
from jax import lax
from jax.experimental import pallas as pl
from jax.experimental.pallas import tpu as pltpu
from jax.sharding import PartitionSpec as P

EPSILON = 1e-06
LANES = 128
F32 = jnp.float32
BF16 = jnp.bfloat16


def whole():
    return pl.BlockSpec(memory_space=pltpu.VMEM)


def dot(a, b):
    return jnp.dot(a, b, preferred_element_type=F32)


def split_rows(capacity):
    main = capacity // 8 * 8
    return main, capacity - main


def col(ref_or_value, c):
    return ref_or_value[:, c * LANES : (c + 1) * LANES]


def selection(index, first, count, dim):
    shape = (count, index.shape[1]) if dim == 0 else (index.shape[0], count)
    return index == first + lax.broadcasted_iota(jnp.int32, shape, dim)


def put_message(out_ref, head_of, tail_of, peers, head, tail, blocks):
    for c in range(0, blocks, 2):
        pair = [head_of(c + i).reshape(peers, head, LANES) for i in range(2)]
        out_ref[:, c * head : (c + 2) * head, :] = jnp.concatenate(pair, axis=1).astype(BF16)
    per = 8 // tail
    base = blocks * head
    for j in range(0, blocks // per, 2):
        pair = [tail_of(j + i).reshape(peers, 8, LANES) for i in range(2)]
        out_ref[:, base + j * 8 : base + (j + 2) * 8, :] = jnp.concatenate(pair, axis=1).astype(BF16)


def dispatch_kernel(
    own_ref,
    all_ref,
    far_gain_ref,
    ids_ref,
    gate_ref,
    up_ref,
    out_ref,
    target_ref,
    *rest,
    experts,
    capacity,
):
    picked, (rows_ref, gain_ref, signals) = rest[:-3], rest[-3:]
    tokens, width = rows_ref.shape
    blocks = width // LANES
    head, tail = split_rows(capacity)
    per = 8 // tail
    copy = pltpu.make_async_copy(
        all_ref.at[pl.ds(pl.multiple_of(own_ref[0] * tokens, 16), tokens), :],
        rows_ref,
        signals.at[0],
    )
    copy.start()
    gain_copy = pltpu.make_async_copy(far_gain_ref, gain_ref, signals.at[1])
    gain_copy.start()

    def moves(source_ref):
        at = 0
        for i, ref in enumerate(picked):
            rows = source_ref.at[at : at + ref.shape[0], :]
            yield pltpu.make_async_copy(rows, ref, signals.at[2 + i])
            at += ref.shape[0]

    for odd, source_ref in ((0, gate_ref), (1, up_ref)):

        @pl.when(own_ref[1] == odd)
        def _(source_ref=source_ref):
            for move in moves(source_ref):
                move.start()

    ids = ids_ref[...]
    onehot = [
        (ids[k : k + 1, :] == lax.broadcasted_iota(jnp.int32, (experts, tokens), 0)).astype(F32)
        for k in range(2)
    ]
    before = lax.broadcasted_iota(jnp.int32, (tokens, tokens), 0) < lax.broadcasted_iota(
        jnp.int32, (tokens, tokens), 1
    )
    before = before.astype(F32).astype(BF16)
    counts = [dot(h.astype(BF16), before) for h in onehot]
    counts[1] = counts[1] + jnp.sum(onehot[0], axis=1, keepdims=True)
    place = [jnp.sum(c * h, axis=0, keepdims=True).astype(jnp.int32) for c, h in zip(counts, onehot)]
    place = jnp.concatenate(place, axis=0)
    target_ref[...] = ids * capacity + place
    in_head = jnp.where(place < head, ids * head + place, -64)
    in_tail = jnp.where(place < head, -64, ids * 8 + place - head)
    pick = jnp.zeros((experts * head, tokens), F32)
    picks = [jnp.zeros((experts * 8, tokens), F32) for _ in range(per)]
    for k in range(2):
        pick = pick + selection(in_head[k : k + 1], 0, experts * head, 0).astype(F32)
        for q in range(per):
            picks[q] = picks[q] + selection(in_tail[k : k + 1], -q * tail, experts * 8, 0).astype(F32)
    pick = pick.astype(BF16)
    picks = jnp.concatenate(picks, axis=1).astype(BF16)
    copy.wait()
    gain_copy.wait()
    rows = rows_ref[...].astype(F32)
    mean_square = jnp.mean(rows * rows, axis=-1, keepdims=True)
    normed = (rows * lax.rsqrt(mean_square + EPSILON) * gain_ref[...]).astype(BF16)

    def tail_of(j):
        stack = [col(normed, per * j + q) for q in range(per)]
        return dot(picks, jnp.concatenate(stack, axis=0))

    put_message(
        out_ref, lambda c: dot(pick, col(normed, c)), tail_of, experts, head, tail, blocks
    )
    for odd, source_ref in ((0, gate_ref), (1, up_ref)):

        @pl.when(own_ref[1] == odd)
        def _(source_ref=source_ref):
            for move in moves(source_ref):
                move.wait()


def dispatch(own, rows, gain, ids, gate, up, cuts, experts, capacity):
    tokens = ids.shape[1]
    width = rows.shape[1]
    hbm = pl.BlockSpec(memory_space=pltpu.HBM)

    def kernel(*refs):
        dispatch_kernel(*refs, experts=experts, capacity=capacity)

    def held(array):
        return pltpu.with_memory_space_constraint(array, pltpu.HBM)

    return pl.pallas_call(
        kernel,
        in_specs=[pl.BlockSpec(memory_space=pltpu.SMEM), hbm, hbm, whole(), hbm, hbm],
        out_specs=[whole(), whole(), *(hbm for _ in cuts)],
        scratch_shapes=[
            pltpu.VMEM((tokens, width), BF16),
            pltpu.VMEM(gain.shape, F32),
            pltpu.SemaphoreType.DMA((2 + len(cuts),)),
        ],
        out_shape=[
            jax.ShapeDtypeStruct((experts, capacity * width // LANES, LANES), BF16),
            jax.ShapeDtypeStruct((2, tokens), jnp.int32),
            *(pltpu.HBM((cut, gate.shape[1]), BF16) for cut in cuts),
        ],
        compiler_params=pltpu.CompilerParams(vmem_limit_bytes=24 << 20),
        name="dispatch",
    )(own, held(rows), held(gain), ids, held(gate), held(up))


def expert_kernel(*refs, sources, far, peers, capacity, blocks):
    odd_ref, message_ref = refs[0], refs[1]
    count = sum(len(rows) for rows in far)
    given = list(refs[2 : count + 2])
    out_ref, rows_ref, hidden_ref = refs[count + 2 : count + 5]
    near, signals = list(refs[count + 5 : -1]), refs[-1]
    odd = odd_ref[0] == 1
    weights, copies = [], []
    used = 0
    for rows in far:
        pieces = [given.pop(0) for _ in rows]
        if rows == (0,):
            weights.append(pieces[0])
            copies.append([])
            continue
        if rows[0] < 0:
            weights.append(near.pop(0))
            copies.append([])
            at = 0
            for piece in pieces:
                weights[-1][at : at + piece.shape[0], :] = piece[...]
                at += piece.shape[0]
            continue
        weights.append(near.pop(0))
        moves, at = [], 0
        for piece, size in zip(pieces, rows):
            place = weights[-1].at[at : at + size, :]
            moves.append(pltpu.make_async_copy(piece, place, signals.at[used]))
            at += size
            used += 1
        copies.append(moves)
    waves = [[*s[0], *s[1]] for s in sources] + [[d for s in sources for d in s[2]]]

    def issue(wave):
        for w in wave:
            for move in copies[w]:
                move.start()

    def settle(wave):
        for w in wave:
            for move in copies[w]:
                move.wait()

    issue(waves[0])
    issue(waves[1])
    head, tail = split_rows(capacity)
    per = 8 // tail
    heads = peers * head
    for c in range(0, blocks, 2):
        both = message_ref[:, c * head : (c + 2) * head, :].astype(F32)
        for i in range(2):
            part = both[:, i * head : (i + 1) * head, :].reshape(heads, LANES)
            rows_ref[0:heads, (c + i) * LANES : (c + i + 1) * LANES] = part.astype(BF16)
    base = blocks * head
    slot = lax.broadcasted_iota(jnp.int32, (peers * tail, peers * 8), 0)
    lane = lax.broadcasted_iota(jnp.int32, (peers * tail, peers * 8), 1)
    gathers = [
        (lane == slot // tail * 8 + q * tail + slot % tail).astype(F32).astype(BF16)
        for q in range(per)
    ]
    for j in range(0, blocks // per, 2):
        both = message_ref[:, base + j * 8 : base + (j + 2) * 8, :].astype(F32)
        for i in range(2):
            part = both[:, i * 8 : (i + 1) * 8, :].reshape(peers * 8, LANES).astype(BF16)
            for q in range(per):
                c = per * (j + i) + q
                rows_ref[heads:, c * LANES : (c + 1) * LANES] = dot(gathers[q], part).astype(BF16)
    at = 0
    downs = []
    for n, (gates, ups, down_parts, swapped) in enumerate(sources):
        settle(waves[n])
        if n + 2 < len(waves):
            issue(waves[n + 2])
        rows = rows_ref[...]
        values = []
        for group in (gates, ups):
            value = None
            begin = 0
            for g in group:
                size = weights[g].shape[0]
                part = dot(rows[:, begin : begin + size], weights[g][...])
                value = part if value is None else value + part
                begin += size
            values.append(value)
        gate_value, up_value = values
        if swapped:
            gate_value, up_value = (
                jnp.where(odd, up_value, gate_value),
                jnp.where(odd, gate_value, up_value),
            )
        hidden = gate_value / (1.0 + jnp.exp(-gate_value)) * up_value
        hidden_ref[:, at : at + hidden.shape[1]] = hidden.astype(BF16)
        for d in down_parts:
            downs.append((at, d))
            at += weights[d].shape[0]
    settle(waves[-1])
    slot = lax.broadcasted_iota(jnp.int32, (peers * 8, peers * tail), 1)
    lane = lax.broadcasted_iota(jnp.int32, (peers * 8, peers * tail), 0)
    spreads = [
        (lane == slot // tail * 8 + q * tail + slot % tail).astype(F32).astype(BF16)
        for q in range(per)
    ]
    step = 2 * per
    for first in range(0, blocks, step):
        cols = slice(first * LANES, (first + step) * LANES)
        total = None
        for begin, d in downs:
            size = weights[d].shape[0]
            part = dot(hidden_ref[:, begin : begin + size], weights[d][:, cols])
            total = part if total is None else total + part
        for c in range(0, step, 2):
            pair = [col(total, c + i)[0:heads].reshape(peers, head, LANES) for i in range(2)]
            at_row = (first + c) * head
            out_ref[:, at_row : at_row + 2 * head, :] = jnp.concatenate(pair, axis=1).astype(BF16)
        last = total[heads:].astype(BF16)
        pair = []
        for i in range(2):
            spread = None
            for q in range(per):
                part = dot(spreads[q], col(last, per * i + q))
                spread = part if spread is None else spread + part
            pair.append(spread.reshape(peers, 8, LANES))
        at_row = base + first // per * 8
        out_ref[:, at_row : at_row + 16, :] = jnp.concatenate(pair, axis=1).astype(BF16)


def experts_apply(odd, message, matrices, direct, sources, capacity):
    peers, lines, _ = message.shape
    blocks = lines // capacity
    far = []
    for pieces, held in zip(matrices, direct):
        rows = tuple(p.shape[0] for p in pieces)
        far.append(rows if not held else (0,) if len(rows) == 1 else tuple(-r for r in rows))
    units = sum(sum(p.shape[0] for p in matrices[d]) for s in sources for d in s[2])

    def kernel(*refs):
        expert_kernel(*refs, sources=sources, far=far, peers=peers, capacity=capacity, blocks=blocks)

    operands, specs, scratch = [], [], []
    for pieces, rows in zip(matrices, far):
        if rows == (0,):
            operands.extend(pieces)
            specs.append(whole())
            continue
        scratch.append(pltpu.VMEM((abs(sum(rows)), pieces[0].shape[1]), BF16))
        if rows[0] < 0:
            operands.extend(pieces)
            specs.extend(whole() for _ in pieces)
            continue
        operands.extend(pltpu.with_memory_space_constraint(p, pltpu.HBM) for p in pieces)
        specs.extend(pl.BlockSpec(memory_space=pltpu.HBM) for _ in pieces)
    return pl.pallas_call(
        kernel,
        in_specs=[pl.BlockSpec(memory_space=pltpu.SMEM), whole(), *specs],
        out_specs=whole(),
        out_shape=jax.ShapeDtypeStruct(message.shape, BF16),
        scratch_shapes=[
            pltpu.VMEM((peers * capacity, blocks * LANES), BF16),
            pltpu.VMEM((peers * capacity, units), BF16),
            *scratch,
            pltpu.SemaphoreType.DMA((len(operands),)),
        ],
        compiler_params=pltpu.CompilerParams(vmem_limit_bytes=40 << 20),
        name="experts",
    )(odd, message, *operands)


def combine_kernel(
    message_ref, target_ref, far_ref, gain_ref, out_ref, mixed_ref, weight_ref, signal, *, capacity
):
    copy = pltpu.make_async_copy(far_ref, weight_ref, signal)
    copy.start()
    peers = message_ref.shape[0]
    tokens, width = out_ref.shape
    blocks = width // LANES
    head, tail = split_rows(capacity)
    per = 8 // tail
    heads = peers * head
    target = target_ref[...]
    peer = target // capacity
    place = target - peer * capacity
    in_head = jnp.where(place < head, peer * head + place, -64)
    in_tail = jnp.where(place < head, -64, peer * 8 + place - head)
    pick = [selection(in_head[:, k : k + 1], 0, heads, 1).astype(F32) for k in range(2)]
    pick = jnp.concatenate(pick, axis=0).astype(BF16)
    picks = []
    for q in range(per):
        both = [selection(in_tail[:, k : k + 1], -q * tail, peers * 8, 1).astype(F32) for k in range(2)]
        picks.append(jnp.concatenate(both, axis=0).astype(BF16))
    copy.wait()
    weight = [weight_ref[:, k : k + 1] for k in range(2)]
    base = blocks * head
    square = jnp.zeros((tokens, LANES), F32)
    for c in range(0, blocks, 2):
        both = message_ref[:, c * head : (c + 2) * head, :].astype(F32)
        for i in range(2):
            part = both[:, i * head : (i + 1) * head, :].reshape(heads, LANES).astype(BF16)
            j = (c + i) // per
            rest = message_ref[:, base + j // 2 * 16 : base + j // 2 * 16 + 16, :].astype(F32)
            rest = rest[:, j % 2 * 8 : j % 2 * 8 + 8, :].reshape(peers * 8, LANES).astype(BF16)
            rows = dot(pick, part) + dot(picks[(c + i) % per], rest)
            mixed = rows[:tokens] * weight[0] + rows[tokens:] * weight[1]
            mixed_ref[:, (c + i) * LANES : (c + i + 1) * LANES] = mixed
            square = square + mixed * mixed
    scale = lax.rsqrt(jnp.sum(square, axis=1, keepdims=True) * (1.0 / width) + EPSILON)
    out_ref[...] = (mixed_ref[...] * scale * gain_ref[...]).astype(BF16)


def combine(message, target, weight, gain, capacity):
    tokens = target.shape[0]
    width = gain.shape[1]

    def kernel(*refs):
        combine_kernel(*refs, capacity=capacity)

    return pl.pallas_call(
        kernel,
        in_specs=[whole(), whole(), pl.BlockSpec(memory_space=pltpu.HBM), whole()],
        out_specs=whole(),
        out_shape=jax.ShapeDtypeStruct((tokens, width), BF16),
        scratch_shapes=[
            pltpu.VMEM((tokens, width), F32),
            pltpu.VMEM(weight.shape, F32),
            pltpu.SemaphoreType.DMA,
        ],
        compiler_params=pltpu.CompilerParams(vmem_limit_bytes=24 << 20),
        name="combine",
    )(message, target, pltpu.with_memory_space_constraint(weight, pltpu.HBM), gain)


def conv_kernel(rows_ref, carried_ref, taps_ref, gain_ref, weight_ref, out_ref, line_ref, sum_ref):
    block, width = rows_ref.shape
    blocks = width // LANES
    reach = taps_ref.shape[0] - 1
    halo = line_ref.shape[1] - block
    step = pl.program_id(0)

    @pl.when(step == 0)
    def _():
        for c in range(blocks):
            line_ref[c, 0:halo, :] = col(carried_ref, c).astype(F32)

    @pl.when(step > 0)
    def _():
        for c in range(blocks):
            line_ref[c, 0:halo, :] = line_ref[c, block : block + halo, :]

    for c in range(blocks):
        line_ref[c, halo:, :] = col(rows_ref, c).astype(F32)

    strip = 64

    def column(c, square):
        parts = []
        for first in range(0, block, strip):
            total = jnp.zeros((strip, LANES), F32)
            for k in range(reach + 1):
                at = first + halo - reach + k
                total = total + line_ref[c, at : at + strip, :] * taps_ref[k, pl.ds(c, 1), :]
            sum_ref[c, first : first + strip, :] = total
            parts.append(total * total)
        return square + jnp.concatenate(parts, axis=0)

    square = lax.fori_loop(0, blocks, column, jnp.zeros((block, LANES), F32))
    scale = lax.rsqrt(jnp.sum(square, axis=1, keepdims=True) * (1.0 / width) + EPSILON)
    result = jnp.zeros((block, out_ref.shape[1]), F32)
    for c in range(0, blocks, 4):
        group = []
        for i in range(4):
            value = sum_ref[c + i] * scale * col(gain_ref, c + i)
            group.append((value / (1.0 + jnp.exp(-value))).astype(BF16))
        part = jnp.concatenate(group, axis=1)
        result = result + dot(part, weight_ref[c * LANES : (c + 4) * LANES, :])
    out_ref[...] = result.astype(BF16)


def conv_module(rows, carried, taps, gain, weight, block=128):
    count, width = rows.shape
    blocks = width // LANES
    halo = carried.shape[0]
    return pl.pallas_call(
        conv_kernel,
        grid=(count // block,),
        in_specs=[
            pl.BlockSpec((block, width), lambda i: (i, 0)),
            pl.BlockSpec((halo, width), lambda i: (0, 0)),
            pl.BlockSpec((taps.shape[0], blocks, LANES), lambda i: (0, 0, 0)),
            pl.BlockSpec((1, width), lambda i: (0, 0)),
            pl.BlockSpec(weight.shape, lambda i: (0, 0)),
        ],
        out_specs=pl.BlockSpec((block, weight.shape[1]), lambda i: (i, 0)),
        out_shape=jax.ShapeDtypeStruct((count, weight.shape[1]), BF16),
        scratch_shapes=[
            pltpu.VMEM((blocks, block + halo, LANES), F32),
            pltpu.VMEM((blocks, block, LANES), F32),
        ],
        compiler_params=pltpu.CompilerParams(vmem_limit_bytes=24 << 20),
        name="conv",
    )(rows, carried, taps.reshape(taps.shape[0], blocks, LANES), gain, weight)


EP = "ep"
GRP_EP = ("grp", "ep")
GRP_EP_TP = ("grp", "ep", "tp")
HALO = 32


def run(
    conv_input,
    conv_taps,
    conv_gain,
    conv_weight,
    moe_input,
    moe_gain,
    expert_ids,
    route_weights,
    gate_weight,
    up_weight,
    down_weight,
    post_gain,
):
    quarters = lax.axis_size("tp")
    ep_count = lax.axis_size(EP)
    width = moe_input.shape[1]
    tokens = moe_input.shape[0] // quarters
    capacity = 2 * tokens // ep_count
    own = lax.axis_index("tp").astype(jnp.int32)

    odd = (lax.axis_index("grp") % 2).astype(jnp.int32)

    right = [(i, (i + 1) % quarters) for i in range(quarters)]
    left = [(i, (i - 1) % quarters) for i in range(quarters)]
    across = [(i, i ^ 1) for i in range(lax.axis_size("grp"))]
    gate, up, down = gate_weight[0], up_weight[0], down_weight[0]
    half, part = gate.shape[0] // 2, down.shape[0] * 7 // 8

    def send(array, pairs):
        return lax.ppermute(array, "tp", pairs)

    def swap(array):
        return lax.ppermute(array, "grp", across)

    down_r = send(down, right)
    own_ids = lax.dynamic_slice_in_dim(expert_ids, own * tokens, tokens, 0).T
    message, target, mine_a, mine_b = dispatch(
        jnp.stack([own, odd]),
        moe_input,
        moe_gain.reshape(1, width),
        own_ids,
        gate,
        up,
        (half, gate.shape[0] - half),
        ep_count,
        capacity,
    )
    mine_a_l, mine_b_l = send(mine_a, left), send(mine_b, left)
    arrived = lax.all_to_all(message, EP, 0, 0, tiled=True)
    mine_a_r, mine_b_r = send(mine_a, right), send(mine_b, right)
    other_a_l, mine_a_far = swap(mine_a_l), send(mine_a_l, left)
    down_l = send(down, left)
    pairs = [(i, i + 1) for i in range(ep_count - 1)]
    carried = lax.ppermute(conv_input[conv_input.shape[0] - HALO :], EP, pairs)
    other_b_l, mine_b_far = swap(mine_b_l), send(mine_b_l, left)
    down_a_far = send(down_r[:part], right)
    other_a_r = swap(mine_a_r)
    other_b_r = swap(mine_b_r)
    other_a_far = swap(mine_a_far)
    other_b_far, down_b_far = send(other_b_r, right), send(down_l[part:], left)

    conv_out = conv_module(conv_input, carried, conv_taps, conv_gain.reshape(1, width), conv_weight)

    matrices = [
        *((gate,), (up,), (down,)),
        *((mine_a_r, mine_b_r), (other_a_r, other_b_r), (down_r,)),
        *((mine_a_l, mine_b_l), (other_a_l, other_b_l), (down_l,)),
        *((mine_a_far,), (mine_b_far,), (other_a_far,), (other_b_far,), (down_a_far, down_b_far)),
    ]
    sources = (
        ((0,), (1,), (2,), False),
        ((6,), (7,), (8,), True),
        ((3,), (4,), (5,), True),
        ((9, 10), (11, 12), (13,), True),
    )
    direct = tuple(n in (11, 12, 13) for n in range(len(matrices)))
    results = experts_apply(odd.reshape(1), arrived, matrices, direct, sources, capacity)
    returned = lax.all_to_all(results, EP, 0, 0, tiled=True)
    own_weights = lax.dynamic_slice_in_dim(route_weights, own * tokens, tokens, 0)
    moe_out = combine(returned, target.T, own_weights, post_gain.reshape(1, width), capacity)
    return (conv_out, moe_out)


def solution(mesh):
    return jax.shard_map(
        run,
        mesh=mesh,
        in_specs=(
            P(GRP_EP, None),
            P(),
            P(),
            P(None, "tp"),
            P(GRP_EP, None),
            P(),
            P(GRP_EP, None),
            P(GRP_EP, None),
            P(EP, None, "tp"),
            P(EP, None, "tp"),
            P(EP, "tp", None),
            P(),
        ),
        out_specs=(P(GRP_EP, "tp"), P(GRP_EP_TP, None)),
        check_vma=False,
    )
```

```python
import jax
import jax.numpy as jnp
from jax import lax
from jax.experimental import pallas as pl
from jax.experimental.pallas import tpu as pltpu
from jax.sharding import PartitionSpec as P

EPSILON = 1e-06
LANES = 128
F32 = jnp.float32
BF16 = jnp.bfloat16


def whole():
    return pl.BlockSpec(memory_space=pltpu.VMEM)


def dot(a, b):
    return jnp.dot(a, b, preferred_element_type=F32)


def split_rows(capacity):
    main = capacity // 8 * 8
    return main, capacity - main


def col(ref_or_value, c):
    return ref_or_value[:, c * LANES : (c + 1) * LANES]


def selection(index, first, count, dim):
    shape = (count, index.shape[1]) if dim == 0 else (index.shape[0], count)
    return index == first + lax.broadcasted_iota(jnp.int32, shape, dim)


def put_message(out_ref, head_of, tail_of, peers, head, tail, blocks):
    for c in range(0, blocks, 2):
        pair = [head_of(c + i).reshape(peers, head, LANES) for i in range(2)]
        out_ref[:, c * head : (c + 2) * head, :] = jnp.concatenate(pair, axis=1).astype(BF16)
    per = 8 // tail
    base = blocks * head
    for j in range(0, blocks // per, 2):
        pair = [tail_of(j + i).reshape(peers, 8, LANES) for i in range(2)]
        out_ref[:, base + j * 8 : base + (j + 2) * 8, :] = jnp.concatenate(pair, axis=1).astype(BF16)


def dispatch_kernel(
    own_ref,
    all_ref,
    far_gain_ref,
    ids_ref,
    gate_ref,
    up_ref,
    out_ref,
    target_ref,
    *rest,
    experts,
    capacity,
):
    picked, (rows_ref, gain_ref, signals) = rest[:-3], rest[-3:]
    tokens, width = rows_ref.shape
    blocks = width // LANES
    head, tail = split_rows(capacity)
    per = 8 // tail
    copy = pltpu.make_async_copy(
        all_ref.at[pl.ds(pl.multiple_of(own_ref[0] * tokens, 16), tokens), :],
        rows_ref,
        signals.at[0],
    )
    copy.start()
    gain_copy = pltpu.make_async_copy(far_gain_ref, gain_ref, signals.at[1])
    gain_copy.start()

    def moves(source_ref):
        at = 0
        for i, ref in enumerate(picked):
            rows = source_ref.at[at : at + ref.shape[0], :]
            yield pltpu.make_async_copy(rows, ref, signals.at[2 + i])
            at += ref.shape[0]

    for odd, source_ref in ((0, gate_ref), (1, up_ref)):

        @pl.when(own_ref[1] == odd)
        def _(source_ref=source_ref):
            for move in moves(source_ref):
                move.start()

    ids = ids_ref[...]
    onehot = [
        (ids[k : k + 1, :] == lax.broadcasted_iota(jnp.int32, (experts, tokens), 0)).astype(F32)
        for k in range(2)
    ]
    before = lax.broadcasted_iota(jnp.int32, (tokens, tokens), 0) < lax.broadcasted_iota(
        jnp.int32, (tokens, tokens), 1
    )
    before = before.astype(F32).astype(BF16)
    counts = [dot(h.astype(BF16), before) for h in onehot]
    counts[1] = counts[1] + jnp.sum(onehot[0], axis=1, keepdims=True)
    place = [jnp.sum(c * h, axis=0, keepdims=True).astype(jnp.int32) for c, h in zip(counts, onehot)]
    place = jnp.concatenate(place, axis=0)
    target_ref[...] = ids * capacity + place
    in_head = jnp.where(place < head, ids * head + place, -64)
    in_tail = jnp.where(place < head, -64, ids * 8 + place - head)
    pick = jnp.zeros((experts * head, tokens), F32)
    picks = [jnp.zeros((experts * 8, tokens), F32) for _ in range(per)]
    for k in range(2):
        pick = pick + selection(in_head[k : k + 1], 0, experts * head, 0).astype(F32)
        for q in range(per):
            picks[q] = picks[q] + selection(in_tail[k : k + 1], -q * tail, experts * 8, 0).astype(F32)
    pick = pick.astype(BF16)
    picks = jnp.concatenate(picks, axis=1).astype(BF16)
    copy.wait()
    gain_copy.wait()
    rows = rows_ref[...].astype(F32)
    mean_square = jnp.mean(rows * rows, axis=-1, keepdims=True)
    normed = (rows * lax.rsqrt(mean_square + EPSILON) * gain_ref[...]).astype(BF16)

    def tail_of(j):
        stack = [col(normed, per * j + q) for q in range(per)]
        return dot(picks, jnp.concatenate(stack, axis=0))

    put_message(
        out_ref, lambda c: dot(pick, col(normed, c)), tail_of, experts, head, tail, blocks
    )
    for odd, source_ref in ((0, gate_ref), (1, up_ref)):

        @pl.when(own_ref[1] == odd)
        def _(source_ref=source_ref):
            for move in moves(source_ref):
                move.wait()


def dispatch(own, rows, gain, ids, gate, up, cuts, experts, capacity):
    tokens = ids.shape[1]
    width = rows.shape[1]
    hbm = pl.BlockSpec(memory_space=pltpu.HBM)

    def kernel(*refs):
        dispatch_kernel(*refs, experts=experts, capacity=capacity)

    def held(array):
        return pltpu.with_memory_space_constraint(array, pltpu.HBM)

    return pl.pallas_call(
        kernel,
        in_specs=[pl.BlockSpec(memory_space=pltpu.SMEM), hbm, hbm, whole(), hbm, hbm],
        out_specs=[whole()] * (2 + len(cuts)),
        scratch_shapes=[
            pltpu.VMEM((tokens, width), BF16),
            pltpu.VMEM(gain.shape, F32),
            pltpu.SemaphoreType.DMA((2 + len(cuts),)),
        ],
        out_shape=[
            jax.ShapeDtypeStruct((experts, capacity * width // LANES, LANES), BF16),
            jax.ShapeDtypeStruct((2, tokens), jnp.int32),
            *(jax.ShapeDtypeStruct((cut, gate.shape[1]), BF16) for cut in cuts),
        ],
        compiler_params=pltpu.CompilerParams(vmem_limit_bytes=24 << 20),
        name="dispatch",
    )(own, held(rows), held(gain), ids, held(gate), held(up))


def expert_kernel(*refs, sources, far, peers, capacity, blocks):
    odd_ref, message_ref = refs[0], refs[1]
    count = sum(len(rows) for rows in far)
    given = list(refs[2 : count + 2])
    out_ref, rows_ref, hidden_ref = refs[count + 2 : count + 5]
    near, signals = list(refs[count + 5 : -1]), refs[-1]
    odd = odd_ref[0] == 1
    weights, copies = [], []
    used = 0
    for rows in far:
        pieces = [given.pop(0) for _ in rows]
        if rows == (0,):
            weights.append(pieces[0])
            copies.append([])
            continue
        if rows[0] < 0:
            weights.append(near.pop(0))
            copies.append([])
            at = 0
            for piece in pieces:
                weights[-1][at : at + piece.shape[0], :] = piece[...]
                at += piece.shape[0]
            continue
        weights.append(near.pop(0))
        moves, at = [], 0
        for piece, size in zip(pieces, rows):
            place = weights[-1].at[at : at + size, :]
            moves.append(pltpu.make_async_copy(piece, place, signals.at[used]))
            at += size
            used += 1
        copies.append(moves)
    waves = [[*s[0], *s[1]] for s in sources] + [[d for s in sources for d in s[2]]]

    def issue(wave):
        for w in wave:
            for move in copies[w]:
                move.start()

    def settle(wave):
        for w in wave:
            for move in copies[w]:
                move.wait()

    issue(waves[0])
    issue(waves[1])
    head, tail = split_rows(capacity)
    per = 8 // tail
    heads = peers * head
    for c in range(0, blocks, 2):
        both = message_ref[:, c * head : (c + 2) * head, :].astype(F32)
        for i in range(2):
            part = both[:, i * head : (i + 1) * head, :].reshape(heads, LANES)
            rows_ref[0:heads, (c + i) * LANES : (c + i + 1) * LANES] = part.astype(BF16)
    base = blocks * head
    slot = lax.broadcasted_iota(jnp.int32, (peers * tail, peers * 8), 0)
    lane = lax.broadcasted_iota(jnp.int32, (peers * tail, peers * 8), 1)
    gathers = [
        (lane == slot // tail * 8 + q * tail + slot % tail).astype(F32).astype(BF16)
        for q in range(per)
    ]
    for j in range(0, blocks // per, 2):
        both = message_ref[:, base + j * 8 : base + (j + 2) * 8, :].astype(F32)
        for i in range(2):
            part = both[:, i * 8 : (i + 1) * 8, :].reshape(peers * 8, LANES).astype(BF16)
            for q in range(per):
                c = per * (j + i) + q
                rows_ref[heads:, c * LANES : (c + 1) * LANES] = dot(gathers[q], part).astype(BF16)
    at = 0
    downs = []
    for n, (gates, ups, down_parts, swapped) in enumerate(sources):
        settle(waves[n])
        if n + 2 < len(waves):
            issue(waves[n + 2])
        rows = rows_ref[...]
        values = []
        for group in (gates, ups):
            value = None
            begin = 0
            for g in group:
                size = weights[g].shape[0]
                part = dot(rows[:, begin : begin + size], weights[g][...])
                value = part if value is None else value + part
                begin += size
            values.append(value)
        gate_value, up_value = values
        if swapped:
            gate_value, up_value = (
                jnp.where(odd, up_value, gate_value),
                jnp.where(odd, gate_value, up_value),
            )
        hidden = gate_value / (1.0 + jnp.exp(-gate_value)) * up_value
        hidden_ref[:, at : at + hidden.shape[1]] = hidden.astype(BF16)
        for d in down_parts:
            downs.append((at, d))
            at += weights[d].shape[0]
    settle(waves[-1])
    slot = lax.broadcasted_iota(jnp.int32, (peers * 8, peers * tail), 1)
    lane = lax.broadcasted_iota(jnp.int32, (peers * 8, peers * tail), 0)
    spreads = [
        (lane == slot // tail * 8 + q * tail + slot % tail).astype(F32).astype(BF16)
        for q in range(per)
    ]
    step = 2 * per
    for first in range(0, blocks, step):
        cols = slice(first * LANES, (first + step) * LANES)
        total = None
        for begin, d in downs:
            size = weights[d].shape[0]
            part = dot(hidden_ref[:, begin : begin + size], weights[d][:, cols])
            total = part if total is None else total + part
        for c in range(0, step, 2):
            pair = [col(total, c + i)[0:heads].reshape(peers, head, LANES) for i in range(2)]
            at_row = (first + c) * head
            out_ref[:, at_row : at_row + 2 * head, :] = jnp.concatenate(pair, axis=1).astype(BF16)
        last = total[heads:].astype(BF16)
        pair = []
        for i in range(2):
            spread = None
            for q in range(per):
                part = dot(spreads[q], col(last, per * i + q))
                spread = part if spread is None else spread + part
            pair.append(spread.reshape(peers, 8, LANES))
        at_row = base + first // per * 8
        out_ref[:, at_row : at_row + 16, :] = jnp.concatenate(pair, axis=1).astype(BF16)


def experts_apply(odd, message, matrices, direct, sources, capacity):
    peers, lines, _ = message.shape
    blocks = lines // capacity
    far = []
    for pieces, held in zip(matrices, direct):
        rows = tuple(p.shape[0] for p in pieces)
        far.append(rows if not held else (0,) if len(rows) == 1 else tuple(-r for r in rows))
    units = sum(sum(p.shape[0] for p in matrices[d]) for s in sources for d in s[2])

    def kernel(*refs):
        expert_kernel(*refs, sources=sources, far=far, peers=peers, capacity=capacity, blocks=blocks)

    operands, specs, scratch = [], [], []
    for pieces, rows in zip(matrices, far):
        if rows == (0,):
            operands.extend(pieces)
            specs.append(whole())
            continue
        scratch.append(pltpu.VMEM((abs(sum(rows)), pieces[0].shape[1]), BF16))
        if rows[0] < 0:
            operands.extend(pieces)
            specs.extend(whole() for _ in pieces)
            continue
        operands.extend(pltpu.with_memory_space_constraint(p, pltpu.HBM) for p in pieces)
        specs.extend(pl.BlockSpec(memory_space=pltpu.HBM) for _ in pieces)
    return pl.pallas_call(
        kernel,
        in_specs=[pl.BlockSpec(memory_space=pltpu.SMEM), whole(), *specs],
        out_specs=whole(),
        out_shape=jax.ShapeDtypeStruct(message.shape, BF16),
        scratch_shapes=[
            pltpu.VMEM((peers * capacity, blocks * LANES), BF16),
            pltpu.VMEM((peers * capacity, units), BF16),
            *scratch,
            pltpu.SemaphoreType.DMA((len(operands),)),
        ],
        compiler_params=pltpu.CompilerParams(vmem_limit_bytes=40 << 20),
        name="experts",
    )(odd, message, *operands)


def combine_kernel(
    message_ref, target_ref, far_ref, gain_ref, out_ref, mixed_ref, weight_ref, signal, *, capacity
):
    copy = pltpu.make_async_copy(far_ref, weight_ref, signal)
    copy.start()
    peers = message_ref.shape[0]
    tokens, width = out_ref.shape
    blocks = width // LANES
    head, tail = split_rows(capacity)
    per = 8 // tail
    heads = peers * head
    target = target_ref[...]
    peer = target // capacity
    place = target - peer * capacity
    in_head = jnp.where(place < head, peer * head + place, -64)
    in_tail = jnp.where(place < head, -64, peer * 8 + place - head)
    pick = [selection(in_head[:, k : k + 1], 0, heads, 1).astype(F32) for k in range(2)]
    pick = jnp.concatenate(pick, axis=0).astype(BF16)
    picks = []
    for q in range(per):
        both = [selection(in_tail[:, k : k + 1], -q * tail, peers * 8, 1).astype(F32) for k in range(2)]
        picks.append(jnp.concatenate(both, axis=0).astype(BF16))
    copy.wait()
    weight = [weight_ref[:, k : k + 1] for k in range(2)]
    base = blocks * head
    square = jnp.zeros((tokens, LANES), F32)
    for c in range(0, blocks, 2):
        both = message_ref[:, c * head : (c + 2) * head, :].astype(F32)
        for i in range(2):
            part = both[:, i * head : (i + 1) * head, :].reshape(heads, LANES).astype(BF16)
            j = (c + i) // per
            rest = message_ref[:, base + j // 2 * 16 : base + j // 2 * 16 + 16, :].astype(F32)
            rest = rest[:, j % 2 * 8 : j % 2 * 8 + 8, :].reshape(peers * 8, LANES).astype(BF16)
            rows = dot(pick, part) + dot(picks[(c + i) % per], rest)
            mixed = rows[:tokens] * weight[0] + rows[tokens:] * weight[1]
            mixed_ref[:, (c + i) * LANES : (c + i + 1) * LANES] = mixed
            square = square + mixed * mixed
    scale = lax.rsqrt(jnp.sum(square, axis=1, keepdims=True) * (1.0 / width) + EPSILON)
    out_ref[...] = (mixed_ref[...] * scale * gain_ref[...]).astype(BF16)


def combine(message, target, weight, gain, capacity):
    tokens = target.shape[0]
    width = gain.shape[1]

    def kernel(*refs):
        combine_kernel(*refs, capacity=capacity)

    return pl.pallas_call(
        kernel,
        in_specs=[whole(), whole(), pl.BlockSpec(memory_space=pltpu.HBM), whole()],
        out_specs=whole(),
        out_shape=jax.ShapeDtypeStruct((tokens, width), BF16),
        scratch_shapes=[
            pltpu.VMEM((tokens, width), F32),
            pltpu.VMEM(weight.shape, F32),
            pltpu.SemaphoreType.DMA,
        ],
        compiler_params=pltpu.CompilerParams(vmem_limit_bytes=24 << 20),
        name="combine",
    )(message, target, pltpu.with_memory_space_constraint(weight, pltpu.HBM), gain)


def conv_kernel(rows_ref, carried_ref, taps_ref, gain_ref, weight_ref, out_ref, line_ref, sum_ref):
    block, width = rows_ref.shape
    blocks = width // LANES
    reach = taps_ref.shape[0] - 1
    halo = line_ref.shape[1] - block
    step = pl.program_id(0)

    @pl.when(step == 0)
    def _():
        for c in range(blocks):
            line_ref[c, 0:halo, :] = col(carried_ref, c).astype(F32)

    @pl.when(step > 0)
    def _():
        for c in range(blocks):
            line_ref[c, 0:halo, :] = line_ref[c, block : block + halo, :]

    for c in range(blocks):
        line_ref[c, halo:, :] = col(rows_ref, c).astype(F32)

    strip = 64

    def column(c, square):
        parts = []
        for first in range(0, block, strip):
            total = jnp.zeros((strip, LANES), F32)
            for k in range(reach + 1):
                at = first + halo - reach + k
                total = total + line_ref[c, at : at + strip, :] * taps_ref[k, pl.ds(c, 1), :]
            sum_ref[c, first : first + strip, :] = total
            parts.append(total * total)
        return square + jnp.concatenate(parts, axis=0)

    square = lax.fori_loop(0, blocks, column, jnp.zeros((block, LANES), F32))
    scale = lax.rsqrt(jnp.sum(square, axis=1, keepdims=True) * (1.0 / width) + EPSILON)
    result = jnp.zeros((block, out_ref.shape[1]), F32)
    for c in range(0, blocks, 4):
        group = []
        for i in range(4):
            value = sum_ref[c + i] * scale * col(gain_ref, c + i)
            group.append((value / (1.0 + jnp.exp(-value))).astype(BF16))
        part = jnp.concatenate(group, axis=1)
        result = result + dot(part, weight_ref[c * LANES : (c + 4) * LANES, :])
    out_ref[...] = result.astype(BF16)


def conv_module(rows, carried, taps, gain, weight, block=128):
    count, width = rows.shape
    blocks = width // LANES
    halo = carried.shape[0]
    return pl.pallas_call(
        conv_kernel,
        grid=(count // block,),
        in_specs=[
            pl.BlockSpec((block, width), lambda i: (i, 0)),
            pl.BlockSpec((halo, width), lambda i: (0, 0)),
            pl.BlockSpec((taps.shape[0], blocks, LANES), lambda i: (0, 0, 0)),
            pl.BlockSpec((1, width), lambda i: (0, 0)),
            pl.BlockSpec(weight.shape, lambda i: (0, 0)),
        ],
        out_specs=pl.BlockSpec((block, weight.shape[1]), lambda i: (i, 0)),
        out_shape=jax.ShapeDtypeStruct((count, weight.shape[1]), BF16),
        scratch_shapes=[
            pltpu.VMEM((blocks, block + halo, LANES), F32),
            pltpu.VMEM((blocks, block, LANES), F32),
        ],
        compiler_params=pltpu.CompilerParams(vmem_limit_bytes=24 << 20),
        name="conv",
    )(rows, carried, taps.reshape(taps.shape[0], blocks, LANES), gain, weight)


EP = "ep"
GRP_EP = ("grp", "ep")
GRP_EP_TP = ("grp", "ep", "tp")
HALO = 32


def run(
    conv_input,
    conv_taps,
    conv_gain,
    conv_weight,
    moe_input,
    moe_gain,
    expert_ids,
    route_weights,
    gate_weight,
    up_weight,
    down_weight,
    post_gain,
):
    quarters = lax.axis_size("tp")
    ep_count = lax.axis_size(EP)
    width = moe_input.shape[1]
    tokens = moe_input.shape[0] // quarters
    capacity = 2 * tokens // ep_count
    own = lax.axis_index("tp").astype(jnp.int32)

    odd = (lax.axis_index("grp") % 2).astype(jnp.int32)

    right = [(i, (i + 1) % quarters) for i in range(quarters)]
    left = [(i, (i - 1) % quarters) for i in range(quarters)]
    across = [(i, i ^ 1) for i in range(lax.axis_size("grp"))]
    gate, up, down = gate_weight[0], up_weight[0], down_weight[0]
    half, part = gate.shape[0] // 2, down.shape[0] * 7 // 8

    def send(array, pairs):
        return lax.ppermute(array, "tp", pairs)

    def swap(array):
        return lax.ppermute(array, "grp", across)

    down_r = send(down, right)
    turn = ep_count - ep_count // 4 - 1
    order = [(turn - i) % ep_count for i in range(ep_count)]

    def exchange(array):
        return lax.all_to_all(array, EP, 0, 0, axis_index_groups=[order], tiled=True)

    own_ids = lax.dynamic_slice_in_dim(expert_ids, own * tokens, tokens, 0).T
    own_ids = (turn + ep_count - own_ids) % ep_count
    message, target, mine_a, mine_b = dispatch(
        jnp.stack([own, odd]),
        moe_input,
        moe_gain.reshape(1, width),
        own_ids,
        gate,
        up,
        (half, gate.shape[0] - half),
        ep_count,
        capacity,
    )
    mine_a_l, mine_b_l = send(mine_a, left), send(mine_b, left)
    arrived = exchange(message)
    mine_a_r, mine_b_r = send(mine_a, right), send(mine_b, right)
    other_a_l, mine_a_far = swap(mine_a_l), send(mine_a_l, left)
    down_l = send(down, left)
    pairs = [(i, i + 1) for i in range(ep_count - 1)]
    carried = lax.ppermute(conv_input[conv_input.shape[0] - HALO :], EP, pairs)
    other_b_l, mine_b_far = swap(mine_b_l), send(mine_b_l, left)
    down_a_far = send(down_r[:part], right)
    other_a_r = swap(mine_a_r)
    other_b_r = swap(mine_b_r)
    other_a_far = swap(mine_a_far)
    other_b_far, down_b_far = send(other_b_r, right), send(down_l[part:], left)

    conv_out = conv_module(conv_input, carried, conv_taps, conv_gain.reshape(1, width), conv_weight)

    matrices = [
        *((gate,), (up,), (down,)),
        *((mine_a_r, mine_b_r), (other_a_r, other_b_r), (down_r,)),
        *((mine_a_l, mine_b_l), (other_a_l, other_b_l), (down_l,)),
        *((mine_a_far,), (mine_b_far,), (other_a_far,), (other_b_far,), (down_a_far, down_b_far)),
    ]
    sources = (
        ((0,), (1,), (2,), False),
        ((6,), (7,), (8,), True),
        ((3,), (4,), (5,), True),
        ((9, 10), (11, 12), (13,), True),
    )
    direct = tuple(n in (11, 12, 13) for n in range(len(matrices)))
    results = experts_apply(odd.reshape(1), arrived, matrices, direct, sources, capacity)
    returned = exchange(results)
    own_weights = lax.dynamic_slice_in_dim(route_weights, own * tokens, tokens, 0)
    moe_out = combine(returned, target.T, own_weights, post_gain.reshape(1, width), capacity)
    return (conv_out, moe_out)


def solution(mesh):
    return jax.shard_map(
        run,
        mesh=mesh,
        in_specs=(
            P(GRP_EP, None),
            P(),
            P(),
            P(None, "tp"),
            P(GRP_EP, None),
            P(),
            P(GRP_EP, None),
            P(GRP_EP, None),
            P(EP, None, "tp"),
            P(EP, None, "tp"),
            P(EP, "tp", None),
            P(),
        ),
        out_specs=(P(GRP_EP, "tp"), P(GRP_EP_TP, None)),
        check_vma=False,
    )
```

```python
import jax
import jax.numpy as jnp
from jax import lax
from jax.experimental import pallas as pl
from jax.experimental.pallas import tpu as pltpu
from jax.sharding import PartitionSpec as P

EPSILON = 1e-06
LANES = 128
F32 = jnp.float32
BF16 = jnp.bfloat16


def whole():
    return pl.BlockSpec(memory_space=pltpu.VMEM)


def dot(a, b):
    return jnp.dot(a, b, preferred_element_type=F32)


def split_rows(capacity):
    main = capacity // 8 * 8
    return main, capacity - main


def col(ref_or_value, c):
    return ref_or_value[:, c * LANES : (c + 1) * LANES]


def selection(index, first, count, dim):
    shape = (count, index.shape[1]) if dim == 0 else (index.shape[0], count)
    return index == first + lax.broadcasted_iota(jnp.int32, shape, dim)


def put_message(out_ref, head_of, tail_of, peers, head, tail, blocks):
    for c in range(0, blocks, 2):
        pair = [head_of(c + i).reshape(peers, head, LANES) for i in range(2)]
        out_ref[:, c * head : (c + 2) * head, :] = jnp.concatenate(pair, axis=1).astype(BF16)
    per = 8 // tail
    base = blocks * head
    for j in range(0, blocks // per, 2):
        pair = [tail_of(j + i).reshape(peers, 8, LANES) for i in range(2)]
        out_ref[:, base + j * 8 : base + (j + 2) * 8, :] = jnp.concatenate(pair, axis=1).astype(BF16)


def dispatch_kernel(
    own_ref,
    all_ref,
    far_gain_ref,
    ids_ref,
    gate_ref,
    up_ref,
    out_ref,
    target_ref,
    *rest,
    turn,
    experts,
    capacity,
):
    picked, (rows_ref, gain_ref, signals) = rest[:-3], rest[-3:]
    tokens, width = rows_ref.shape
    blocks = width // LANES
    head, tail = split_rows(capacity)
    per = 8 // tail
    copy = pltpu.make_async_copy(
        all_ref.at[pl.ds(pl.multiple_of(own_ref[0] * tokens, 16), tokens), :],
        rows_ref,
        signals.at[0],
    )
    copy.start()
    gain_copy = pltpu.make_async_copy(far_gain_ref, gain_ref, signals.at[1])
    gain_copy.start()

    def moves(source_ref):
        at = 0
        for i, ref in enumerate(picked):
            rows = source_ref.at[at : at + ref.shape[0], :]
            yield pltpu.make_async_copy(rows, ref, signals.at[2 + i])
            at += ref.shape[0]

    for odd, source_ref in ((0, gate_ref), (1, up_ref)):

        @pl.when(own_ref[1] == odd)
        def _(source_ref=source_ref):
            for move in moves(source_ref):
                move.start()

    ids = turn - ids_ref[...]
    ids = jnp.where(ids < 0, ids + experts, ids)
    onehot = [
        (ids[k : k + 1, :] == lax.broadcasted_iota(jnp.int32, (experts, tokens), 0)).astype(F32)
        for k in range(2)
    ]
    before = lax.broadcasted_iota(jnp.int32, (tokens, tokens), 0) < lax.broadcasted_iota(
        jnp.int32, (tokens, tokens), 1
    )
    before = before.astype(F32).astype(BF16)
    counts = [dot(h.astype(BF16), before) for h in onehot]
    counts[1] = counts[1] + jnp.sum(onehot[0], axis=1, keepdims=True)
    place = [jnp.sum(c * h, axis=0, keepdims=True).astype(jnp.int32) for c, h in zip(counts, onehot)]
    place = jnp.concatenate(place, axis=0)
    target_ref[...] = ids * capacity + place
    in_head = jnp.where(place < head, ids * head + place, -64)
    in_tail = jnp.where(place < head, -64, ids * 8 + place - head)
    pick = jnp.zeros((experts * head, tokens), F32)
    picks = [jnp.zeros((experts * 8, tokens), F32) for _ in range(per)]
    for k in range(2):
        pick = pick + selection(in_head[k : k + 1], 0, experts * head, 0).astype(F32)
        for q in range(per):
            picks[q] = picks[q] + selection(in_tail[k : k + 1], -q * tail, experts * 8, 0).astype(F32)
    pick = pick.astype(BF16)
    picks = jnp.concatenate(picks, axis=1).astype(BF16)
    copy.wait()
    gain_copy.wait()
    rows = rows_ref[...].astype(F32)
    mean_square = jnp.mean(rows * rows, axis=-1, keepdims=True)
    normed = (rows * lax.rsqrt(mean_square + EPSILON) * gain_ref[...]).astype(BF16)

    def tail_of(j):
        stack = [col(normed, per * j + q) for q in range(per)]
        return dot(picks, jnp.concatenate(stack, axis=0))

    put_message(
        out_ref, lambda c: dot(pick, col(normed, c)), tail_of, experts, head, tail, blocks
    )
    for odd, source_ref in ((0, gate_ref), (1, up_ref)):

        @pl.when(own_ref[1] == odd)
        def _(source_ref=source_ref):
            for move in moves(source_ref):
                move.wait()


def dispatch(own, rows, gain, ids, gate, up, cuts, turn, experts, capacity):
    tokens = ids.shape[1]
    width = rows.shape[1]
    hbm = pl.BlockSpec(memory_space=pltpu.HBM)

    def kernel(*refs):
        dispatch_kernel(*refs, turn=turn, experts=experts, capacity=capacity)

    def held(array):
        return pltpu.with_memory_space_constraint(array, pltpu.HBM)

    return pl.pallas_call(
        kernel,
        in_specs=[pl.BlockSpec(memory_space=pltpu.SMEM), hbm, hbm, whole(), hbm, hbm],
        out_specs=[whole()] * (2 + len(cuts)),
        scratch_shapes=[
            pltpu.VMEM((tokens, width), BF16),
            pltpu.VMEM(gain.shape, F32),
            pltpu.SemaphoreType.DMA((2 + len(cuts),)),
        ],
        out_shape=[
            jax.ShapeDtypeStruct((experts, capacity * width // LANES, LANES), BF16),
            jax.ShapeDtypeStruct((2, tokens), jnp.int32),
            *(jax.ShapeDtypeStruct((cut, gate.shape[1]), BF16) for cut in cuts),
        ],
        compiler_params=pltpu.CompilerParams(vmem_limit_bytes=24 << 20),
        name="dispatch",
    )(own, held(rows), held(gain), ids, held(gate), held(up))


def expert_kernel(*refs, sources, far, peers, capacity, blocks):
    odd_ref, message_ref = refs[0], refs[1]
    count = sum(len(rows) for rows in far)
    given = list(refs[2 : count + 2])
    out_ref, rows_ref, hidden_ref = refs[count + 2 : count + 5]
    near, signals = list(refs[count + 5 : -1]), refs[-1]
    odd = odd_ref[0] == 1
    weights, copies = [], []
    used = 0
    for rows in far:
        pieces = [given.pop(0) for _ in rows]
        if rows == (0,):
            weights.append(pieces[0])
            copies.append([])
            continue
        if rows[0] < 0:
            weights.append(near.pop(0))
            copies.append([])
            at = 0
            for piece in pieces:
                weights[-1][at : at + piece.shape[0], :] = piece[...]
                at += piece.shape[0]
            continue
        weights.append(near.pop(0))
        moves, at = [], 0
        for piece, size in zip(pieces, rows):
            place = weights[-1].at[at : at + size, :]
            moves.append(pltpu.make_async_copy(piece, place, signals.at[used]))
            at += size
            used += 1
        copies.append(moves)
    waves = [[*s[0], *s[1]] for s in sources] + [[d for s in sources for d in s[2]]]

    def issue(wave):
        for w in wave:
            for move in copies[w]:
                move.start()

    def settle(wave):
        for w in wave:
            for move in copies[w]:
                move.wait()

    issue(waves[0])
    issue(waves[1])
    head, tail = split_rows(capacity)
    per = 8 // tail
    heads = peers * head
    for c in range(0, blocks, 2):
        both = message_ref[:, c * head : (c + 2) * head, :].astype(F32)
        for i in range(2):
            part = both[:, i * head : (i + 1) * head, :].reshape(heads, LANES)
            rows_ref[0:heads, (c + i) * LANES : (c + i + 1) * LANES] = part.astype(BF16)
    base = blocks * head
    slot = lax.broadcasted_iota(jnp.int32, (peers * tail, peers * 8), 0)
    lane = lax.broadcasted_iota(jnp.int32, (peers * tail, peers * 8), 1)
    gathers = [
        (lane == slot // tail * 8 + q * tail + slot % tail).astype(F32).astype(BF16)
        for q in range(per)
    ]
    for j in range(0, blocks // per, 2):
        both = message_ref[:, base + j * 8 : base + (j + 2) * 8, :].astype(F32)
        for i in range(2):
            part = both[:, i * 8 : (i + 1) * 8, :].reshape(peers * 8, LANES).astype(BF16)
            for q in range(per):
                c = per * (j + i) + q
                rows_ref[heads:, c * LANES : (c + 1) * LANES] = dot(gathers[q], part).astype(BF16)
    at = 0
    downs = []
    for n, (gates, ups, down_parts, swapped) in enumerate(sources):
        settle(waves[n])
        if n + 2 < len(waves):
            issue(waves[n + 2])
        rows = rows_ref[...]
        values = []
        for group in (gates, ups):
            value = None
            begin = 0
            for g in group:
                size = weights[g].shape[0]
                part = dot(rows[:, begin : begin + size], weights[g][...])
                value = part if value is None else value + part
                begin += size
            values.append(value)
        gate_value, up_value = values
        if swapped:
            gate_value, up_value = (
                jnp.where(odd, up_value, gate_value),
                jnp.where(odd, gate_value, up_value),
            )
        hidden = gate_value / (1.0 + jnp.exp(-gate_value)) * up_value
        hidden_ref[:, at : at + hidden.shape[1]] = hidden.astype(BF16)
        for d in down_parts:
            downs.append((at, d))
            at += weights[d].shape[0]
    settle(waves[-1])
    slot = lax.broadcasted_iota(jnp.int32, (peers * 8, peers * tail), 1)
    lane = lax.broadcasted_iota(jnp.int32, (peers * 8, peers * tail), 0)
    spreads = [
        (lane == slot // tail * 8 + q * tail + slot % tail).astype(F32).astype(BF16)
        for q in range(per)
    ]
    step = 2 * per
    for first in range(0, blocks, step):
        cols = slice(first * LANES, (first + step) * LANES)
        total = None
        for begin, d in downs:
            size = weights[d].shape[0]
            part = dot(hidden_ref[:, begin : begin + size], weights[d][:, cols])
            total = part if total is None else total + part
        for c in range(0, step, 2):
            pair = [col(total, c + i)[0:heads].reshape(peers, head, LANES) for i in range(2)]
            at_row = (first + c) * head
            out_ref[:, at_row : at_row + 2 * head, :] = jnp.concatenate(pair, axis=1).astype(BF16)
        last = total[heads:].astype(BF16)
        pair = []
        for i in range(2):
            spread = None
            for q in range(per):
                part = dot(spreads[q], col(last, per * i + q))
                spread = part if spread is None else spread + part
            pair.append(spread.reshape(peers, 8, LANES))
        at_row = base + first // per * 8
        out_ref[:, at_row : at_row + 16, :] = jnp.concatenate(pair, axis=1).astype(BF16)


def experts_apply(odd, message, matrices, direct, sources, capacity):
    peers, lines, _ = message.shape
    blocks = lines // capacity
    far = []
    for pieces, held in zip(matrices, direct):
        rows = tuple(p.shape[0] for p in pieces)
        far.append(rows if not held else (0,) if len(rows) == 1 else tuple(-r for r in rows))
    units = sum(sum(p.shape[0] for p in matrices[d]) for s in sources for d in s[2])

    def kernel(*refs):
        expert_kernel(*refs, sources=sources, far=far, peers=peers, capacity=capacity, blocks=blocks)

    operands, specs, scratch = [], [], []
    for pieces, rows in zip(matrices, far):
        if rows == (0,):
            operands.extend(pieces)
            specs.append(whole())
            continue
        scratch.append(pltpu.VMEM((abs(sum(rows)), pieces[0].shape[1]), BF16))
        if rows[0] < 0:
            operands.extend(pieces)
            specs.extend(whole() for _ in pieces)
            continue
        operands.extend(pltpu.with_memory_space_constraint(p, pltpu.HBM) for p in pieces)
        specs.extend(pl.BlockSpec(memory_space=pltpu.HBM) for _ in pieces)
    return pl.pallas_call(
        kernel,
        in_specs=[pl.BlockSpec(memory_space=pltpu.SMEM), whole(), *specs],
        out_specs=whole(),
        out_shape=jax.ShapeDtypeStruct(message.shape, BF16),
        scratch_shapes=[
            pltpu.VMEM((peers * capacity, blocks * LANES), BF16),
            pltpu.VMEM((peers * capacity, units), BF16),
            *scratch,
            pltpu.SemaphoreType.DMA((len(operands),)),
        ],
        compiler_params=pltpu.CompilerParams(vmem_limit_bytes=40 << 20),
        name="experts",
    )(odd, message, *operands)


def combine_kernel(
    message_ref, target_ref, far_ref, gain_ref, out_ref, mixed_ref, weight_ref, signal, *, capacity
):
    copy = pltpu.make_async_copy(far_ref, weight_ref, signal)
    copy.start()
    peers = message_ref.shape[0]
    tokens, width = out_ref.shape
    blocks = width // LANES
    head, tail = split_rows(capacity)
    per = 8 // tail
    heads = peers * head
    target = target_ref[...]
    peer = target // capacity
    place = target - peer * capacity
    in_head = jnp.where(place < head, peer * head + place, -64)
    in_tail = jnp.where(place < head, -64, peer * 8 + place - head)
    pick = [selection(in_head[:, k : k + 1], 0, heads, 1).astype(F32) for k in range(2)]
    pick = jnp.concatenate(pick, axis=0).astype(BF16)
    picks = []
    for q in range(per):
        both = [selection(in_tail[:, k : k + 1], -q * tail, peers * 8, 1).astype(F32) for k in range(2)]
        picks.append(jnp.concatenate(both, axis=0).astype(BF16))
    copy.wait()
    weight = [weight_ref[:, k : k + 1] for k in range(2)]
    base = blocks * head
    square = jnp.zeros((tokens, LANES), F32)
    for c in range(0, blocks, 2):
        both = message_ref[:, c * head : (c + 2) * head, :].astype(F32)
        for i in range(2):
            part = both[:, i * head : (i + 1) * head, :].reshape(heads, LANES).astype(BF16)
            j = (c + i) // per
            rest = message_ref[:, base + j // 2 * 16 : base + j // 2 * 16 + 16, :].astype(F32)
            rest = rest[:, j % 2 * 8 : j % 2 * 8 + 8, :].reshape(peers * 8, LANES).astype(BF16)
            rows = dot(pick, part) + dot(picks[(c + i) % per], rest)
            mixed = rows[:tokens] * weight[0] + rows[tokens:] * weight[1]
            mixed_ref[:, (c + i) * LANES : (c + i + 1) * LANES] = mixed
            square = square + mixed * mixed
    scale = lax.rsqrt(jnp.sum(square, axis=1, keepdims=True) * (1.0 / width) + EPSILON)
    out_ref[...] = (mixed_ref[...] * scale * gain_ref[...]).astype(BF16)


def combine(message, target, weight, gain, capacity):
    tokens = target.shape[0]
    width = gain.shape[1]

    def kernel(*refs):
        combine_kernel(*refs, capacity=capacity)

    return pl.pallas_call(
        kernel,
        in_specs=[whole(), whole(), pl.BlockSpec(memory_space=pltpu.HBM), whole()],
        out_specs=whole(),
        out_shape=jax.ShapeDtypeStruct((tokens, width), BF16),
        scratch_shapes=[
            pltpu.VMEM((tokens, width), F32),
            pltpu.VMEM(weight.shape, F32),
            pltpu.SemaphoreType.DMA,
        ],
        compiler_params=pltpu.CompilerParams(vmem_limit_bytes=24 << 20),
        name="combine",
    )(message, target, pltpu.with_memory_space_constraint(weight, pltpu.HBM), gain)


def conv_kernel(rows_ref, carried_ref, taps_ref, gain_ref, weight_ref, out_ref, line_ref, sum_ref):
    block, width = rows_ref.shape
    blocks = width // LANES
    reach = taps_ref.shape[0] - 1
    halo = line_ref.shape[1] - block
    step = pl.program_id(0)

    @pl.when(step == 0)
    def _():
        for c in range(blocks):
            line_ref[c, 0:halo, :] = col(carried_ref, c).astype(F32)

    @pl.when(step > 0)
    def _():
        for c in range(blocks):
            line_ref[c, 0:halo, :] = line_ref[c, block : block + halo, :]

    for c in range(blocks):
        line_ref[c, halo:, :] = col(rows_ref, c).astype(F32)

    strip = 64

    def column(c, square):
        parts = []
        for first in range(0, block, strip):
            total = jnp.zeros((strip, LANES), F32)
            for k in range(reach + 1):
                at = first + halo - reach + k
                total = total + line_ref[c, at : at + strip, :] * taps_ref[k, pl.ds(c, 1), :]
            sum_ref[c, first : first + strip, :] = total
            parts.append(total * total)
        return square + jnp.concatenate(parts, axis=0)

    square = lax.fori_loop(0, blocks, column, jnp.zeros((block, LANES), F32))
    scale = lax.rsqrt(jnp.sum(square, axis=1, keepdims=True) * (1.0 / width) + EPSILON)
    result = jnp.zeros((block, out_ref.shape[1]), F32)
    for c in range(0, blocks, 4):
        group = []
        for i in range(4):
            value = sum_ref[c + i] * scale * col(gain_ref, c + i)
            group.append((value / (1.0 + jnp.exp(-value))).astype(BF16))
        part = jnp.concatenate(group, axis=1)
        result = result + dot(part, weight_ref[c * LANES : (c + 4) * LANES, :])
    out_ref[...] = result.astype(BF16)


def conv_module(rows, carried, taps, gain, weight, block=128):
    count, width = rows.shape
    blocks = width // LANES
    halo = carried.shape[0]
    return pl.pallas_call(
        conv_kernel,
        grid=(count // block,),
        in_specs=[
            pl.BlockSpec((block, width), lambda i: (i, 0)),
            pl.BlockSpec((halo, width), lambda i: (0, 0)),
            pl.BlockSpec((taps.shape[0], blocks, LANES), lambda i: (0, 0, 0)),
            pl.BlockSpec((1, width), lambda i: (0, 0)),
            pl.BlockSpec(weight.shape, lambda i: (0, 0)),
        ],
        out_specs=pl.BlockSpec((block, weight.shape[1]), lambda i: (i, 0)),
        out_shape=jax.ShapeDtypeStruct((count, weight.shape[1]), BF16),
        scratch_shapes=[
            pltpu.VMEM((blocks, block + halo, LANES), F32),
            pltpu.VMEM((blocks, block, LANES), F32),
        ],
        compiler_params=pltpu.CompilerParams(vmem_limit_bytes=24 << 20),
        name="conv",
    )(rows, carried, taps.reshape(taps.shape[0], blocks, LANES), gain, weight)


EP = "ep"
GRP_EP = ("grp", "ep")
GRP_EP_TP = ("grp", "ep", "tp")
HALO = 32


def run(
    conv_input,
    conv_taps,
    conv_gain,
    conv_weight,
    moe_input,
    moe_gain,
    expert_ids,
    route_weights,
    gate_weight,
    up_weight,
    down_weight,
    post_gain,
):
    quarters = lax.axis_size("tp")
    ep_count = lax.axis_size(EP)
    width = moe_input.shape[1]
    tokens = moe_input.shape[0] // quarters
    capacity = 2 * tokens // ep_count
    own = lax.axis_index("tp").astype(jnp.int32)

    odd = (lax.axis_index("grp") % 2).astype(jnp.int32)

    right = [(i, (i + 1) % quarters) for i in range(quarters)]
    left = [(i, (i - 1) % quarters) for i in range(quarters)]
    across = [(i, i ^ 1) for i in range(lax.axis_size("grp"))]
    gate, up, down = gate_weight[0], up_weight[0], down_weight[0]
    half, part = gate.shape[0] // 2, down.shape[0] * 7 // 8

    def send(array, pairs):
        return lax.ppermute(array, "tp", pairs)

    def swap(array):
        return lax.ppermute(array, "grp", across)

    down_r = send(down, right)
    turn = ep_count - ep_count // 4 - 1
    order = [(turn - i) % ep_count for i in range(ep_count)]

    def exchange(array):
        return lax.all_to_all(array, EP, 0, 0, axis_index_groups=[order], tiled=True)

    own_ids = lax.dynamic_slice_in_dim(expert_ids, own * tokens, tokens, 0).T
    message, target, mine_a, mine_b = dispatch(
        jnp.stack([own, odd]),
        moe_input,
        moe_gain.reshape(1, width),
        own_ids,
        gate,
        up,
        (half, gate.shape[0] - half),
        turn,
        ep_count,
        capacity,
    )
    mine_a_l, mine_b_l = send(mine_a, left), send(mine_b, left)
    arrived = exchange(message)
    other_a_l, mine_a_far = swap(mine_a_l), send(mine_a_l, left)
    mine_a_r, mine_b_r = send(mine_a, right), send(mine_b, right)
    down_l = send(down, left)
    pairs = [(i, i + 1) for i in range(ep_count - 1)]
    carried = lax.ppermute(conv_input[conv_input.shape[0] - HALO :], EP, pairs)
    other_b_l, mine_b_far = swap(mine_b_l), send(mine_b_l, left)
    down_a_far = send(down_r[:part], right)
    other_a_r = swap(mine_a_r)
    other_b_r = swap(mine_b_r)
    other_a_far = swap(mine_a_far)
    other_b_far, down_b_far = send(other_b_r, right), send(down_l[part:], left)

    conv_out = conv_module(conv_input, carried, conv_taps, conv_gain.reshape(1, width), conv_weight)

    matrices = [
        *((gate,), (up,), (down,)),
        *((mine_a_r, mine_b_r), (other_a_r, other_b_r), (down_r,)),
        *((mine_a_l, mine_b_l), (other_a_l, other_b_l), (down_l,)),
        *((mine_a_far,), (mine_b_far,), (other_a_far,), (other_b_far,), (down_a_far, down_b_far)),
    ]
    sources = (
        ((0,), (1,), (2,), False),
        ((6,), (7,), (8,), True),
        ((3,), (4,), (5,), True),
        ((9, 10), (11, 12), (13,), True),
    )
    direct = tuple(n in (11, 12, 13) for n in range(len(matrices)))
    results = experts_apply(odd.reshape(1), arrived, matrices, direct, sources, capacity)
    returned = exchange(results)
    own_weights = lax.dynamic_slice_in_dim(route_weights, own * tokens, tokens, 0)
    moe_out = combine(returned, target.T, own_weights, post_gain.reshape(1, width), capacity)
    return (conv_out, moe_out)


def solution(mesh):
    return jax.shard_map(
        run,
        mesh=mesh,
        in_specs=(
            P(GRP_EP, None),
            P(),
            P(),
            P(None, "tp"),
            P(GRP_EP, None),
            P(),
            P(GRP_EP, None),
            P(GRP_EP, None),
            P(EP, None, "tp"),
            P(EP, None, "tp"),
            P(EP, "tp", None),
            P(),
        ),
        out_specs=(P(GRP_EP, "tp"), P(GRP_EP_TP, None)),
        check_vma=False,
    )
```

```python
import jax
import jax.numpy as jnp
from jax import lax
from jax.experimental import pallas as pl
from jax.experimental.pallas import tpu as pltpu
from jax.sharding import PartitionSpec as P

EPSILON = 1e-06
LANES = 128
F32 = jnp.float32
BF16 = jnp.bfloat16


def whole():
    return pl.BlockSpec(memory_space=pltpu.VMEM)


def dot(a, b):
    return jnp.dot(a, b, preferred_element_type=F32)


def split_rows(capacity):
    main = capacity // 8 * 8
    return main, capacity - main


def col(ref_or_value, c):
    return ref_or_value[:, c * LANES : (c + 1) * LANES]


def selection(index, first, count, dim):
    shape = (count, index.shape[1]) if dim == 0 else (index.shape[0], count)
    return index == first + lax.broadcasted_iota(jnp.int32, shape, dim)


def put_message(out_ref, head_of, tail_of, peers, head, tail, blocks):
    for c in range(0, blocks, 2):
        pair = [head_of(c + i).reshape(peers, head, LANES) for i in range(2)]
        out_ref[:, c * head : (c + 2) * head, :] = jnp.concatenate(pair, axis=1).astype(BF16)
    per = 8 // tail
    base = blocks * head
    for j in range(0, blocks // per, 2):
        pair = [tail_of(j + i).reshape(peers, 8, LANES) for i in range(2)]
        out_ref[:, base + j * 8 : base + (j + 2) * 8, :] = jnp.concatenate(pair, axis=1).astype(BF16)


def dispatch_kernel(
    own_ref,
    all_ref,
    far_gain_ref,
    ids_ref,
    gate_ref,
    up_ref,
    out_ref,
    target_ref,
    *rest,
    turn,
    experts,
    capacity,
):
    picked, (rows_ref, gain_ref, signals) = rest[:-3], rest[-3:]
    tokens, width = rows_ref.shape
    blocks = width // LANES
    head, tail = split_rows(capacity)
    per = 8 // tail
    copy = pltpu.make_async_copy(
        all_ref.at[pl.ds(pl.multiple_of(own_ref[0] * tokens, 16), tokens), :],
        rows_ref,
        signals.at[0],
    )
    copy.start()
    gain_copy = pltpu.make_async_copy(far_gain_ref, gain_ref, signals.at[1])
    gain_copy.start()

    def moves(source_ref):
        at = 0
        for i, ref in enumerate(picked):
            rows = source_ref.at[at : at + ref.shape[0], :]
            yield pltpu.make_async_copy(rows, ref, signals.at[2 + i])
            at += ref.shape[0]

    for odd, source_ref in ((0, gate_ref), (1, up_ref)):

        @pl.when(own_ref[1] == odd)
        def _(source_ref=source_ref):
            for move in moves(source_ref):
                move.start()

    ids = turn - ids_ref[...]
    ids = jnp.where(ids < 0, ids + experts, ids)
    onehot = [
        (ids[k : k + 1, :] == lax.broadcasted_iota(jnp.int32, (experts, tokens), 0)).astype(F32)
        for k in range(2)
    ]
    before = lax.broadcasted_iota(jnp.int32, (tokens, tokens), 0) < lax.broadcasted_iota(
        jnp.int32, (tokens, tokens), 1
    )
    before = before.astype(F32).astype(BF16)
    counts = [dot(h.astype(BF16), before) for h in onehot]
    counts[1] = counts[1] + jnp.sum(onehot[0], axis=1, keepdims=True)
    place = [jnp.sum(c * h, axis=0, keepdims=True).astype(jnp.int32) for c, h in zip(counts, onehot)]
    place = jnp.concatenate(place, axis=0)
    target_ref[...] = ids * capacity + place
    in_head = jnp.where(place < head, ids * head + place, -64)
    in_tail = jnp.where(place < head, -64, ids * 8 + place - head)
    pick = jnp.zeros((experts * head, tokens), F32)
    picks = [jnp.zeros((experts * 8, tokens), F32) for _ in range(per)]
    for k in range(2):
        pick = pick + selection(in_head[k : k + 1], 0, experts * head, 0).astype(F32)
        for q in range(per):
            picks[q] = picks[q] + selection(in_tail[k : k + 1], -q * tail, experts * 8, 0).astype(F32)
    pick = pick.astype(BF16)
    picks = jnp.concatenate(picks, axis=1).astype(BF16)
    copy.wait()
    gain_copy.wait()
    rows = rows_ref[...].astype(F32)
    mean_square = jnp.mean(rows * rows, axis=-1, keepdims=True)
    normed = (rows * lax.rsqrt(mean_square + EPSILON) * gain_ref[...]).astype(BF16)

    def tail_of(j):
        stack = [col(normed, per * j + q) for q in range(per)]
        return dot(picks, jnp.concatenate(stack, axis=0))

    put_message(
        out_ref, lambda c: dot(pick, col(normed, c)), tail_of, experts, head, tail, blocks
    )
    for odd, source_ref in ((0, gate_ref), (1, up_ref)):

        @pl.when(own_ref[1] == odd)
        def _(source_ref=source_ref):
            for move in moves(source_ref):
                move.wait()


def dispatch(own, rows, gain, ids, gate, up, cuts, turn, experts, capacity):
    tokens = ids.shape[1]
    width = rows.shape[1]
    hbm = pl.BlockSpec(memory_space=pltpu.HBM)

    def kernel(*refs):
        dispatch_kernel(*refs, turn=turn, experts=experts, capacity=capacity)

    def held(array):
        return pltpu.with_memory_space_constraint(array, pltpu.HBM)

    return pl.pallas_call(
        kernel,
        in_specs=[pl.BlockSpec(memory_space=pltpu.SMEM), hbm, hbm, whole(), hbm, hbm],
        out_specs=[whole()] * (2 + len(cuts)),
        scratch_shapes=[
            pltpu.VMEM((tokens, width), BF16),
            pltpu.VMEM(gain.shape, F32),
            pltpu.SemaphoreType.DMA((2 + len(cuts),)),
        ],
        out_shape=[
            jax.ShapeDtypeStruct((experts, capacity * width // LANES, LANES), BF16),
            jax.ShapeDtypeStruct((2, tokens), jnp.int32),
            *(jax.ShapeDtypeStruct((cut, gate.shape[1]), BF16) for cut in cuts),
        ],
        compiler_params=pltpu.CompilerParams(vmem_limit_bytes=24 << 20),
        name="dispatch",
    )(own, held(rows), held(gain), ids, held(gate), held(up))


def expert_kernel(*refs, sources, far, peers, capacity, blocks):
    odd_ref, message_ref = refs[0], refs[1]
    count = sum(len(rows) for rows in far)
    given = list(refs[2 : count + 2])
    out_ref, rows_ref, hidden_ref = refs[count + 2 : count + 5]
    near, signals = list(refs[count + 5 : -1]), refs[-1]
    odd = odd_ref[0] == 1
    weights, copies = [], []
    used = 0
    for rows in far:
        pieces = [given.pop(0) for _ in rows]
        if rows == (0,):
            weights.append(pieces[0])
            copies.append([])
            continue
        if rows[0] < 0:
            weights.append(near.pop(0))
            copies.append([])
            at = 0
            for piece in pieces:
                weights[-1][at : at + piece.shape[0], :] = piece[...]
                at += piece.shape[0]
            continue
        weights.append(near.pop(0))
        moves, at = [], 0
        for piece, size in zip(pieces, rows):
            place = weights[-1].at[at : at + size, :]
            moves.append(pltpu.make_async_copy(piece, place, signals.at[used]))
            at += size
            used += 1
        copies.append(moves)
    waves = [[*s[0], *s[1]] for s in sources] + [[d for s in sources for d in s[2]]]

    def issue(wave):
        for w in wave:
            for move in copies[w]:
                move.start()

    def settle(wave):
        for w in wave:
            for move in copies[w]:
                move.wait()

    issue(waves[0])
    issue(waves[1])
    head, tail = split_rows(capacity)
    per = 8 // tail
    heads = peers * head
    for c in range(0, blocks, 2):
        both = message_ref[:, c * head : (c + 2) * head, :].astype(F32)
        for i in range(2):
            part = both[:, i * head : (i + 1) * head, :].reshape(heads, LANES)
            rows_ref[0:heads, (c + i) * LANES : (c + i + 1) * LANES] = part.astype(BF16)
    base = blocks * head
    slot = lax.broadcasted_iota(jnp.int32, (peers * tail, peers * 8), 0)
    lane = lax.broadcasted_iota(jnp.int32, (peers * tail, peers * 8), 1)
    gathers = [
        (lane == slot // tail * 8 + q * tail + slot % tail).astype(F32).astype(BF16)
        for q in range(per)
    ]
    for j in range(0, blocks // per, 2):
        both = message_ref[:, base + j * 8 : base + (j + 2) * 8, :].astype(F32)
        for i in range(2):
            part = both[:, i * 8 : (i + 1) * 8, :].reshape(peers * 8, LANES).astype(BF16)
            for q in range(per):
                c = per * (j + i) + q
                rows_ref[heads:, c * LANES : (c + 1) * LANES] = dot(gathers[q], part).astype(BF16)
    at = 0
    downs = []
    for n, (gates, ups, down_parts, swapped) in enumerate(sources):
        settle(waves[n])
        if n + 2 < len(waves):
            issue(waves[n + 2])
        rows = rows_ref[...]
        values = []
        for group in (gates, ups):
            value = None
            begin = 0
            for g in group:
                size = weights[g].shape[0]
                part = dot(rows[:, begin : begin + size], weights[g][...])
                value = part if value is None else value + part
                begin += size
            values.append(value)
        gate_value, up_value = values
        if swapped:
            gate_value, up_value = (
                jnp.where(odd, up_value, gate_value),
                jnp.where(odd, gate_value, up_value),
            )
        hidden = gate_value / (1.0 + jnp.exp(-gate_value)) * up_value
        hidden_ref[:, at : at + hidden.shape[1]] = hidden.astype(BF16)
        for d in down_parts:
            downs.append((at, d))
            at += weights[d].shape[0]
    settle(waves[-1])
    slot = lax.broadcasted_iota(jnp.int32, (peers * 8, peers * tail), 1)
    lane = lax.broadcasted_iota(jnp.int32, (peers * 8, peers * tail), 0)
    spreads = [
        (lane == slot // tail * 8 + q * tail + slot % tail).astype(F32).astype(BF16)
        for q in range(per)
    ]
    step = 2 * per
    for first in range(0, blocks, step):
        cols = slice(first * LANES, (first + step) * LANES)
        total = None
        for begin, d in downs:
            size = weights[d].shape[0]
            part = dot(hidden_ref[:, begin : begin + size], weights[d][:, cols])
            total = part if total is None else total + part
        for c in range(0, step, 2):
            pair = [col(total, c + i)[0:heads].reshape(peers, head, LANES) for i in range(2)]
            at_row = (first + c) * head
            out_ref[:, at_row : at_row + 2 * head, :] = jnp.concatenate(pair, axis=1).astype(BF16)
        last = total[heads:].astype(BF16)
        pair = []
        for i in range(2):
            spread = None
            for q in range(per):
                part = dot(spreads[q], col(last, per * i + q))
                spread = part if spread is None else spread + part
            pair.append(spread.reshape(peers, 8, LANES))
        at_row = base + first // per * 8
        out_ref[:, at_row : at_row + 16, :] = jnp.concatenate(pair, axis=1).astype(BF16)


def experts_apply(odd, message, matrices, direct, sources, capacity):
    peers, lines, _ = message.shape
    blocks = lines // capacity
    far = []
    for pieces, held in zip(matrices, direct):
        rows = tuple(p.shape[0] for p in pieces)
        far.append(rows if not held else (0,) if len(rows) == 1 else tuple(-r for r in rows))
    units = sum(sum(p.shape[0] for p in matrices[d]) for s in sources for d in s[2])

    def kernel(*refs):
        expert_kernel(*refs, sources=sources, far=far, peers=peers, capacity=capacity, blocks=blocks)

    operands, specs, scratch = [], [], []
    for pieces, rows in zip(matrices, far):
        if rows == (0,):
            operands.extend(pieces)
            specs.append(whole())
            continue
        scratch.append(pltpu.VMEM((abs(sum(rows)), pieces[0].shape[1]), BF16))
        if rows[0] < 0:
            operands.extend(pieces)
            specs.extend(whole() for _ in pieces)
            continue
        operands.extend(pltpu.with_memory_space_constraint(p, pltpu.HBM) for p in pieces)
        specs.extend(pl.BlockSpec(memory_space=pltpu.HBM) for _ in pieces)
    return pl.pallas_call(
        kernel,
        in_specs=[pl.BlockSpec(memory_space=pltpu.SMEM), whole(), *specs],
        out_specs=whole(),
        out_shape=jax.ShapeDtypeStruct(message.shape, BF16),
        scratch_shapes=[
            pltpu.VMEM((peers * capacity, blocks * LANES), BF16),
            pltpu.VMEM((peers * capacity, units), BF16),
            *scratch,
            pltpu.SemaphoreType.DMA((len(operands),)),
        ],
        compiler_params=pltpu.CompilerParams(vmem_limit_bytes=40 << 20),
        name="experts",
    )(odd, message, *operands)


def combine_kernel(
    message_ref, target_ref, far_ref, gain_ref, out_ref, mixed_ref, weight_ref, signal, *, capacity
):
    copy = pltpu.make_async_copy(far_ref, weight_ref, signal)
    copy.start()
    peers = message_ref.shape[0]
    tokens, width = out_ref.shape
    blocks = width // LANES
    head, tail = split_rows(capacity)
    per = 8 // tail
    heads = peers * head
    target = target_ref[...]
    peer = target // capacity
    place = target - peer * capacity
    in_head = jnp.where(place < head, peer * head + place, -64)
    in_tail = jnp.where(place < head, -64, peer * 8 + place - head)
    pick = [selection(in_head[:, k : k + 1], 0, heads, 1).astype(F32) for k in range(2)]
    pick = jnp.concatenate(pick, axis=0).astype(BF16)
    picks = []
    for q in range(per):
        both = [selection(in_tail[:, k : k + 1], -q * tail, peers * 8, 1).astype(F32) for k in range(2)]
        picks.append(jnp.concatenate(both, axis=0).astype(BF16))
    copy.wait()
    weight = [weight_ref[:, k : k + 1] for k in range(2)]
    base = blocks * head
    square = jnp.zeros((tokens, LANES), F32)
    for c in range(0, blocks, 2):
        both = message_ref[:, c * head : (c + 2) * head, :].astype(F32)
        for i in range(2):
            part = both[:, i * head : (i + 1) * head, :].reshape(heads, LANES).astype(BF16)
            j = (c + i) // per
            rest = message_ref[:, base + j // 2 * 16 : base + j // 2 * 16 + 16, :].astype(F32)
            rest = rest[:, j % 2 * 8 : j % 2 * 8 + 8, :].reshape(peers * 8, LANES).astype(BF16)
            rows = dot(pick, part) + dot(picks[(c + i) % per], rest)
            mixed = rows[:tokens] * weight[0] + rows[tokens:] * weight[1]
            mixed_ref[:, (c + i) * LANES : (c + i + 1) * LANES] = mixed
            square = square + mixed * mixed
    scale = lax.rsqrt(jnp.sum(square, axis=1, keepdims=True) * (1.0 / width) + EPSILON)
    out_ref[...] = (mixed_ref[...] * scale * gain_ref[...]).astype(BF16)


def combine(message, target, weight, gain, capacity):
    tokens = target.shape[0]
    width = gain.shape[1]

    def kernel(*refs):
        combine_kernel(*refs, capacity=capacity)

    return pl.pallas_call(
        kernel,
        in_specs=[whole(), whole(), pl.BlockSpec(memory_space=pltpu.HBM), whole()],
        out_specs=whole(),
        out_shape=jax.ShapeDtypeStruct((tokens, width), BF16),
        scratch_shapes=[
            pltpu.VMEM((tokens, width), F32),
            pltpu.VMEM(weight.shape, F32),
            pltpu.SemaphoreType.DMA,
        ],
        compiler_params=pltpu.CompilerParams(vmem_limit_bytes=24 << 20),
        name="combine",
    )(message, target, pltpu.with_memory_space_constraint(weight, pltpu.HBM), gain)


def conv_kernel(rows_ref, carried_ref, taps_ref, gain_ref, weight_ref, out_ref, line_ref, sum_ref):
    block, width = rows_ref.shape
    blocks = width // LANES
    reach = taps_ref.shape[0] - 1
    halo = line_ref.shape[1] - block
    step = pl.program_id(0)

    @pl.when(step == 0)
    def _():
        for c in range(blocks):
            line_ref[c, 0:halo, :] = col(carried_ref, c).astype(F32)

    @pl.when(step > 0)
    def _():
        for c in range(blocks):
            line_ref[c, 0:halo, :] = line_ref[c, block : block + halo, :]

    for c in range(blocks):
        line_ref[c, halo:, :] = col(rows_ref, c).astype(F32)

    strip = 64

    def column(c, square):
        parts = []
        for first in range(0, block, strip):
            total = jnp.zeros((strip, LANES), F32)
            for k in range(reach + 1):
                at = first + halo - reach + k
                total = total + line_ref[c, at : at + strip, :] * taps_ref[k, pl.ds(c, 1), :]
            sum_ref[c, first : first + strip, :] = total
            parts.append(total * total)
        return square + jnp.concatenate(parts, axis=0)

    square = lax.fori_loop(0, blocks, column, jnp.zeros((block, LANES), F32))
    scale = lax.rsqrt(jnp.sum(square, axis=1, keepdims=True) * (1.0 / width) + EPSILON)
    result = jnp.zeros((block, out_ref.shape[1]), F32)
    for c in range(0, blocks, 4):
        group = []
        for i in range(4):
            value = sum_ref[c + i] * scale * col(gain_ref, c + i)
            group.append((value / (1.0 + jnp.exp(-value))).astype(BF16))
        part = jnp.concatenate(group, axis=1)
        result = result + dot(part, weight_ref[c * LANES : (c + 4) * LANES, :])
    out_ref[...] = result.astype(BF16)


def conv_module(rows, carried, taps, gain, weight, block=128):
    count, width = rows.shape
    blocks = width // LANES
    halo = carried.shape[0]
    return pl.pallas_call(
        conv_kernel,
        grid=(count // block,),
        in_specs=[
            pl.BlockSpec((block, width), lambda i: (i, 0)),
            pl.BlockSpec((halo, width), lambda i: (0, 0)),
            pl.BlockSpec((taps.shape[0], blocks, LANES), lambda i: (0, 0, 0)),
            pl.BlockSpec((1, width), lambda i: (0, 0)),
            pl.BlockSpec(weight.shape, lambda i: (0, 0)),
        ],
        out_specs=pl.BlockSpec((block, weight.shape[1]), lambda i: (i, 0)),
        out_shape=jax.ShapeDtypeStruct((count, weight.shape[1]), BF16),
        scratch_shapes=[
            pltpu.VMEM((blocks, block + halo, LANES), F32),
            pltpu.VMEM((blocks, block, LANES), F32),
        ],
        compiler_params=pltpu.CompilerParams(vmem_limit_bytes=24 << 20),
        name="conv",
    )(rows, carried, taps.reshape(taps.shape[0], blocks, LANES), gain, weight)


EP = "ep"
GRP_EP = ("grp", "ep")
GRP_EP_TP = ("grp", "ep", "tp")
HALO = 32


def run(
    conv_input,
    conv_taps,
    conv_gain,
    conv_weight,
    moe_input,
    moe_gain,
    expert_ids,
    route_weights,
    gate_weight,
    up_weight,
    down_weight,
    post_gain,
):
    quarters = lax.axis_size("tp")
    ep_count = lax.axis_size(EP)
    width = moe_input.shape[1]
    tokens = moe_input.shape[0] // quarters
    capacity = 2 * tokens // ep_count
    own = lax.axis_index("tp").astype(jnp.int32)

    odd = (lax.axis_index("grp") % 2).astype(jnp.int32)

    right = [(i, (i + 1) % quarters) for i in range(quarters)]
    left = [(i, (i - 1) % quarters) for i in range(quarters)]
    across = [(i, i ^ 1) for i in range(lax.axis_size("grp"))]
    gate, up, down = gate_weight[0], up_weight[0], down_weight[0]
    half, part = gate.shape[0] // 2, down.shape[0] * 7 // 8

    def send(array, pairs):
        return lax.ppermute(array, "tp", pairs)

    def swap(array):
        return lax.ppermute(array, "grp", across)

    down_r = send(down, right)
    turn = ep_count - ep_count // 4 - 1
    order = [(turn - i) % ep_count for i in range(ep_count)]

    def exchange(array):
        return lax.all_to_all(array, EP, 0, 0, axis_index_groups=[order], tiled=True)

    own_ids = lax.dynamic_slice_in_dim(expert_ids, own * tokens, tokens, 0).T
    message, target, mine_a, mine_b = dispatch(
        jnp.stack([own, odd]),
        moe_input,
        moe_gain.reshape(1, width),
        own_ids,
        gate,
        up,
        (half, gate.shape[0] - half),
        turn,
        ep_count,
        capacity,
    )
    mine_a_l, mine_b_l = send(mine_a, left), send(mine_b, left)
    arrived = exchange(message)
    other_a_l, mine_a_far = swap(mine_a_l), send(mine_a_l, left)
    mine_a_r, mine_b_r = send(mine_a, right), send(mine_b, right)
    down_l = send(down, left)
    pairs = [(i, i + 1) for i in range(ep_count - 1)]
    carried = lax.ppermute(conv_input[conv_input.shape[0] - HALO :], EP, pairs)
    other_b_l = swap(mine_b_l)
    down_a_far = send(down_r[:part], right)
    other_a_r = swap(mine_a_r)
    other_b_r, mine_b_far = swap(mine_b_r), send(mine_b_r, right)
    other_a_far = swap(mine_a_far)
    other_b_far, down_b_far = send(other_b_l, left), send(down_l[part:], left)

    conv_out = conv_module(conv_input, carried, conv_taps, conv_gain.reshape(1, width), conv_weight)

    matrices = [
        *((gate,), (up,), (down,)),
        *((mine_a_r, mine_b_r), (other_a_r, other_b_r), (down_r,)),
        *((mine_a_l, mine_b_l), (other_a_l, other_b_l), (down_l,)),
        *((mine_a_far,), (mine_b_far,), (other_a_far,), (other_b_far,), (down_a_far, down_b_far)),
    ]
    sources = (
        ((0,), (1,), (2,), False),
        ((6,), (7,), (8,), True),
        ((3,), (4,), (5,), True),
        ((9, 10), (11, 12), (13,), True),
    )
    direct = tuple(n in (11, 12, 13) for n in range(len(matrices)))
    results = experts_apply(odd.reshape(1), arrived, matrices, direct, sources, capacity)
    returned = exchange(results)
    own_weights = lax.dynamic_slice_in_dim(route_weights, own * tokens, tokens, 0)
    moe_out = combine(returned, target.T, own_weights, post_gain.reshape(1, width), capacity)
    return (conv_out, moe_out)


def solution(mesh):
    return jax.shard_map(
        run,
        mesh=mesh,
        in_specs=(
            P(GRP_EP, None),
            P(),
            P(),
            P(None, "tp"),
            P(GRP_EP, None),
            P(),
            P(GRP_EP, None),
            P(GRP_EP, None),
            P(EP, None, "tp"),
            P(EP, None, "tp"),
            P(EP, "tp", None),
            P(),
        ),
        out_specs=(P(GRP_EP, "tp"), P(GRP_EP_TP, None)),
        check_vma=False,
    )
```
